32 devices in a mesh: sp: 4 (over z), fs: 4 (over y, x), tp: 2 (over core).
Axes of the slice: x: 2, y: 2, z: 4, core: 2. Of those that a mesh axis runs over, the one named last changes fastest.
Arguments:
- tokens: bfloat16 [4, 512, 2048], P('fs', 'sp'), may hold values from -6 to 6
- norm_gain: float32 [2048], replicated, may hold values from 0.1 to 1.9
- w_ret_query: bfloat16 [2048, 2048], P(('sp', 'fs'), 'tp'), may hold values from -0.125 to 0.125
- w_ret_key: bfloat16 [2048, 2048], P(('sp', 'fs'), 'tp'), may hold values from -0.125 to 0.125
- w_ret_value: bfloat16 [2048, 2048], P(('sp', 'fs'), 'tp'), may hold values from -0.125 to 0.125
- w_q_down: bfloat16 [2048, 768], P(('sp', 'fs'), 'tp'), may hold values from -0.125 to 0.125
- w_kv_down: bfloat16 [2048, 512], P(('sp', 'fs'), 'tp'), may hold values from -0.125 to 0.125
- w_rope_key: bfloat16 [2048, 64], P(('sp', 'fs')), may hold values from -0.125 to 0.125
- w_q_up: bfloat16 [768, 3072], P(None, 'tp'), may hold values from -0.21875 to 0.21875
- w_kv_up: bfloat16 [512, 4096], P(None, 'tp'), may hold values from -0.25 to 0.25
- q_lat_gain: float32 [768], replicated, may hold values from 0.4 to 10
- kv_lat_gain: float32 [512], replicated, may hold values from 0.4 to 10
- att_norm_gain: float32 [2048], P('tp'), may hold values from 0.1 to 1.9
- ret_norm_gain: float32 [2048], P('tp'), may hold values from 0.1 to 1.9
- w_ret_out: bfloat16 [2048, 2048], P(('sp', 'fs'), 'tp'), may hold values from -0.09375 to 0.09375
- w_att_out: bfloat16 [2048, 2048], P(('sp', 'fs'), 'tp'), may hold values from -0.09375 to 0.09375
- head_rate: float32 [8], P('tp'), may hold values from -0.05 to 0
- decay_shift: float32 [4, 8, 512], P('fs', 'tp', 'sp'), may hold values from -1.1 to 0
- start_state: float32 [4, 8, 256, 256], P('fs', 'tp'), may hold values from -20 to 20
Outputs:
- mixed: bfloat16 [4, 512, 2048], P('fs', ('sp', 'tp'))
The draws below stay inside these ranges and needn't reach their ends.
All inputs are finite; a program needn't handle non-finite values.
Results may differ from the reference program's by a relative error of at most 0.018.
The reference program's roundings to bfloat16 on the way count: a program that leaves them out, or rounds other values in their place, can miss the bound.
Values may be sent and summed in bfloat16 or wider, within the bound.
A program may use at most 64 MiB of HBM per device.

```python
import jax
import jax.numpy as jnp
from jax import lax

D = 2048
RETENTION_HEADS = 8
RET_DIM = 256
ATT_HEADS = 16
NOPE_DIM = 128
ROPE_DIM = 64
VAL_DIM = 128
Q_LAT = 768
KV_LAT = 512
TOK_DEV = 128
SEQUENCE_LENGTH = 512
SEQUENCE_COUNT = 4
N_SP = 4
N_TP = 2


def draw_head_rate(key, part):
    key_perm, key_fast, key_slow = jax.random.split(key, 3)
    shuffled = jax.random.permutation(key_perm, RETENTION_HEADS)
    quick_count = RETENTION_HEADS // 2
    is_fast = shuffled < quick_count
    fast_rate = jnp.exp(jax.random.uniform(key_fast, (RETENTION_HEADS,), jnp.float32, jnp.log(0.02), jnp.log(0.05)))
    slow_rate = jnp.exp(jax.random.uniform(key_slow, (RETENTION_HEADS,), jnp.float32, jnp.log(0.05), jnp.log(0.5))) / SEQUENCE_LENGTH
    return -jnp.where(is_fast, fast_rate, slow_rate)


def draw_decay_shift(key, part):
    key_block, key_jitter, key_offsets, key_decay_factor = jax.random.split(key, 4)
    blocks = SEQUENCE_LENGTH // TOK_DEV
    block_level = jax.random.uniform(key_block, (SEQUENCE_COUNT, RETENTION_HEADS, blocks, 1), jnp.float32, 0.1, 0.6)
    jitter = jax.random.uniform(key_jitter, (SEQUENCE_COUNT, RETENTION_HEADS, blocks, TOK_DEV), jnp.float32, 0.5, 1.5)
    constant_decay = -(block_level * jitter).reshape(SEQUENCE_COUNT, RETENTION_HEADS, SEQUENCE_LENGTH) / SEQUENCE_LENGTH
    segment_index = jax.random.randint(key_offsets, (SEQUENCE_COUNT, RETENTION_HEADS, 2), 0, SEQUENCE_LENGTH)
    segment_length = jax.random.uniform(key_decay_factor, (SEQUENCE_COUNT, RETENTION_HEADS, 2), jnp.float32, 0.22, 0.5)
    position_offsets = jnp.arange(SEQUENCE_LENGTH)[None, None, None, :] == segment_index[..., None]
    segment_count = jnp.sum(jnp.where(position_offsets, segment_length[..., None], 0.0), axis=2)
    return constant_decay - segment_count


def draw_q_lat_gain(key, part):
    return jnp.clip(1.0 + 0.18 * jax.random.normal(key, (Q_LAT,), jnp.float32), 0.4, 1.6)


def draw_kv_lat_gain(key, part):
    return jnp.clip(1.0 + 0.18 * jax.random.normal(key, (KV_LAT,), jnp.float32), 0.4, 1.6)


def shard_levels(stream_key, shape, shards, least, high):
    factor_of, own = 1.0, jax.random.fold_in(stream_key, 6)
    for axis_at, shards_of in shards:
        draws = jnp.exp(jax.random.uniform(jax.random.fold_in(own, axis_at), (shards_of,), jnp.float32, least / len(shards), high / len(shards)))
        factor_of = factor_of * jnp.repeat(draws, shape[axis_at] // shards_of).reshape([-1 if axis == axis_at else 1 for axis in range(len(shape))])
    return factor_of


def noise(own_key, dims, scale, reach, shards=(), kind=jnp.bfloat16):
    gain = shard_levels(own_key, dims, shards, -0.22, 0.18) if shards else 1.0
    array = jax.random.normal(own_key, dims, jnp.float32) * scale * gain
    return jnp.minimum(jnp.maximum(array, -reach), reach).astype(kind)


def setup_inputs(seed: int = 0) -> dict:
    seeds = jax.random.split(jax.random.key(seed), 20)
    return {
        "tokens": noise(seeds[0], (SEQUENCE_COUNT, SEQUENCE_LENGTH, D), 1.0, 6.0, ((0, 4), (1, 4))),
        "norm_gain": jnp.clip(1.0 + 0.18 * jax.random.normal(seeds[1], (D,), jnp.float32), 0.1, 1.9),
        "w_ret_query": noise(seeds[2], (D, RETENTION_HEADS * RET_DIM), D ** -0.5, 0.125, ((0, 16), (1, 2))),
        "w_ret_key": noise(seeds[3], (D, RETENTION_HEADS * RET_DIM), D ** -0.5, 0.125, ((0, 16), (1, 2))),
        "w_ret_value": noise(seeds[4], (D, RETENTION_HEADS * RET_DIM), D ** -0.5, 0.125, ((0, 16), (1, 2))),
        "w_q_down": noise(seeds[5], (D, Q_LAT), D ** -0.5, 0.125, ((0, 16), (1, 2))),
        "w_kv_down": noise(seeds[6], (D, KV_LAT), D ** -0.5, 0.125, ((0, 16), (1, 2))),
        "w_rope_key": noise(seeds[7], (D, ROPE_DIM), D ** -0.5, 0.125, ((0, 16),)),
        "w_q_up": noise(seeds[8], (Q_LAT, ATT_HEADS * (NOPE_DIM + ROPE_DIM)), Q_LAT ** -0.5, 0.21875, ((1, 2),)),
        "w_kv_up": noise(seeds[9], (KV_LAT, ATT_HEADS * (NOPE_DIM + VAL_DIM)), KV_LAT ** -0.5, 0.25, ((1, 2),)),
        "q_lat_gain": draw_q_lat_gain(jax.random.fold_in(seeds[19], 71), 0),
        "kv_lat_gain": draw_kv_lat_gain(jax.random.fold_in(seeds[19], 71), 0),
        "att_norm_gain": jnp.clip(1.0 + 0.18 * jax.random.normal(seeds[12], (ATT_HEADS * VAL_DIM,), jnp.float32), 0.1, 1.9),
        "ret_norm_gain": jnp.clip(1.0 + 0.18 * jax.random.normal(seeds[13], (RETENTION_HEADS * RET_DIM,), jnp.float32), 0.1, 1.9),
        "w_ret_out": noise(seeds[14], (D, RETENTION_HEADS * RET_DIM), (RETENTION_HEADS * RET_DIM + ATT_HEADS * VAL_DIM) ** -0.5, 0.09375, ((0, 16), (1, 2))),
        "w_att_out": noise(seeds[15], (D, ATT_HEADS * VAL_DIM), (RETENTION_HEADS * RET_DIM + ATT_HEADS * VAL_DIM) ** -0.5, 0.09375, ((0, 16), (1, 2))),
        "head_rate": draw_head_rate(jax.random.fold_in(seeds[19], 71), 0),
        "decay_shift": draw_decay_shift(jax.random.fold_in(seeds[19], 71), 0),
        "start_state": noise(seeds[18], (SEQUENCE_COUNT, RETENTION_HEADS, RET_DIM, RET_DIM), (0.15 * (TOK_DEV * N_SP) ** 0.5), 20.0, ((0, 4), (1, 2)), jnp.float32),
    }


EPSILON = 1e-06
THETA_BASE = 10000.0
TOP_PRECISION = lax.Precision.HIGHEST

def angle_tables(positions, rot_width):
    half_width = rot_width // 2
    inverse = THETA_BASE ** (-jnp.arange(half_width, dtype=jnp.float32) * 2.0 / rot_width)
    angles = positions.astype(jnp.float32)[:, None] * inverse[None, :]
    return (jnp.cos(angles), jnp.sin(angles))

def rotate(values, cosine, sine):
    half_width = values.shape[-1] // 2
    front_half = values[..., :half_width]
    back_half = values[..., half_width:]
    return jnp.concatenate([front_half * cosine - back_half * sine, back_half * cosine + front_half * sine], axis=-1)

def rms_scale(values, gain_vector):
    return values * lax.rsqrt(lax.optimization_barrier(jnp.mean(values * values, axis=-1, keepdims=True)) + EPSILON) * gain_vector

def saved_states(values):
    return lax.optimization_barrier(values.astype(jnp.bfloat16))

def reference(tokens, norm_gain, w_ret_query, w_ret_key, w_ret_value, w_q_down, w_kv_down, w_rope_key, w_q_up, w_kv_up, q_lat_gain, kv_lat_gain, att_norm_gain, ret_norm_gain, w_ret_out, w_att_out, head_rate, decay_shift, start_state):
    positions = jnp.arange(SEQUENCE_LENGTH, dtype=jnp.int32)
    ret_cos, ret_sin = angle_tables(positions, RET_DIM)
    rope_cos, rope_sin = angle_tables(positions, ROPE_DIM)
    att_scale = (NOPE_DIM + ROPE_DIM) ** (-0.5)
    group_ret = RETENTION_HEADS * RET_DIM // N_TP
    group_att = ATT_HEADS * VAL_DIM // N_TP

    def one_sequence(inputs):
        sequence, shift_rows, first_state = inputs
        source = sequence.astype(jnp.float32)
        normed = saved_states(rms_scale(source, norm_gain))

        def project(weight):
            return jnp.dot(normed, weight, preferred_element_type=jnp.float32)
        retention_query = saved_states(rotate(project(w_ret_query).reshape(SEQUENCE_LENGTH, RETENTION_HEADS, RET_DIM), ret_cos[:, None], ret_sin[:, None]))
        retention_key = saved_states(rotate(project(w_ret_key).reshape(SEQUENCE_LENGTH, RETENTION_HEADS, RET_DIM), ret_cos[:, None], ret_sin[:, None]) * RET_DIM ** (-0.5))
        retention_value = saved_states(project(w_ret_value).reshape(SEQUENCE_LENGTH, RETENTION_HEADS, RET_DIM))
        lat_q_raw = saved_states(project(w_q_down))
        lat_kv_raw = saved_states(project(w_kv_down))
        rope_key = saved_states(rotate(project(w_rope_key), rope_cos, rope_sin))
        q_latent = saved_states(rms_scale(lat_q_raw.astype(jnp.float32), q_lat_gain))
        kv_latent = saved_states(rms_scale(lat_kv_raw.astype(jnp.float32), kv_lat_gain))
        query_full = jnp.dot(q_latent, w_q_up, preferred_element_type=jnp.float32).reshape(SEQUENCE_LENGTH, ATT_HEADS, NOPE_DIM + ROPE_DIM)
        att_query = saved_states(jnp.concatenate([query_full[..., :NOPE_DIM], rotate(query_full[..., NOPE_DIM:], rope_cos[:, None], rope_sin[:, None])], axis=-1))
        expanded = saved_states(jnp.dot(kv_latent, w_kv_up, preferred_element_type=jnp.float32)).reshape(SEQUENCE_LENGTH, ATT_HEADS, NOPE_DIM + VAL_DIM)
        key_nope = expanded[..., :NOPE_DIM].astype(jnp.float32)
        key_values = expanded[..., NOPE_DIM:].astype(jnp.float32)
        rope_wide = rope_key.astype(jnp.float32)

        def query_block(block_index):
            first_row = block_index * TOK_DEV
            block_query = lax.dynamic_slice_in_dim(att_query, first_row, TOK_DEV, 0).astype(jnp.float32)
            score_matrix = (jnp.einsum('qhd,khd->hqk', block_query[..., :NOPE_DIM], key_nope) + jnp.einsum('qhd,kd->hqk', block_query[..., NOPE_DIM:], rope_wide)) * att_scale
            allowed = positions[None, :] <= (first_row + jnp.arange(TOK_DEV, dtype=jnp.int32))[:, None]
            masked = jnp.where(allowed[None], score_matrix, -jnp.inf)
            weights = jnp.exp(masked - lax.optimization_barrier(jnp.max(masked, axis=-1, keepdims=True)))
            rounded = saved_states(weights).astype(jnp.float32)
            numerator = jnp.einsum('hqk,khd->qhd', rounded, key_values)
            denominator = lax.optimization_barrier(jnp.sum(weights, axis=-1))
            return numerator / denominator.T[:, :, None]
        att_raw = lax.map(query_block, jnp.arange(N_SP)).reshape(SEQUENCE_LENGTH, ATT_HEADS, VAL_DIM)
        att_out = saved_states(rms_scale(att_raw, att_norm_gain.reshape(ATT_HEADS, VAL_DIM))).reshape(SEQUENCE_LENGTH, ATT_HEADS * VAL_DIM)
        log_rates = head_rate[:, None] + shift_rows
        offsets = jnp.arange(TOK_DEV, dtype=jnp.int32)
        lower_mask = offsets[None, :] <= offsets[:, None]

        def ret_block(carried_state, block_index):
            first_row = block_index * TOK_DEV
            cumul = jnp.cumsum(lax.dynamic_slice_in_dim(log_rates, first_row, TOK_DEV, 1), axis=1)
            decay_matrix = jnp.exp(jnp.where(lower_mask[None], cumul[:, :, None] - cumul[:, None, :], -jnp.inf))
            block_queries = lax.dynamic_slice_in_dim(retention_query, first_row, TOK_DEV, 0).astype(jnp.float32)
            block_keys = lax.dynamic_slice_in_dim(retention_key, first_row, TOK_DEV, 0).astype(jnp.float32)
            block_values = lax.dynamic_slice_in_dim(retention_value, first_row, TOK_DEV, 0).astype(jnp.float32)
            score_matrix = saved_states(jnp.einsum('zgq,ugq->gzu', block_queries, block_keys) * decay_matrix).astype(jnp.float32)
            inside_block_output = jnp.einsum('vzs,svp->zvp', score_matrix, block_values)
            carried_term = jnp.einsum('nhd,hde->nhe', block_queries, carried_state, precision=TOP_PRECISION) * jnp.exp(cumul).T[:, :, None]
            block_output_sum = cumul[:, -1]
            weighted_values = block_keys * jnp.exp(block_output_sum[:, None] - cumul).T[:, :, None]
            updated_state = jnp.exp(block_output_sum)[:, None, None] * carried_state + jnp.einsum('uzj,uzv->zjv', weighted_values, block_values, precision=TOP_PRECISION)
            return (updated_state, inside_block_output + carried_term)
        ignored_state, ret_blocks = lax.scan(ret_block, first_state, jnp.arange(N_SP))
        ret_raw = ret_blocks.reshape(SEQUENCE_LENGTH, RETENTION_HEADS, RET_DIM)
        row_mean = lax.optimization_barrier(jnp.mean(ret_raw, axis=-1, keepdims=True))
        centered = ret_raw - row_mean
        row_var = lax.optimization_barrier(jnp.mean(centered * centered, axis=-1, keepdims=True))
        ret_out = saved_states(centered * lax.rsqrt(row_var + EPSILON) * ret_norm_gain.reshape(RETENTION_HEADS, RET_DIM)).reshape(SEQUENCE_LENGTH, RETENTION_HEADS * RET_DIM)
        summed = jnp.zeros((SEQUENCE_LENGTH, D), jnp.float32)
        for group_index in range(N_TP):
            ret_cols = slice(group_index * group_ret, (group_index + 1) * group_ret)
            att_cols = slice(group_index * group_att, (group_index + 1) * group_att)
            partial_value = jnp.dot(ret_out[:, ret_cols], w_ret_out[:, ret_cols].T, preferred_element_type=jnp.float32) + jnp.dot(att_out[:, att_cols], w_att_out[:, att_cols].T, preferred_element_type=jnp.float32)
            summed = summed + saved_states(partial_value).astype(jnp.float32)
        return summed.astype(jnp.bfloat16)
    return lax.map(one_sequence, (tokens, decay_shift, start_state))
```

```python
import functools

import numpy as np

import jax
import jax.numpy as jnp
from jax import lax
from jax.experimental import pallas as pl
from jax.experimental.pallas import tpu as pltpu
from jax.sharding import PartitionSpec as P

RET_DIM = 256
NOPE_DIM = 128
ROPE_DIM = 64
VAL_DIM = 128
KV_LAT = 512


EPSILON = 1e-06
THETA_BASE = 10000.0
TOP_PRECISION = lax.Precision.HIGHEST


def prefix(x, axis, combine, identity):
    peers, position = (lax.axis_size(axis), lax.axis_index(axis))
    everything = jax.tree.map(
        lambda part, kind: lax.all_gather(part.astype(kind), axis), x, (jnp.bfloat16, jnp.bfloat16)
    )
    start = jax.tree.map(
        lambda part, zero: jnp.broadcast_to(jnp.asarray(zero, part.dtype), part.shape), x, identity
    )

    def lap(k, before):
        reached = k < position
        new = combine(
            before, jax.tree.map(lambda part, own: part[k].astype(own.dtype), everything, x)
        )
        return jax.tree.map(lambda a, b: jnp.where(reached, a, b), new, before)

    return lax.fori_loop(0, peers, lap, start)


def angle_tables(positions, rot_width):
    half_width = rot_width // 2
    inverse = THETA_BASE ** (-jnp.arange(half_width, dtype=jnp.float32) * 2.0 / rot_width)
    angles = positions.astype(jnp.float32)[:, None] * inverse[None, :]
    return (jnp.cos(angles), jnp.sin(angles))


def rotate(values, cosine, sine):
    half_width = values.shape[-1] // 2
    front_half = values[..., :half_width]
    back_half = values[..., half_width:]
    return jnp.concatenate(
        [front_half * cosine - back_half * sine, back_half * cosine + front_half * sine], axis=-1
    )


def rms_scale(values, gain_vector):
    return (
        values
        * lax.rsqrt(jnp.mean(values * values, axis=-1, keepdims=True) + EPSILON)
        * gain_vector
    )


def chain_states(earlier, later):
    early_log, early_state = earlier
    late_log, late_state = later
    return (early_log + late_log, jnp.exp(late_log)[:, None, None] * early_state + late_state)


def rows_plan(
    tokens,
    norm_gain,
    w_ret_query,
    w_ret_key,
    w_ret_value,
    w_q_down,
    w_kv_down,
    w_rope_key,
    w_q_up,
    w_kv_up,
    q_lat_gain,
    kv_lat_gain,
    att_norm_gain,
    ret_norm_gain,
    w_ret_out,
    w_att_out,
    head_rate,
    decay_shift,
    start_state,
):
    tok_rows = tokens.shape[1]
    ret_local = head_rate.shape[0]
    att_local = w_q_up.shape[1] // (NOPE_DIM + ROPE_DIM)
    row_offset = lax.axis_index("sp") * tok_rows
    positions = row_offset + jnp.arange(tok_rows, dtype=jnp.int32)
    (
        full_query,
        full_key,
        full_value,
        full_q_down,
        full_kv_down,
        full_rope,
        full_ret_out,
        full_att_out,
    ) = (
        lax.all_gather(w_ret_query, ("sp", "fs"), axis=0, tiled=True),
        lax.all_gather(w_ret_key, ("sp", "fs"), axis=0, tiled=True),
        lax.all_gather(w_ret_value, ("sp", "fs"), axis=0, tiled=True),
        lax.all_gather(w_q_down, ("sp", "fs"), axis=0, tiled=True),
        lax.all_gather(w_kv_down, ("sp", "fs"), axis=0, tiled=True),
        lax.all_gather(w_rope_key, ("sp", "fs"), axis=0, tiled=True),
        lax.all_gather(w_ret_out, ("sp", "fs"), axis=0, tiled=True),
        lax.all_gather(w_att_out, ("sp", "fs"), axis=0, tiled=True),
    )
    source = tokens[0].astype(jnp.float32)
    normed = rms_scale(source, norm_gain).astype(jnp.bfloat16)
    ret_cos, ret_sin = angle_tables(positions, RET_DIM)
    rope_cos, rope_sin = angle_tables(positions, ROPE_DIM)

    def project(weight):
        return jnp.dot(normed, weight, preferred_element_type=jnp.float32)

    part_q = project(full_q_down).astype(jnp.bfloat16)
    part_kv = project(full_kv_down).astype(jnp.bfloat16)
    lat_q_raw, lat_kv_raw = (
        lax.all_gather(part_q, "tp", axis=1, tiled=True),
        lax.all_gather(part_kv, "tp", axis=1, tiled=True),
    )
    retention_query = rotate(
        project(full_query).reshape(tok_rows, ret_local, RET_DIM),
        ret_cos[:, None],
        ret_sin[:, None],
    ).astype(jnp.bfloat16)
    retention_key = (
        rotate(
            project(full_key).reshape(tok_rows, ret_local, RET_DIM),
            ret_cos[:, None],
            ret_sin[:, None],
        )
        * RET_DIM ** (-0.5)
    ).astype(jnp.bfloat16)
    retention_value = project(full_value).reshape(tok_rows, ret_local, RET_DIM).astype(jnp.bfloat16)
    rope_key = rotate(project(full_rope), rope_cos, rope_sin).astype(jnp.bfloat16)
    log_rates = head_rate[:, None] + decay_shift[0]
    cumul = jnp.cumsum(log_rates, axis=1)
    offsets = jnp.arange(tok_rows, dtype=jnp.int32)
    lower_mask = offsets[None, :] <= offsets[:, None]
    decay_matrix = jnp.exp(
        jnp.where(lower_mask[None], cumul[:, :, None] - cumul[:, None, :], -jnp.inf)
    )
    block_score_grid = (
        jnp.einsum(
            "zgq,ugq->gzu", retention_query, retention_key, preferred_element_type=jnp.float32
        )
        * decay_matrix
    ).astype(jnp.bfloat16)
    inside_block_output = jnp.einsum(
        "vzs,svp->zvp", block_score_grid, retention_value, preferred_element_type=jnp.float32
    )
    block_output_sum = cumul[:, -1]
    weighted_values = (
        retention_key.astype(jnp.float32) * jnp.exp(block_output_sum[:, None] - cumul).T[:, :, None]
    )
    contribution = jnp.einsum(
        "uzj,uzv->zjv",
        weighted_values,
        retention_value.astype(jnp.float32),
        precision=TOP_PRECISION,
    )
    identity = (jnp.zeros_like(block_output_sum), jnp.zeros_like(contribution))
    before_log, before_state = prefix(
        (block_output_sum, contribution), "sp", chain_states, identity
    )
    q_latent = rms_scale(lat_q_raw.astype(jnp.float32), q_lat_gain).astype(jnp.bfloat16)
    kv_latent = rms_scale(lat_kv_raw.astype(jnp.float32), kv_lat_gain).astype(jnp.bfloat16)
    query_full = jnp.dot(q_latent, w_q_up, preferred_element_type=jnp.float32).reshape(
        tok_rows, att_local, NOPE_DIM + ROPE_DIM
    )
    query_nope = query_full[..., :NOPE_DIM].astype(jnp.bfloat16)
    query_rope = rotate(query_full[..., NOPE_DIM:], rope_cos[:, None], rope_sin[:, None]).astype(
        jnp.bfloat16
    )
    att_scale = (NOPE_DIM + ROPE_DIM) ** (-0.5)

    def attend(carry, key_nope, key_values, key_rope, start):
        running_max, running_sum, running_acc = carry
        key_count = key_rope.shape[0]
        score_matrix = (
            jnp.einsum("qhd,khd->hqk", query_nope, key_nope, preferred_element_type=jnp.float32)
            + jnp.einsum("qhd,kd->hqk", query_rope, key_rope, preferred_element_type=jnp.float32)
        ) * att_scale
        key_positions = start + jnp.arange(key_count, dtype=jnp.int32)
        allowed = key_positions[None, :] <= positions[:, None]
        masked = jnp.where(allowed[None], score_matrix, -jnp.inf)
        new_max = jnp.maximum(running_max, jnp.max(masked, axis=-1))
        safe_max = jnp.where(jnp.isfinite(new_max), new_max, 0.0)
        weights = jnp.exp(masked - safe_max[..., None])
        rescale = jnp.exp(running_max - safe_max)
        new_sum = running_sum * rescale + jnp.sum(weights, axis=-1)
        new_acc = running_acc * rescale[..., None] + jnp.einsum(
            "hqk,khd->hqd",
            weights.astype(jnp.bfloat16),
            key_values,
            preferred_element_type=jnp.float32,
        )
        return (new_max, new_sum, new_acc)

    def expand_attend(carry_in, lat_piece, rope_piece, start):
        wide = (
            jnp.dot(lat_piece, w_kv_up, preferred_element_type=jnp.float32)
            .astype(jnp.bfloat16)
            .reshape(rope_piece.shape[0], att_local, NOPE_DIM + VAL_DIM)
        )
        return attend(carry_in, wide[..., :NOPE_DIM], wide[..., NOPE_DIM:], rope_piece, start)

    empty = (
        jnp.full((att_local, tok_rows), -jnp.inf, jnp.float32),
        jnp.zeros((att_local, tok_rows), jnp.float32),
        jnp.zeros((att_local, tok_rows, VAL_DIM), jnp.float32),
    )
    groups = lax.axis_size("tp")
    kv_part = KV_LAT // groups
    rope_part = ROPE_DIM // groups
    my_group = lax.axis_index("tp")
    joined = jnp.concatenate(
        [
            lax.dynamic_slice_in_dim(kv_latent, my_group * kv_part, kv_part, 1),
            lax.dynamic_slice_in_dim(rope_key, my_group * rope_part, rope_part, 1),
        ],
        axis=1,
    )
    all_rows = lax.all_gather(joined, "sp", axis=0, tiled=True)
    complete = lax.all_gather(all_rows, "tp", axis=1, tiled=True)
    total_rows = complete.shape[0]
    grouped = complete.reshape(total_rows, groups, kv_part + rope_part)
    lat_all = grouped[:, :, :kv_part].reshape(total_rows, KV_LAT)
    rope_all = grouped[:, :, kv_part:].reshape(total_rows, ROPE_DIM)

    def visit(block_index, carry_in):
        start = block_index * tok_rows
        lat_piece = lax.dynamic_slice_in_dim(lat_all, start, tok_rows, 0)
        rope_piece = lax.dynamic_slice_in_dim(rope_all, start, tok_rows, 0)
        return expand_attend(carry_in, lat_piece, rope_piece, start)

    final = lax.fori_loop(0, lax.axis_index("sp") + 1, visit, empty)
    att_raw = jnp.transpose(final[2] / final[1][..., None], (1, 0, 2))
    att_out = (
        rms_scale(att_raw, att_norm_gain.reshape(att_local, VAL_DIM))
        .astype(jnp.bfloat16)
        .reshape(tok_rows, att_local * VAL_DIM)
    )
    entering = jnp.exp(before_log)[:, None, None] * start_state[0] + before_state
    carried_term = (
        jnp.einsum(
            "nhd,hde->nhe", retention_query.astype(jnp.float32), entering, precision=TOP_PRECISION
        )
        * jnp.exp(cumul).T[:, :, None]
    )
    ret_raw = inside_block_output + carried_term
    row_mean = jnp.mean(ret_raw, axis=-1, keepdims=True)
    centered = ret_raw - row_mean
    row_var = jnp.mean(centered * centered, axis=-1, keepdims=True)
    ret_out = (
        (centered * lax.rsqrt(row_var + EPSILON) * ret_norm_gain.reshape(ret_local, RET_DIM))
        .astype(jnp.bfloat16)
        .reshape(tok_rows, ret_local * RET_DIM)
    )
    contract = (((1,), (1,)), ((), ()))
    mixed = lax.psum_scatter(
        (
            lax.dot_general(ret_out, full_ret_out, contract, preferred_element_type=jnp.float32)
            + lax.dot_general(att_out, full_att_out, contract, preferred_element_type=jnp.float32)
        ).astype(jnp.bfloat16),
        "tp",
        scatter_dimension=0,
        tiled=True,
    )
    return mixed[None]


MESH = pl.DeviceIdType.MESH
WIDE = RET_DIM
CONTRACT = (((1,), (1,)), ((), ()))
UNITS = 6
LAT, QUERY, KEY, VALUE, OUT_RET, OUT_ATT = range(UNITS)
LAT_PARTS = 2


def heads_fit(mesh, ret_local, sequences, q_wide, kv_wide, up_wide):
    sizes = mesh.shape
    return (
        sizes["sp"] == 4
        and sizes["fs"] == 4
        and sizes["tp"] == 2
        and ret_local == sizes["sp"]
        and sequences == 1
        and up_wide == 2 * (NOPE_DIM + ROPE_DIM) * ret_local
        and q_wide % 128 == 0
        and kv_wide % 128 == 0
        and q_wide + kv_wide + 2 * ROPE_DIM <= ret_local * WIDE
    )


def wave_tables(length, wide):
    half_wide = wide // 2
    powers = np.arange(half_wide, dtype=np.float32) * np.float32(2.0 / wide)
    inverse = np.power(np.float32(THETA_BASE), -powers).astype(np.float32)
    angles = np.arange(length, dtype=np.float32)[:, None] * inverse[None, :]
    return np.cos(angles), np.sin(angles)


def three_parts(x):
    high = x.astype(jnp.bfloat16)
    rest = x - high.astype(jnp.float32)
    middle = rest.astype(jnp.bfloat16)
    low = (rest - middle.astype(jnp.float32)).astype(jnp.bfloat16)
    return high, middle, low


def layer_kernel(
    n_sp,
    q_wide,
    kv_wide,
    tok_ref,
    lat_ref,
    wq_ref,
    wk_ref,
    wv_ref,
    wr_ref,
    wa_ref,
    shift_ref,
    rate_ref,
    gain_ref,
    qgain_ref,
    kvgain_ref,
    again_ref,
    rgain_ref,
    rcos_ref,
    rsin_ref,
    pcos_ref,
    psin_ref,
    qup_ref,
    kvup_ref,
    start_ref,
    out_ref,
    tok_all,
    w_all,
    shift_all,
    normed,
    acc,
    ret_q,
    ret_k,
    ret_v,
    lat_all,
    state,
    qn,
    qr,
    expanded,
    rope_key,
    kvup,
    qup,
    merged,
    own_sum,
    pair_out,
    pair_in,
    row_out,
    row_in,
    local_sem,
    z_send,
    z_recv,
    x_send,
    x_recv,
    y_send,
    y_recv,
    f_send,
    f_recv,
    m_send,
    m_recv,
    l_send,
    l_recv,
    l_relay,
    p_send,
    p_recv,
):
    z, f, t = lax.axis_index("sp"), lax.axis_index("fs"), lax.axis_index("tp")
    xn = f + 1 - 2 * (f % 2)
    yn = (f + 2) % 4
    other = 1 - t
    fs = 4
    rows = tok_ref.shape[0]
    length = n_sp * rows
    half = rows // 2
    weights = (lat_ref, wq_ref, wk_ref, wv_ref, wr_ref, wa_ref)
    f32, bf16 = jnp.float32, jnp.bfloat16
    lat_used = -(-(q_wide + kv_wide + 2 * ROPE_DIM) // WIDE)
    others = range(1, n_sp)

    def remote(src, dst, send, recv, **where):
        return pltpu.make_async_remote_copy(
            src_ref=src,
            dst_ref=dst,
            send_sem=send,
            recv_sem=recv,
            device_id={"sp": z, "fs": f, "tp": t, **where},
            device_id_type=MESH,
        )

    barrier = pltpu.get_barrier_semaphore()
    peers = [{"sp": (z + d) % n_sp, "fs": f, "tp": t} for d in others]
    peers += [{"sp": z, "fs": xn, "tp": t}, {"sp": z, "fs": yn, "tp": t}]
    peers += [{"sp": z, "fs": f, "tp": other}]
    for peer in peers:
        pl.semaphore_signal(barrier, inc=1, device_id=peer, device_id_type=MESH)
    with jax.named_scope("barrier"):
        pl.semaphore_wait(barrier, len(peers))

    def at(i, size=rows):
        if isinstance(i, int):
            return slice(i * size, (i + 1) * size)
        return pl.ds(pl.multiple_of(i * size, size), size)

    def owner(d):
        return (z + n_sp - d) % n_sp


    def piece(u, dest):
        return weights[u].at[:, at(dest, WIDE)]

    def part(owner_z, owner_f, u):
        return w_all.at[at(owner_z * fs + owner_f), u * WIDE : (u + 1) * WIDE]

    def has(u, place):
        return place < lat_used if u == LAT else True

    def when(condition, action):
        if condition is True:
            action()
        else:
            pl.when(condition)(action)

    def z_copy(d, u):
        to = (z + d) % n_sp
        return remote(piece(u, to), part(z, f, u), z_send.at[d, u], z_recv.at[d, u], sp=to)

    def x_copy(d, u):
        ref = part(owner(d), f, u)
        return remote(ref, ref, x_send.at[d, u], x_recv.at[d, u], fs=xn)

    def y_copy(d, u):
        ref = part(owner(d), f, u)
        return remote(ref, ref, y_send.at[d, u], y_recv.at[d, u], fs=yn)

    def f_copy(d, u):
        source, to = (xn, yn) if (d + u) % 2 == 0 else (yn, xn)
        ref = part(owner(d), source, u)
        return remote(ref, ref, f_send.at[d, u], f_recv.at[d, u], fs=to)

    def own_copy(u):
        return pltpu.make_async_copy(piece(u, z), part(z, f, u), local_sem.at[u])

    def on_relay_link(to):
        return ((z == 1) & (to == 0)) | ((z == n_sp - 2) & (to == n_sp - 1))

    def send(units, held):
        for u in units:
            for d in others:
                to = (z + d) % n_sp
                condition = on_relay_link(to) if held else ~on_relay_link(to)
                if u == LAT:
                    condition = condition & has(u, to)
                pl.when(condition)(lambda d=d, u=u: z_copy(d, u).start())

    def spread(d, u):
        def action():
            with jax.named_scope(f"spread#d={d}#u={u}"):
                if d == 0:
                    own_copy(u).wait()
                else:
                    z_copy(d, u).wait_recv()
            x_copy(d, u).start()
            y_copy(d, u).start()

        when(has(u, z), action)

    def relay(d, u):
        def action():
            with jax.named_scope(f"relay#d={d}#u={u}"):
                (x_copy if (d + u) % 2 == 0 else y_copy)(d, u).wait_recv()
            f_copy(d, u).start()

        when(has(u, z), action)

    def arrive(d, u):
        def action():
            with jax.named_scope(f"arrive#d={d}#u={u}"):
                (y_copy if (d + u) % 2 == 0 else x_copy)(d, u).wait_recv()
                f_copy(d, u).wait_recv()

        when(has(u, z), action)


    mine = pl.ds(pl.multiple_of(t * half, half), half)

    def tok_part(origin):
        return tok_all.at[origin, mine]

    lat_rows = length // LAT_PARTS

    def lat_part(i):
        return lambda origin: lat_all.at[t, origin, pl.ds(i * lat_rows, lat_rows)]

    def sends(row, origin):
        return True if row == 0 else origin < lat_used

    def both(condition, more):
        return condition if more is True else condition & more

    def line_copy(where, row, dest, src=None):
        return remote(
            where(z) if src is None else src,
            where(z),
            l_send.at[row, dest],
            l_recv.at[row, z],
            sp=dest,
        )

    def relay_copy(where, row, origin, dest):
        ref = where(origin)
        return remote(ref, ref, l_relay.at[row, origin], l_recv.at[row, origin], sp=dest)

    def pair_copy(where, row, origin):
        ref = where(origin)
        return remote(ref, ref, p_send.at[row, origin], p_recv.at[row, origin], tp=other)

    def direct(dest):
        near = (z - dest == 1) | (dest - z == 1)
        return near if dest in (0, n_sp - 1) else z != dest

    def line_start(where, row, src=None):
        for distance in others:
            for dest in range(n_sp):
                condition = direct(dest) & ((z - dest == distance) | (dest - z == distance))
                pl.when(both(condition, sends(row, z)))(
                    lambda dest=dest: line_copy(where, row, dest, src).start()
                )

    ends = ((1, 0), (n_sp - 2, n_sp - 1))

    def line_relay(where, row, distance):
        for middle, dest in ends:
            origin = middle + (middle - dest) * distance

            @pl.when(both(z == middle, sends(row, origin)))
            def _(origin=origin, dest=dest):
                with jax.named_scope(f"line#r={row}#k={distance}"):
                    relay_copy(where, row, origin, dest).wait_recv()
                relay_copy(where, row, origin, dest).start()

    def was_relayed(origin):
        return z == (n_sp - 2 if origin < n_sp // 2 else 1)

    def line_pair(where, row):
        for distance in others:
            for origin in range(n_sp):
                here = (z - origin == distance) | (origin - z == distance)

                @pl.when(both(here, sends(row, origin)))
                def _(origin=origin):
                    with jax.named_scope(f"pass#r={row}#k={distance}"):
                        pl.when(~was_relayed(origin))(
                            lambda: relay_copy(where, row, origin, 0).wait_recv()
                        )
                    pair_copy(where, row, origin).start()

    def pair_own(where, row):
        for origin in range(n_sp):
            pl.when(both(origin == z, sends(row, origin)))(
                lambda origin=origin: pair_copy(where, row, origin).start()
            )

    def pair_arrive(where, row, own):
        with jax.named_scope(f"pair#r={row}"):
            for origin in range(n_sp):
                condition = sends(row, origin) if own else both(origin != z, sends(row, origin))
                when(condition, lambda origin=origin: pair_copy(where, row, origin).wait_recv())

    def line_drain(where, row, own):
        for dest in range(n_sp):
            pl.when(both(direct(dest), sends(row, z)))(
                lambda dest=dest: line_copy(where, row, dest).wait_send()
            )
        for middle, dest in ends:
            for distance in range(1, n_sp - 1):
                origin = middle + (middle - dest) * distance
                pl.when(both(z == middle, sends(row, origin)))(
                    lambda origin=origin, dest=dest: relay_copy(
                        where, row, origin, dest
                    ).wait_send()
                )
        for origin in range(n_sp):
            condition = sends(row, origin) if own else both(origin != z, sends(row, origin))
            when(condition, lambda origin=origin: pair_copy(where, row, origin).wait_send())

    def shift_copy(d):
        to = (z + d) % n_sp
        return remote(shift_ref, shift_all.at[z], m_send.at[0, d], m_recv.at[0, d], sp=to)


    line_start(tok_part, 0, tok_ref.at[mine])
    for d in others:
        shift_copy(d).start()
    for u in range(UNITS):
        when(has(u, z), lambda u=u: own_copy(u).start())
    send((LAT,), True)
    send((LAT, QUERY, KEY, VALUE), False)
    own_tok = pltpu.make_async_copy(tok_ref, tok_all.at[z], local_sem.at[6])
    own_tok.start()
    own_shift = pltpu.make_async_copy(shift_ref, shift_all.at[z], local_sem.at[7])
    own_shift.start()
    att_wide = kvup.shape[1]
    own_kvup = pltpu.make_async_copy(kvup_ref.at[:, at(z, att_wide)], kvup, local_sem.at[8])
    own_kvup.start()
    up_wide = qup.shape[1]
    own_qup = pltpu.make_async_copy(qup_ref.at[:, at(z, up_wide)], qup, local_sem.at[10])
    own_qup.start()
    own_state = pltpu.make_async_copy(start_ref.at[z], state, local_sem.at[9])
    own_state.start()

    def norm_block(i):
        x = tok_all[i].astype(f32)
        scaled = x * lax.rsqrt(jnp.mean(x * x, axis=-1, keepdims=True) + EPSILON)
        normed[at(i), :] = (scaled * gain_ref[...]).astype(bf16)

    depth = fs * rows

    def multiply(u):
        with jax.named_scope(f"multiply#u={u}"):
            acc[...] = jnp.dot(
                normed[:, :depth],
                w_all[:depth, u * WIDE : (u + 1) * WIDE],
                preferred_element_type=f32,
            )

            def chunk(i, carry):
                begin = at(i, depth)
                acc[...] += jnp.dot(
                    normed[:, begin],
                    w_all[begin, u * WIDE : (u + 1) * WIDE],
                    preferred_element_type=f32,
                )
                return carry

            lax.fori_loop(1, n_sp, chunk, 0)

    rope_index = (q_wide + kv_wide) // WIDE
    rope_lane = (q_wide + kv_wide) % WIDE
    rd = RET_DIM // 2

    def finish_lat():
        def block(i, carry):
            raw = acc[at(i), :]
            pair = raw[:, rope_lane : rope_lane + 2 * ROPE_DIM]
            turned = pair * pcos_ref[at(i), :] + pltpu.roll(pair, ROPE_DIM, 1) * psin_ref[at(i), :]
            lane = lax.broadcasted_iota(jnp.int32, turned.shape, 1)
            turned = jnp.where(lane < ROPE_DIM, turned, pltpu.roll(turned, ROPE_DIM, 1))
            pieces = [raw[:, :rope_lane]] if rope_lane else []
            pieces.append(jnp.where(z == rope_index, turned, pair))
            if rope_lane + 2 * ROPE_DIM < WIDE:
                pieces.append(raw[:, rope_lane + 2 * ROPE_DIM :])
            lat_all[t, z, at(i), :] = jnp.concatenate(pieces, axis=1).astype(bf16)
            return carry

        lax.fori_loop(0, n_sp, block, 0)

    def finish_turned(dst, factor):
        def block(i, carry):
            cosine, sine = rcos_ref[at(i), :], rsin_ref[at(i), :]
            a, b = acc[at(i), :rd], acc[at(i), rd:]
            dst[at(i), :rd] = ((a * cosine - b * sine) * factor).astype(bf16)
            dst[at(i), rd:] = ((b * cosine + a * sine) * factor).astype(bf16)
            return carry

        lax.fori_loop(0, n_sp, block, 0)

    def project(u):
        for d in range(n_sp):
            arrive(d, u)
        multiply(u)
        if u == QUERY:
            finish_turned(ret_q, 1.0)
        elif u == KEY:
            finish_turned(ret_k, RET_DIM ** (-0.5))
        else:
            ret_v[...] = acc[...].astype(bf16)

    r_iota = lax.broadcasted_iota(jnp.int32, (rows, rows), 0)
    c_iota = lax.broadcasted_iota(jnp.int32, (rows, rows), 1)

    def retention(b):
        rates = shift_all[b]
        pick = lax.broadcasted_iota(jnp.int32, rates.shape, 0) == z
        chosen = lax.broadcasted_iota(jnp.int32, rate_ref.shape, 1) == z
        rate = jnp.sum(jnp.where(chosen, rate_ref[...], 0.0), axis=1, keepdims=True)
        row = jnp.sum(jnp.where(pick, rates, 0.0), axis=0, keepdims=True) + rate
        column = jnp.sum(jnp.where(r_iota == c_iota, row, 0.0), axis=1, keepdims=True)
        c_col = jnp.sum(jnp.where(c_iota <= r_iota, row, 0.0), axis=1, keepdims=True)
        c_row = jnp.sum(jnp.where(r_iota <= c_iota, column, 0.0), axis=0, keepdims=True)
        last = jnp.sum(row, axis=1, keepdims=True)
        decay = jnp.exp(jnp.where(c_iota <= r_iota, c_col - c_row, -jnp.inf))
        block = slice(b * rows, (b + 1) * rows)
        q, k, v = ret_q[block, :], ret_k[block, :], ret_v[block, :]
        scores = lax.dot_general(q, k, CONTRACT, preferred_element_type=f32) * decay
        raw = jnp.dot(scores.astype(bf16), v, preferred_element_type=f32)
        carried = sum(
            jnp.dot(q, s, preferred_element_type=f32) for s in three_parts(state[...])
        )
        raw = raw + carried * jnp.exp(c_col)
        if b < n_sp - 1:
            weighted = k.astype(f32) * jnp.exp(last - c_col)
            added = sum(
                lax.dot_general(w, v, (((0,), (0,)), ((), ())), preferred_element_type=f32)
                for w in three_parts(weighted)
            )
            state[...] = jnp.exp(last) * state[...] + added
        centered = raw - jnp.mean(raw, axis=-1, keepdims=True)
        variance = jnp.mean(centered * centered, axis=-1, keepdims=True)
        merged[block, :WIDE] = (centered * lax.rsqrt(variance + EPSILON) * rgain_ref[z]).astype(
            bf16
        )

    def chunks(first, count):
        found = []
        for core in range(2):
            for j in range(count // 128):
                lane = first + j * 128
                found.append((core, lane // WIDE, lane % WIDE))
        return found

    q_chunks, kv_chunks = chunks(0, q_wide), chunks(q_wide, kv_wide)
    rope_at = (rope_index, rope_lane)
    att_heads = att_wide // (NOPE_DIM + VAL_DIM)

    def expand(i):
        def latent(found, gain):
            x = jnp.concatenate(
                [lat_all[c, s, at(i), lane : lane + 128] for c, s, lane in found], axis=1
            ).astype(f32)
            scaled = x * lax.rsqrt(jnp.mean(x * x, axis=-1, keepdims=True) + EPSILON)
            return (scaled * gain[...]).astype(bf16)

        query = jnp.dot(latent(q_chunks, qgain_ref), qup[...], preferred_element_type=f32)
        first, middle, end = query[:, :128], query[:, 128:256], query[:, 256:]
        lane = lax.broadcasted_iota(jnp.int32, first.shape, 1)
        second = jnp.where(
            lane < ROPE_DIM, pltpu.roll(middle, ROPE_DIM, 1), pltpu.roll(end, ROPE_DIM, 1)
        )
        pair = jnp.where(lane < ROPE_DIM, middle, end)
        quarter = ROPE_DIM // 2
        swapped = jnp.where(
            lane % ROPE_DIM < quarter,
            pltpu.roll(pair, 2 * ROPE_DIM - quarter, 1),
            pltpu.roll(pair, quarter, 1),
        )
        qn[at(i), :NOPE_DIM] = first.astype(bf16)
        qn[at(i), NOPE_DIM:] = second.astype(bf16)
        qr[at(i), :] = (pair * pcos_ref[at(i), :] + swapped * psin_ref[at(i), :]).astype(bf16)
        expanded[at(i), :] = jnp.dot(
            latent(kv_chunks, kvgain_ref), kvup[...], preferred_element_type=f32
        ).astype(bf16)
        rope_key[at(i), :] = lat_all[0, rope_at[0], at(i), rope_at[1] : rope_at[1] + 128]

    scale = (NOPE_DIM + ROPE_DIM) ** (-0.5)

    def attend(b):
        seen = (b + 1) * rows
        block = slice(b * rows, seen)
        q_at = lax.broadcasted_iota(jnp.int32, (rows, seen), 0) + b * rows
        k_at = lax.broadcasted_iota(jnp.int32, (rows, seen), 1)
        for h in range(att_heads):
            base = h * (NOPE_DIM + VAL_DIM)
            turned = qr[block, :]
            lane = lax.broadcasted_iota(jnp.int32, turned.shape, 1)
            turned = jnp.where(lane // ROPE_DIM == h, turned, jnp.zeros_like(turned))
            s = lax.dot_general(
                qn[block, h * NOPE_DIM : (h + 1) * NOPE_DIM],
                expanded[:seen, base : base + NOPE_DIM],
                CONTRACT,
                preferred_element_type=f32,
            ) + lax.dot_general(
                turned, rope_key[:seen, :], CONTRACT, preferred_element_type=f32
            )
            s = jnp.where(k_at <= q_at, s * scale, -jnp.inf)
            p = jnp.exp(s - jnp.max(s, axis=-1, keepdims=True))
            raw = jnp.dot(
                p.astype(bf16),
                expanded[:seen, base + NOPE_DIM : base + NOPE_DIM + VAL_DIM],
                preferred_element_type=f32,
            ) / jnp.sum(p, axis=-1, keepdims=True)
            scaled = raw * lax.rsqrt(jnp.mean(raw * raw, axis=-1, keepdims=True) + EPSILON)
            gain = again_ref[z][:, h * VAL_DIM : (h + 1) * VAL_DIM]
            merged[block, WIDE + h * VAL_DIM : WIDE + (h + 1) * VAL_DIM] = (
                scaled * gain
            ).astype(bf16)

    def out_copy(b):
        return remote(pair_out.at[b], pair_in.at[b], m_send.at[1, b], m_recv.at[1, b], tp=other)

    def row_copy(b, origin):
        return remote(row_out.at[b], row_in.at[origin], m_send.at[2, b], m_recv.at[2, origin], sp=b)

    def project_out(b):
        got = lax.dot_general(
            merged[at(b), :],
            w_all[:, OUT_RET * WIDE :],
            CONTRACT,
            preferred_element_type=f32,
        )
        front, back = got[:half, :], got[half:, :]
        pair_out[b] = jnp.where(t == 0, back, front).astype(bf16)
        out_copy(b).start()
        own_sum[b] = jnp.where(t == 0, front, back)

    def send_rows(b):
        with jax.named_scope("rows_pair"):
            out_copy(b).wait_recv()
        total = own_sum[b] + pair_in[b].astype(f32)
        own_sum[b] = total

        @pl.when(z != b)
        def _():
            row_out[b] = total.astype(bf16)
            row_copy(b, z).start()


    for u in range(UNITS):
        spread(0, u)
    own_tok.wait()
    norm_block(z)
    for u in range(3):
        relay(0, u)
    line_relay(tok_part, 0, 1)
    send((QUERY,), True)
    for u in range(3, UNITS):
        relay(0, u)
    line_relay(tok_part, 0, 2)
    send((KEY, VALUE), True)
    for d in others:
        spread(d, LAT)
    for d in others:
        relay(d, LAT)
    line_pair(tok_part, 0)
    for d in others:
        spread(d, QUERY)
    pair_arrive(tok_part, 0, False)
    for d in others:
        norm_block(owner(d))
    for d in range(n_sp):
        arrive(d, LAT)

    @pl.when(has(LAT, z))
    def _():
        multiply(LAT)
        finish_lat()

    for i in range(LAT_PARTS):
        line_start(lat_part(i), i + 1)
    for i in range(LAT_PARTS):
        pair_own(lat_part(i), i + 1)
    send((OUT_RET, OUT_ATT), False)
    for d in others:
        relay(d, QUERY)
    for d in others:
        spread(d, KEY)
    project(QUERY)
    for d in others:
        relay(d, KEY)
    for d in others:
        spread(d, VALUE)
    project(KEY)
    for d in others:
        relay(d, VALUE)
    for distance in range(1, n_sp - 1):
        for i in range(LAT_PARTS):
            line_relay(lat_part(i), i + 1, distance)
    send((OUT_RET, OUT_ATT), True)
    project(VALUE)
    for d in others:
        shift_copy(d).wait_recv()
    own_shift.wait()
    own_state.wait()
    own_kvup.wait()
    own_qup.wait()
    for b in range(n_sp):
        with jax.named_scope(f"retention#b={b}"):
            retention(b)
    for i in range(LAT_PARTS):
        line_pair(lat_part(i), i + 1)
    for i in range(LAT_PARTS):
        pair_arrive(lat_part(i), i + 1, True)
    for i in range(n_sp):
        with jax.named_scope(f"expand#b={i}"):
            expand(i)
    for d in others:
        spread(d, OUT_RET)
    for b in range(n_sp // 2):
        attend(b)
    for d in others:
        relay(d, OUT_RET)
    for b in range(n_sp // 2, n_sp):
        attend(b)
    for d in others:
        spread(d, OUT_ATT)
    for d in others:
        relay(d, OUT_ATT)
    for u in (OUT_RET, OUT_ATT):
        for d in range(n_sp):
            arrive(d, u)
    upper = z // (n_sp // 2)
    order = (3 - 3 * upper, 2 - upper, z + 1 - 2 * (z % 2), z)
    for step, b in enumerate(order):
        with jax.named_scope(f"out#b={step}"):
            project_out(b)
        if step:
            send_rows(order[step - 1])
    send_rows(order[-1])
    total = own_sum[z]
    for d in others:
        with jax.named_scope(f"rows#d={d}"):
            row_copy(0, owner(d)).wait_recv()
        total = total + row_in[owner(d)].astype(f32)
    out_ref[...] = total.astype(bf16)

    for u in range(UNITS):
        for d in range(n_sp):

            def drain(d=d, u=u):
                x_copy(d, u).wait_send()
                y_copy(d, u).wait_send()
                f_copy(d, u).wait_send()

            when(has(u, z), drain)
            if d:
                to = (z + d) % n_sp
                when(has(u, to), lambda d=d, u=u: z_copy(d, u).wait_send())
    for d in others:
        shift_copy(d).wait_send()
    line_drain(tok_part, 0, False)
    for i in range(LAT_PARTS):
        line_drain(lat_part(i), i + 1, True)
    for b in range(n_sp):
        out_copy(b).wait_send()
        pl.when(z != b)(lambda b=b: row_copy(b, z).wait_send())


def heads_plan(
    tokens,
    norm_gain,
    w_ret_query,
    w_ret_key,
    w_ret_value,
    w_q_down,
    w_kv_down,
    w_rope_key,
    w_q_up,
    w_kv_up,
    q_lat_gain,
    kv_lat_gain,
    att_norm_gain,
    ret_norm_gain,
    w_ret_out,
    w_att_out,
    head_rate,
    decay_shift,
    start_state,
):
    n_sp = lax.axis_size("sp")
    rows, width = tokens.shape[1:]
    length = n_sp * rows
    q_wide, kv_wide = w_q_down.shape[1], w_kv_down.shape[1]
    rope_half = ROPE_DIM // 2
    w_rows = w_q_down.shape[0]
    att_heads = w_q_up.shape[1] // (NOPE_DIM + ROPE_DIM) // n_sp

    def swap(x):
        return jnp.concatenate([x[..., rope_half:], x[..., :rope_half]], axis=-1)

    lat = jnp.concatenate([w_q_down, w_kv_down, w_rope_key, swap(w_rope_key)], axis=1)
    lat = jnp.pad(lat, ((0, 0), (0, n_sp * WIDE - lat.shape[1])))
    ret_cos, ret_sin = wave_tables(length, RET_DIM)
    rope_cos, rope_sin = wave_tables(length, ROPE_DIM)
    pair_cos = np.concatenate([rope_cos] * 4, axis=1)
    pair_sin = np.concatenate([-rope_sin, rope_sin] * 2, axis=1)
    dma = pltpu.SemaphoreType.DMA
    vmem = pltpu.VMEM
    f32, bf16 = jnp.float32, jnp.bfloat16
    half = rows // 2
    out_wide = 4 * n_sp * w_rows
    any_spec = pl.BlockSpec(memory_space=pl.ANY)
    vmem_spec = pl.BlockSpec(memory_space=pltpu.VMEM)
    mixed = pl.pallas_call(
        functools.partial(layer_kernel, n_sp, q_wide, kv_wide),
        out_shape=jax.ShapeDtypeStruct((half, out_wide), bf16),
        in_specs=[any_spec] * 8 + [vmem_spec] * 10 + [any_spec] * 3,
        out_specs=vmem_spec,
        scratch_shapes=[
            vmem((n_sp, rows, width), bf16),
            vmem((n_sp * 4 * w_rows, 6 * WIDE), bf16),
            vmem((n_sp,) + decay_shift.shape[1:], f32),
            vmem((length, width), bf16),
            vmem((length, WIDE), f32),
            vmem((length, WIDE), bf16),
            vmem((length, WIDE), bf16),
            vmem((length, WIDE), bf16),
            vmem((2, n_sp, length, WIDE), bf16),
            vmem((RET_DIM, RET_DIM), f32),
            vmem((length, att_heads * NOPE_DIM), bf16),
            vmem((length, att_heads * ROPE_DIM), bf16),
            vmem((length, att_heads * (NOPE_DIM + VAL_DIM)), bf16),
            vmem((length, 2 * ROPE_DIM), bf16),
            vmem((w_kv_up.shape[0], att_heads * (NOPE_DIM + VAL_DIM)), bf16),
            vmem((w_q_up.shape[0], att_heads * (NOPE_DIM + ROPE_DIM)), bf16),
            vmem((length, WIDE + att_heads * VAL_DIM), bf16),
            vmem((n_sp, half, out_wide), f32),
            vmem((n_sp, half, out_wide), bf16),
            vmem((n_sp, half, out_wide), bf16),
            vmem((n_sp, half, out_wide), bf16),
            vmem((n_sp, half, out_wide), bf16),
            dma((11,)),
            *[dma((n_sp, UNITS))] * 8,
            *[dma((3, n_sp))] * 2,
            *[dma((LAT_PARTS + 1, n_sp))] * 5,
        ],
        compiler_params=pltpu.CompilerParams(
            collective_id=0, has_side_effects=True, vmem_limit_bytes=62 * 1024 * 1024
        ),
    )(
        tokens[0],
        lat,
        w_ret_query,
        w_ret_key,
        w_ret_value,
        w_ret_out,
        w_att_out,
        decay_shift[0],
        head_rate[None],
        norm_gain[None],
        q_lat_gain[None],
        kv_lat_gain[None],
        att_norm_gain.reshape(n_sp, 1, -1),
        ret_norm_gain.reshape(n_sp, 1, -1),
        ret_cos,
        ret_sin,
        pair_cos,
        pair_sin,
        w_q_up,
        w_kv_up,
        start_state[0],
    )
    return mixed[None]


def solution(mesh):
    placed = (
        P("fs", "sp", None),
        P(),
        P(("sp", "fs"), "tp"),
        P(("sp", "fs"), "tp"),
        P(("sp", "fs"), "tp"),
        P(("sp", "fs"), "tp"),
        P(("sp", "fs"), "tp"),
        P(("sp", "fs"), None),
        P(None, "tp"),
        P(None, "tp"),
        P(),
        P(),
        P("tp"),
        P("tp"),
        P(("sp", "fs"), "tp"),
        P(("sp", "fs"), "tp"),
        P("tp"),
        P("fs", "tp", "sp"),
        P("fs", "tp", None, None),
    )

    def pick(*args):
        if heads_fit(
            mesh, args[16].shape[0], args[0].shape[0], args[5].shape[1], args[6].shape[1], args[8].shape[1]
        ):
            return heads_plan(*args)
        return rows_plan(*args)

    return jax.shard_map(
        pick,
        mesh=mesh,
        in_specs=placed,
        out_specs=P("fs", ("sp", "tp"), None),
        check_vma=False,
    )
```

```python
import functools

import numpy as np

import jax
import jax.numpy as jnp
from jax import lax
from jax.experimental import pallas as pl
from jax.experimental.pallas import tpu as pltpu
from jax.sharding import PartitionSpec as P

RET_DIM = 256
NOPE_DIM = 128
ROPE_DIM = 64
VAL_DIM = 128
KV_LAT = 512


EPSILON = 1e-06
THETA_BASE = 10000.0
TOP_PRECISION = lax.Precision.HIGHEST


def prefix(x, axis, combine, identity):
    peers, position = (lax.axis_size(axis), lax.axis_index(axis))
    everything = jax.tree.map(
        lambda part, kind: lax.all_gather(part.astype(kind), axis), x, (jnp.bfloat16, jnp.bfloat16)
    )
    start = jax.tree.map(
        lambda part, zero: jnp.broadcast_to(jnp.asarray(zero, part.dtype), part.shape), x, identity
    )

    def lap(k, before):
        reached = k < position
        new = combine(
            before, jax.tree.map(lambda part, own: part[k].astype(own.dtype), everything, x)
        )
        return jax.tree.map(lambda a, b: jnp.where(reached, a, b), new, before)

    return lax.fori_loop(0, peers, lap, start)


def angle_tables(positions, rot_width):
    half_width = rot_width // 2
    inverse = THETA_BASE ** (-jnp.arange(half_width, dtype=jnp.float32) * 2.0 / rot_width)
    angles = positions.astype(jnp.float32)[:, None] * inverse[None, :]
    return (jnp.cos(angles), jnp.sin(angles))


def rotate(values, cosine, sine):
    half_width = values.shape[-1] // 2
    front_half = values[..., :half_width]
    back_half = values[..., half_width:]
    return jnp.concatenate(
        [front_half * cosine - back_half * sine, back_half * cosine + front_half * sine], axis=-1
    )


def rms_scale(values, gain_vector):
    return (
        values
        * lax.rsqrt(jnp.mean(values * values, axis=-1, keepdims=True) + EPSILON)
        * gain_vector
    )


def chain_states(earlier, later):
    early_log, early_state = earlier
    late_log, late_state = later
    return (early_log + late_log, jnp.exp(late_log)[:, None, None] * early_state + late_state)


def rows_plan(
    tokens,
    norm_gain,
    w_ret_query,
    w_ret_key,
    w_ret_value,
    w_q_down,
    w_kv_down,
    w_rope_key,
    w_q_up,
    w_kv_up,
    q_lat_gain,
    kv_lat_gain,
    att_norm_gain,
    ret_norm_gain,
    w_ret_out,
    w_att_out,
    head_rate,
    decay_shift,
    start_state,
):
    tok_rows = tokens.shape[1]
    ret_local = head_rate.shape[0]
    att_local = w_q_up.shape[1] // (NOPE_DIM + ROPE_DIM)
    row_offset = lax.axis_index("sp") * tok_rows
    positions = row_offset + jnp.arange(tok_rows, dtype=jnp.int32)
    (
        full_query,
        full_key,
        full_value,
        full_q_down,
        full_kv_down,
        full_rope,
        full_ret_out,
        full_att_out,
    ) = (
        lax.all_gather(w_ret_query, ("sp", "fs"), axis=0, tiled=True),
        lax.all_gather(w_ret_key, ("sp", "fs"), axis=0, tiled=True),
        lax.all_gather(w_ret_value, ("sp", "fs"), axis=0, tiled=True),
        lax.all_gather(w_q_down, ("sp", "fs"), axis=0, tiled=True),
        lax.all_gather(w_kv_down, ("sp", "fs"), axis=0, tiled=True),
        lax.all_gather(w_rope_key, ("sp", "fs"), axis=0, tiled=True),
        lax.all_gather(w_ret_out, ("sp", "fs"), axis=0, tiled=True),
        lax.all_gather(w_att_out, ("sp", "fs"), axis=0, tiled=True),
    )
    source = tokens[0].astype(jnp.float32)
    normed = rms_scale(source, norm_gain).astype(jnp.bfloat16)
    ret_cos, ret_sin = angle_tables(positions, RET_DIM)
    rope_cos, rope_sin = angle_tables(positions, ROPE_DIM)

    def project(weight):
        return jnp.dot(normed, weight, preferred_element_type=jnp.float32)

    part_q = project(full_q_down).astype(jnp.bfloat16)
    part_kv = project(full_kv_down).astype(jnp.bfloat16)
    lat_q_raw, lat_kv_raw = (
        lax.all_gather(part_q, "tp", axis=1, tiled=True),
        lax.all_gather(part_kv, "tp", axis=1, tiled=True),
    )
    retention_query = rotate(
        project(full_query).reshape(tok_rows, ret_local, RET_DIM),
        ret_cos[:, None],
        ret_sin[:, None],
    ).astype(jnp.bfloat16)
    retention_key = (
        rotate(
            project(full_key).reshape(tok_rows, ret_local, RET_DIM),
            ret_cos[:, None],
            ret_sin[:, None],
        )
        * RET_DIM ** (-0.5)
    ).astype(jnp.bfloat16)
    retention_value = project(full_value).reshape(tok_rows, ret_local, RET_DIM).astype(jnp.bfloat16)
    rope_key = rotate(project(full_rope), rope_cos, rope_sin).astype(jnp.bfloat16)
    log_rates = head_rate[:, None] + decay_shift[0]
    cumul = jnp.cumsum(log_rates, axis=1)
    offsets = jnp.arange(tok_rows, dtype=jnp.int32)
    lower_mask = offsets[None, :] <= offsets[:, None]
    decay_matrix = jnp.exp(
        jnp.where(lower_mask[None], cumul[:, :, None] - cumul[:, None, :], -jnp.inf)
    )
    block_score_grid = (
        jnp.einsum(
            "zgq,ugq->gzu", retention_query, retention_key, preferred_element_type=jnp.float32
        )
        * decay_matrix
    ).astype(jnp.bfloat16)
    inside_block_output = jnp.einsum(
        "vzs,svp->zvp", block_score_grid, retention_value, preferred_element_type=jnp.float32
    )
    block_output_sum = cumul[:, -1]
    weighted_values = (
        retention_key.astype(jnp.float32) * jnp.exp(block_output_sum[:, None] - cumul).T[:, :, None]
    )
    contribution = jnp.einsum(
        "uzj,uzv->zjv",
        weighted_values,
        retention_value.astype(jnp.float32),
        precision=TOP_PRECISION,
    )
    identity = (jnp.zeros_like(block_output_sum), jnp.zeros_like(contribution))
    before_log, before_state = prefix(
        (block_output_sum, contribution), "sp", chain_states, identity
    )
    q_latent = rms_scale(lat_q_raw.astype(jnp.float32), q_lat_gain).astype(jnp.bfloat16)
    kv_latent = rms_scale(lat_kv_raw.astype(jnp.float32), kv_lat_gain).astype(jnp.bfloat16)
    query_full = jnp.dot(q_latent, w_q_up, preferred_element_type=jnp.float32).reshape(
        tok_rows, att_local, NOPE_DIM + ROPE_DIM
    )
    query_nope = query_full[..., :NOPE_DIM].astype(jnp.bfloat16)
    query_rope = rotate(query_full[..., NOPE_DIM:], rope_cos[:, None], rope_sin[:, None]).astype(
        jnp.bfloat16
    )
    att_scale = (NOPE_DIM + ROPE_DIM) ** (-0.5)

    def attend(carry, key_nope, key_values, key_rope, start):
        running_max, running_sum, running_acc = carry
        key_count = key_rope.shape[0]
        score_matrix = (
            jnp.einsum("qhd,khd->hqk", query_nope, key_nope, preferred_element_type=jnp.float32)
            + jnp.einsum("qhd,kd->hqk", query_rope, key_rope, preferred_element_type=jnp.float32)
        ) * att_scale
        key_positions = start + jnp.arange(key_count, dtype=jnp.int32)
        allowed = key_positions[None, :] <= positions[:, None]
        masked = jnp.where(allowed[None], score_matrix, -jnp.inf)
        new_max = jnp.maximum(running_max, jnp.max(masked, axis=-1))
        safe_max = jnp.where(jnp.isfinite(new_max), new_max, 0.0)
        weights = jnp.exp(masked - safe_max[..., None])
        rescale = jnp.exp(running_max - safe_max)
        new_sum = running_sum * rescale + jnp.sum(weights, axis=-1)
        new_acc = running_acc * rescale[..., None] + jnp.einsum(
            "hqk,khd->hqd",
            weights.astype(jnp.bfloat16),
            key_values,
            preferred_element_type=jnp.float32,
        )
        return (new_max, new_sum, new_acc)

    def expand_attend(carry_in, lat_piece, rope_piece, start):
        wide = (
            jnp.dot(lat_piece, w_kv_up, preferred_element_type=jnp.float32)
            .astype(jnp.bfloat16)
            .reshape(rope_piece.shape[0], att_local, NOPE_DIM + VAL_DIM)
        )
        return attend(carry_in, wide[..., :NOPE_DIM], wide[..., NOPE_DIM:], rope_piece, start)

    empty = (
        jnp.full((att_local, tok_rows), -jnp.inf, jnp.float32),
        jnp.zeros((att_local, tok_rows), jnp.float32),
        jnp.zeros((att_local, tok_rows, VAL_DIM), jnp.float32),
    )
    groups = lax.axis_size("tp")
    kv_part = KV_LAT // groups
    rope_part = ROPE_DIM // groups
    my_group = lax.axis_index("tp")
    joined = jnp.concatenate(
        [
            lax.dynamic_slice_in_dim(kv_latent, my_group * kv_part, kv_part, 1),
            lax.dynamic_slice_in_dim(rope_key, my_group * rope_part, rope_part, 1),
        ],
        axis=1,
    )
    all_rows = lax.all_gather(joined, "sp", axis=0, tiled=True)
    complete = lax.all_gather(all_rows, "tp", axis=1, tiled=True)
    total_rows = complete.shape[0]
    grouped = complete.reshape(total_rows, groups, kv_part + rope_part)
    lat_all = grouped[:, :, :kv_part].reshape(total_rows, KV_LAT)
    rope_all = grouped[:, :, kv_part:].reshape(total_rows, ROPE_DIM)

    def visit(block_index, carry_in):
        start = block_index * tok_rows
        lat_piece = lax.dynamic_slice_in_dim(lat_all, start, tok_rows, 0)
        rope_piece = lax.dynamic_slice_in_dim(rope_all, start, tok_rows, 0)
        return expand_attend(carry_in, lat_piece, rope_piece, start)

    final = lax.fori_loop(0, lax.axis_index("sp") + 1, visit, empty)
    att_raw = jnp.transpose(final[2] / final[1][..., None], (1, 0, 2))
    att_out = (
        rms_scale(att_raw, att_norm_gain.reshape(att_local, VAL_DIM))
        .astype(jnp.bfloat16)
        .reshape(tok_rows, att_local * VAL_DIM)
    )
    entering = jnp.exp(before_log)[:, None, None] * start_state[0] + before_state
    carried_term = (
        jnp.einsum(
            "nhd,hde->nhe", retention_query.astype(jnp.float32), entering, precision=TOP_PRECISION
        )
        * jnp.exp(cumul).T[:, :, None]
    )
    ret_raw = inside_block_output + carried_term
    row_mean = jnp.mean(ret_raw, axis=-1, keepdims=True)
    centered = ret_raw - row_mean
    row_var = jnp.mean(centered * centered, axis=-1, keepdims=True)
    ret_out = (
        (centered * lax.rsqrt(row_var + EPSILON) * ret_norm_gain.reshape(ret_local, RET_DIM))
        .astype(jnp.bfloat16)
        .reshape(tok_rows, ret_local * RET_DIM)
    )
    contract = (((1,), (1,)), ((), ()))
    mixed = lax.psum_scatter(
        (
            lax.dot_general(ret_out, full_ret_out, contract, preferred_element_type=jnp.float32)
            + lax.dot_general(att_out, full_att_out, contract, preferred_element_type=jnp.float32)
        ).astype(jnp.bfloat16),
        "tp",
        scatter_dimension=0,
        tiled=True,
    )
    return mixed[None]


MESH = pl.DeviceIdType.MESH
WIDE = RET_DIM
CONTRACT = (((1,), (1,)), ((), ()))
UNITS = 6
LAT, QUERY, KEY, VALUE, OUT_RET, OUT_ATT = range(UNITS)
LAT_PARTS = 2


def heads_fit(mesh, ret_local, sequences, q_wide, kv_wide, up_wide):
    sizes = mesh.shape
    return (
        sizes["sp"] == 4
        and sizes["fs"] == 4
        and sizes["tp"] == 2
        and ret_local == sizes["sp"]
        and sequences == 1
        and up_wide == 2 * (NOPE_DIM + ROPE_DIM) * ret_local
        and q_wide % 128 == 0
        and kv_wide % 128 == 0
        and q_wide == kv_wide + 2 * ROPE_DIM
    )


def wave_tables(length, wide):
    half_wide = wide // 2
    powers = np.arange(half_wide, dtype=np.float32) * np.float32(2.0 / wide)
    inverse = np.power(np.float32(THETA_BASE), -powers).astype(np.float32)
    angles = np.arange(length, dtype=np.float32)[:, None] * inverse[None, :]
    return np.cos(angles), np.sin(angles)


def three_parts(x):
    high = x.astype(jnp.bfloat16)
    rest = x - high.astype(jnp.float32)
    middle = rest.astype(jnp.bfloat16)
    low = (rest - middle.astype(jnp.float32)).astype(jnp.bfloat16)
    return high, middle, low


def layer_kernel(
    n_sp,
    q_wide,
    kv_wide,
    tok_ref,
    wqd_ref,
    wkvd_ref,
    wq_ref,
    wk_ref,
    wv_ref,
    wr_ref,
    wa_ref,
    rope_ref,
    shift_ref,
    rate_ref,
    gain_ref,
    qgain_ref,
    kvgain_ref,
    again_ref,
    rgain_ref,
    rcos_ref,
    rsin_ref,
    pcos_ref,
    psin_ref,
    qup_ref,
    kvup_ref,
    start_ref,
    out_ref,
    tok_all,
    w_all,
    w_lat,
    kv_src,
    shift_all,
    normed,
    acc_ret,
    acc_lat,
    ret_q,
    ret_k,
    ret_v,
    lat_all,
    state,
    qn,
    qr,
    expanded,
    rope_key,
    kvup,
    qup,
    merged,
    own_sum,
    pair_out,
    pair_in,
    row_out,
    row_in,
    local_sem,
    z_send,
    z_recv,
    x_send,
    x_recv,
    y_send,
    y_recv,
    f_send,
    f_recv,
    m_send,
    m_recv,
    l_send,
    l_recv,
    l_relay,
    p_send,
    p_recv,
):
    z, f, t = lax.axis_index("sp"), lax.axis_index("fs"), lax.axis_index("tp")
    xn = f + 1 - 2 * (f % 2)
    yn = (f + 2) % 4
    other = 1 - t
    fs = 4
    rows = tok_ref.shape[0]
    length = n_sp * rows
    half = rows // 2
    weights = (None, wq_ref, wk_ref, wv_ref, wr_ref, wa_ref)
    f32, bf16 = jnp.float32, jnp.bfloat16
    q_place, kv_place = n_sp // 2 - 1, n_sp // 2
    others = range(1, n_sp)

    def remote(src, dst, send, recv, **where):
        return pltpu.make_async_remote_copy(
            src_ref=src,
            dst_ref=dst,
            send_sem=send,
            recv_sem=recv,
            device_id={"sp": z, "fs": f, "tp": t, **where},
            device_id_type=MESH,
        )

    barrier = pltpu.get_barrier_semaphore()
    peers = [{"sp": (z + d) % n_sp, "fs": f, "tp": t} for d in others]
    peers += [{"sp": z, "fs": xn, "tp": t}, {"sp": z, "fs": yn, "tp": t}]
    peers += [{"sp": z, "fs": f, "tp": other}]
    for peer in peers:
        pl.semaphore_signal(barrier, inc=1, device_id=peer, device_id_type=MESH)
    with jax.named_scope("barrier"):
        pl.semaphore_wait(barrier, len(peers))

    def at(i, size=rows):
        if isinstance(i, int):
            return slice(i * size, (i + 1) * size)
        return pl.ds(pl.multiple_of(i * size, size), size)

    upper = z // (n_sp // 2)
    is_end = (z == 0) | (z == n_sp - 1)

    def origin_of(k):
        depth_in = z + upper * (n_sp - 1 - 2 * z)
        found = (depth_in * 0, 1 + depth_in, 2 - 2 * depth_in, depth_in * 0 + 3)[k]
        return z if k == 0 else found + upper * (n_sp - 1 - 2 * found)


    def piece(u, dest):
        return weights[u].at[:, at(dest, WIDE)]

    def part(owner_z, owner_f, u):
        where = at(owner_z * fs + owner_f)
        if u == LAT:
            return w_lat.at[where]
        return w_all.at[where, (u - 1) * WIDE : u * WIDE]

    def has(u, place):
        return (place == q_place) | (place == kv_place) if u == LAT else True

    def when(condition, action):
        if condition is True:
            action()
        else:
            pl.when(condition)(action)

    lat_sources = {q_place: wqd_ref, kv_place: kv_src}

    def z_copy(to, u, src=None):
        return remote(
            piece(u, to) if src is None else src,
            part(z, f, u),
            z_send.at[to, u],
            z_recv.at[z, u],
            sp=to,
        )

    def z_arrival(k, u):
        ref = part(origin_of(k), f, u)
        return remote(ref, ref, z_send.at[z, u], z_recv.at[origin_of(k), u], tp=other)

    def x_copy(k, u):
        ref = part(origin_of(k), f, u)
        return remote(ref, ref, x_send.at[k, u], x_recv.at[k, u], fs=xn)

    def y_copy(k, u):
        ref = part(origin_of(k), f, u)
        return remote(ref, ref, y_send.at[k, u], y_recv.at[k, u], fs=yn)

    def f_copy(k, u):
        source, to = (xn, yn) if (k + u) % 2 == 0 else (yn, xn)
        ref = part(origin_of(k), source, u)
        return remote(ref, ref, f_send.at[k, u], f_recv.at[k, u], fs=to)

    def own_copy(u):
        return pltpu.make_async_copy(piece(u, z), part(z, f, u), local_sem.at[u])

    def own_lat_copy(place):
        return pltpu.make_async_copy(lat_sources[place], part(z, f, LAT), local_sem.at[LAT])

    def send(u):
        for k in others:
            z_copy(origin_of(k), u).start()

    def send_lat(place):
        pl.when(z != place)(lambda: z_copy(place, LAT, lat_sources[place]).start())

    def spread(d, u):
        def action():
            with jax.named_scope(f"spread#d={d}#u={u}"):
                if d:
                    z_arrival(d, u).wait_recv()
                elif u == LAT:
                    own_lat_copy(q_place).wait()
                else:
                    own_copy(u).wait()
            x_copy(d, u).start()
            y_copy(d, u).start()

        when(has(u, z), action)

    def relay(d, u):
        def action():
            with jax.named_scope(f"relay#d={d}#u={u}"):
                (x_copy if (d + u) % 2 == 0 else y_copy)(d, u).wait_recv()
            f_copy(d, u).start()

        when(has(u, z), action)

    def arrive(d, u):
        def action():
            with jax.named_scope(f"arrive#d={d}#u={u}"):
                (y_copy if (d + u) % 2 == 0 else x_copy)(d, u).wait_recv()
                f_copy(d, u).wait_recv()

        when(has(u, z), action)


    mine = pl.ds(pl.multiple_of(t * half, half), half)

    def tok_part(origin):
        return tok_all.at[origin, mine]

    lat_rows = length // LAT_PARTS

    def lat_part(i):
        return lambda origin: lat_all.at[t, origin - q_place, pl.ds(i * lat_rows, lat_rows)]

    def sends(row, origin):
        return True if row == 0 else has(LAT, origin)

    def both(condition, more):
        return condition if more is True else condition & more

    def steps(row):
        return range(1, n_sp - 1 if row == 0 else 2)

    def line_copy(where, row, dest, src=None):
        return remote(
            where(z) if src is None else src,
            where(z),
            l_send.at[row, dest],
            l_recv.at[row, z],
            sp=dest,
        )

    def relay_copy(where, row, origin, dest):
        ref = where(origin)
        return remote(ref, ref, l_relay.at[row, origin], l_recv.at[row, origin], sp=dest)

    def pair_copy(where, row, origin):
        ref = where(origin)
        return remote(ref, ref, p_send.at[row, origin], p_recv.at[row, origin], tp=other)

    def direct(dest):
        near = (z - dest == 1) | (dest - z == 1)
        return near if dest in (0, n_sp - 1) else z != dest

    def line_start(where, row, src=None, distances=others):
        for distance in distances:
            for dest in range(n_sp):
                condition = direct(dest) & ((z - dest == distance) | (dest - z == distance))
                pl.when(both(condition, sends(row, z)))(
                    lambda dest=dest: line_copy(where, row, dest, src).start()
                )

    ends = ((1, 0), (n_sp - 2, n_sp - 1))

    def line_relay(where, row, distance):
        for middle, dest in ends:
            origin = middle + (middle - dest) * distance

            @pl.when(both(z == middle, sends(row, origin)))
            def _(origin=origin, dest=dest):
                with jax.named_scope(f"line#r={row}#k={distance}"):
                    relay_copy(where, row, origin, dest).wait_recv()
                relay_copy(where, row, origin, dest).start()

    def was_relayed(origin):
        return z == (n_sp - 2 if origin < n_sp // 2 else 1)

    def line_pair(where, row):
        for distance in others:
            for origin in range(n_sp):
                here = (z - origin == distance) | (origin - z == distance)

                @pl.when(both(here, sends(row, origin)))
                def _(origin=origin):
                    with jax.named_scope(f"pass#r={row}#k={distance}"):
                        pl.when(~was_relayed(origin))(
                            lambda: relay_copy(where, row, origin, 0).wait_recv()
                        )
                    pair_copy(where, row, origin).start()

    def pair_own(where, row):
        for origin in range(n_sp):
            pl.when(both(origin == z, sends(row, origin)))(
                lambda origin=origin: pair_copy(where, row, origin).start()
            )

    def pair_arrive(where, row, own):
        with jax.named_scope(f"pair#r={row}"):
            for origin in range(n_sp):
                condition = sends(row, origin) if own else both(origin != z, sends(row, origin))
                when(condition, lambda origin=origin: pair_copy(where, row, origin).wait_recv())

    def line_drain(where, row, own):
        for dest in range(n_sp):
            pl.when(both(direct(dest), sends(row, z)))(
                lambda dest=dest: line_copy(where, row, dest).wait_send()
            )
        for middle, dest in ends:
            for distance in steps(row):
                origin = middle + (middle - dest) * distance
                pl.when(both(z == middle, sends(row, origin)))(
                    lambda origin=origin, dest=dest: relay_copy(
                        where, row, origin, dest
                    ).wait_send()
                )
        for origin in range(n_sp):
            condition = sends(row, origin) if own else both(origin != z, sends(row, origin))
            when(condition, lambda origin=origin: pair_copy(where, row, origin).wait_send())

    def shift_copy(d):
        to = (z + d) % n_sp
        return remote(shift_ref, shift_all.at[z], m_send.at[0, d], m_recv.at[0, d], sp=to)


    def start_inputs():
        own_tok.start()
        own_shift.start()
        own_kvup.start()
        own_qup.start()
        own_state.start()
        for d in others:
            shift_copy(d).start()

    own_tok = pltpu.make_async_copy(tok_ref, tok_all.at[z], local_sem.at[6])
    own_shift = pltpu.make_async_copy(shift_ref, shift_all.at[z], local_sem.at[7])
    att_wide = kvup.shape[1]
    own_kvup = pltpu.make_async_copy(kvup_ref.at[:, at(z, att_wide)], kvup, local_sem.at[8])
    own_state = pltpu.make_async_copy(start_ref.at[z], state, local_sem.at[9])
    up_wide = qup.shape[1]
    own_qup = pltpu.make_async_copy(qup_ref.at[:, at(z, up_wide)], qup, local_sem.at[10])
    own_kvd = pltpu.make_async_copy(wkvd_ref, kv_src.at[:, :kv_wide], local_sem.at[11])

    def norm_block(i):
        x = tok_all[i].astype(f32)
        scaled = x * lax.rsqrt(jnp.mean(x * x, axis=-1, keepdims=True) + EPSILON)
        normed[at(i), :] = (scaled * gain_ref[...]).astype(bf16)

    depth = fs * rows

    def multiply(u):
        weight, columns = (
            (w_lat, slice(None)) if u == LAT else (w_all, slice((u - 1) * WIDE, u * WIDE))
        )
        acc = acc_lat if u == LAT else acc_ret
        with jax.named_scope(f"multiply#u={u}"):
            acc[...] = jnp.dot(
                normed[:, :depth],
                weight[:depth, columns],
                preferred_element_type=f32,
            )

            def chunk(i, carry):
                begin = at(i, depth)
                acc[...] += jnp.dot(
                    normed[:, begin],
                    weight[begin, columns],
                    preferred_element_type=f32,
                )
                return carry

            lax.fori_loop(1, n_sp, chunk, 0)

    rd = RET_DIM // 2

    def finish_lat():
        def block(i, carry):
            lat_all[t, z - q_place, at(i), :kv_wide] = acc_lat[at(i), :kv_wide].astype(bf16)
            pair = acc_lat[at(i), kv_wide:]
            turned = pair * pcos_ref[at(i), :] + pltpu.roll(pair, ROPE_DIM, 1) * psin_ref[at(i), :]
            lane = lax.broadcasted_iota(jnp.int32, turned.shape, 1)
            turned = jnp.where(lane < ROPE_DIM, turned, pltpu.roll(turned, ROPE_DIM, 1))
            lat_all[t, z - q_place, at(i), kv_wide:] = jnp.where(
                z == kv_place, turned, pair
            ).astype(bf16)
            return carry

        lax.fori_loop(0, n_sp, block, 0)

    def finish_turned(dst, factor):
        def block(i, carry):
            cosine, sine = rcos_ref[at(i), :], rsin_ref[at(i), :]
            a, b = acc_ret[at(i), :rd], acc_ret[at(i), rd:]
            dst[at(i), :rd] = ((a * cosine - b * sine) * factor).astype(bf16)
            dst[at(i), rd:] = ((b * cosine + a * sine) * factor).astype(bf16)
            return carry

        lax.fori_loop(0, n_sp, block, 0)

    def project(u):
        for d in range(n_sp):
            arrive(d, u)
        multiply(u)
        if u == QUERY:
            finish_turned(ret_q, 1.0)
        elif u == KEY:
            finish_turned(ret_k, RET_DIM ** (-0.5))
        else:
            ret_v[...] = acc_ret[...].astype(bf16)

    r_iota = lax.broadcasted_iota(jnp.int32, (rows, rows), 0)
    c_iota = lax.broadcasted_iota(jnp.int32, (rows, rows), 1)

    def retention(b):
        rates = shift_all[b]
        pick = lax.broadcasted_iota(jnp.int32, rates.shape, 0) == z
        chosen = lax.broadcasted_iota(jnp.int32, rate_ref.shape, 1) == z
        rate = jnp.sum(jnp.where(chosen, rate_ref[...], 0.0), axis=1, keepdims=True)
        row = jnp.sum(jnp.where(pick, rates, 0.0), axis=0, keepdims=True) + rate
        column = jnp.sum(jnp.where(r_iota == c_iota, row, 0.0), axis=1, keepdims=True)
        c_col = jnp.sum(jnp.where(c_iota <= r_iota, row, 0.0), axis=1, keepdims=True)
        c_row = jnp.sum(jnp.where(r_iota <= c_iota, column, 0.0), axis=0, keepdims=True)
        last = jnp.sum(row, axis=1, keepdims=True)
        decay = jnp.exp(jnp.where(c_iota <= r_iota, c_col - c_row, -jnp.inf))
        block = slice(b * rows, (b + 1) * rows)
        q, k, v = ret_q[block, :], ret_k[block, :], ret_v[block, :]
        scores = lax.dot_general(q, k, CONTRACT, preferred_element_type=f32) * decay
        raw = jnp.dot(scores.astype(bf16), v, preferred_element_type=f32)
        carried = sum(
            jnp.dot(q, s, preferred_element_type=f32) for s in three_parts(state[...])
        )
        raw = raw + carried * jnp.exp(c_col)
        if b < n_sp - 1:
            weighted = k.astype(f32) * jnp.exp(last - c_col)
            added = sum(
                lax.dot_general(w, v, (((0,), (0,)), ((), ())), preferred_element_type=f32)
                for w in three_parts(weighted)
            )
            state[...] = jnp.exp(last) * state[...] + added
        centered = raw - jnp.mean(raw, axis=-1, keepdims=True)
        variance = jnp.mean(centered * centered, axis=-1, keepdims=True)
        merged[block, :WIDE] = (centered * lax.rsqrt(variance + EPSILON) * rgain_ref[z]).astype(
            bf16
        )

    att_heads = att_wide // (NOPE_DIM + VAL_DIM)

    def expand(i):
        def latent(slot, wide, gain):
            x = jnp.concatenate(
                [lat_all[core, slot, at(i), :wide] for core in range(2)], axis=1
            ).astype(f32)
            scaled = x * lax.rsqrt(jnp.mean(x * x, axis=-1, keepdims=True) + EPSILON)
            return (scaled * gain[...]).astype(bf16)

        query = jnp.dot(latent(0, q_wide, qgain_ref), qup[...], preferred_element_type=f32)
        first, middle, end = query[:, :128], query[:, 128:256], query[:, 256:]
        lane = lax.broadcasted_iota(jnp.int32, first.shape, 1)
        second = jnp.where(
            lane < ROPE_DIM, pltpu.roll(middle, ROPE_DIM, 1), pltpu.roll(end, ROPE_DIM, 1)
        )
        pair = jnp.where(lane < ROPE_DIM, middle, end)
        quarter = ROPE_DIM // 2
        swapped = jnp.where(
            lane % ROPE_DIM < quarter,
            pltpu.roll(pair, 2 * ROPE_DIM - quarter, 1),
            pltpu.roll(pair, quarter, 1),
        )
        qn[at(i), :NOPE_DIM] = first.astype(bf16)
        qn[at(i), NOPE_DIM:] = second.astype(bf16)
        qr[at(i), :] = (pair * pcos_ref[at(i), :] + swapped * psin_ref[at(i), :]).astype(bf16)
        expanded[at(i), :] = jnp.dot(
            latent(1, kv_wide, kvgain_ref), kvup[...], preferred_element_type=f32
        ).astype(bf16)
        rope_key[at(i), :] = lat_all[0, 1, at(i), kv_wide:]

    scale = (NOPE_DIM + ROPE_DIM) ** (-0.5)

    def attend(b):
        seen = (b + 1) * rows
        block = slice(b * rows, seen)
        q_at = lax.broadcasted_iota(jnp.int32, (rows, seen), 0) + b * rows
        k_at = lax.broadcasted_iota(jnp.int32, (rows, seen), 1)
        for h in range(att_heads):
            base = h * (NOPE_DIM + VAL_DIM)
            turned = qr[block, :]
            lane = lax.broadcasted_iota(jnp.int32, turned.shape, 1)
            turned = jnp.where(lane // ROPE_DIM == h, turned, jnp.zeros_like(turned))
            s = lax.dot_general(
                qn[block, h * NOPE_DIM : (h + 1) * NOPE_DIM],
                expanded[:seen, base : base + NOPE_DIM],
                CONTRACT,
                preferred_element_type=f32,
            ) + lax.dot_general(
                turned, rope_key[:seen, :], CONTRACT, preferred_element_type=f32
            )
            s = jnp.where(k_at <= q_at, s * scale, -jnp.inf)
            p = jnp.exp(s - jnp.max(s, axis=-1, keepdims=True))
            raw = jnp.dot(
                p.astype(bf16),
                expanded[:seen, base + NOPE_DIM : base + NOPE_DIM + VAL_DIM],
                preferred_element_type=f32,
            ) / jnp.sum(p, axis=-1, keepdims=True)
            scaled = raw * lax.rsqrt(jnp.mean(raw * raw, axis=-1, keepdims=True) + EPSILON)
            gain = again_ref[z][:, h * VAL_DIM : (h + 1) * VAL_DIM]
            merged[block, WIDE + h * VAL_DIM : WIDE + (h + 1) * VAL_DIM] = (
                scaled * gain
            ).astype(bf16)

    def out_copy(b):
        return remote(pair_out.at[b], pair_in.at[b], m_send.at[1, b], m_recv.at[1, b], tp=other)

    def row_copy(b, origin):
        return remote(row_out.at[b], row_in.at[origin], m_send.at[2, b], m_recv.at[2, origin], sp=b)

    def project_out(b):
        got = lax.dot_general(
            merged[at(b), :],
            w_all[:, (OUT_RET - 1) * WIDE :],
            CONTRACT,
            preferred_element_type=f32,
        )
        front, back = got[:half, :], got[half:, :]
        pair_out[b] = jnp.where(t == 0, back, front).astype(bf16)
        out_copy(b).start()
        own_sum[b] = jnp.where(t == 0, front, back)

    def send_rows(b):
        with jax.named_scope("rows_pair"):
            out_copy(b).wait_recv()
        total = own_sum[b] + pair_in[b].astype(f32)
        own_sum[b] = total

        @pl.when(z != b)
        def _():
            row_out[b] = total.astype(bf16)
            row_copy(b, z).start()


    def many(action, *pairs):
        for k, u in pairs:
            action(k, u)

    def norm_others():
        pair_arrive(tok_part, 0, False)
        for k in others:
            norm_block(origin_of(k))

    def send_near_end(u):
        for dest in (0, n_sp - 1):
            pl.when(direct(dest))(lambda dest=dest: z_copy(dest, u).start())

    def send_far_end(u):
        for dest in (0, n_sp - 1):
            pl.when((z - dest == 2) | (dest - z == 2))(lambda dest=dest: z_copy(dest, u).start())

    def send_middle(u):
        for dest in lat_sources:
            pl.when(z != dest)(lambda dest=dest: z_copy(dest, u).start())

    ret_weights = (QUERY, KEY, VALUE)
    out_weights = (OUT_RET, OUT_ATT)

    own_kvd.start()
    pl.when(~is_end)(lambda: line_start(tok_part, 0, tok_ref.at[mine]))

    @pl.when(z == q_place)
    def _():
        own_lat_copy(q_place).start()

    for u in ret_weights + out_weights:
        own_copy(u).start()
    send_lat(q_place)
    for u in ret_weights + out_weights:
        send_near_end(u)
    with jax.named_scope("kvsrc"):
        own_kvd.wait()
    rope = rope_ref[...]
    kv_src[:, kv_wide:] = jnp.concatenate(
        [rope, rope[:, ROPE_DIM // 2 :], rope[:, : ROPE_DIM // 2]], axis=1
    )

    @pl.when(z == kv_place)
    def _():
        own_lat_copy(kv_place).start()

    send_lat(kv_place)

    @pl.when(is_end)
    def _():
        line_start(tok_part, 0, tok_ref.at[mine], (2, 1))
        for u in ret_weights:
            send(u)
        start_inputs()
        many(spread, (0, QUERY), (0, KEY), (0, VALUE), (0, OUT_RET), (0, OUT_ATT))
        own_tok.wait()
        norm_block(z)
        many(spread, (1, QUERY), (1, KEY))
        many(relay, (0, QUERY), (0, KEY))
        many(spread, (1, VALUE))
        many(relay, (0, VALUE))
        many(spread, (1, OUT_RET), (1, OUT_ATT))
        many(relay, (0, OUT_RET), (0, OUT_ATT))
        many(relay, (1, QUERY), (1, KEY))
        many(spread, (2, QUERY))
        many(relay, (1, VALUE))
        many(spread, (2, KEY))
        many(relay, (1, OUT_RET), (1, OUT_ATT))
        many(spread, (2, VALUE))
        many(relay, (2, QUERY), (2, KEY))
        many(spread, (3, QUERY))
        many(relay, (2, VALUE))
        many(spread, (3, KEY))
        many(relay, (3, QUERY))
        many(spread, (3, VALUE))
        many(relay, (3, KEY))
        line_pair(tok_part, 0)
        send(OUT_RET)
        send(OUT_ATT)
        norm_others()
        project(QUERY)
        many(relay, (3, VALUE))
        project(KEY)

    @pl.when(~is_end)
    def _():
        for u in ret_weights:
            send_far_end(u)
        for u in ret_weights:
            send_middle(u)
        start_inputs()
        many(spread, (0, LAT), (0, QUERY), (0, KEY))
        many(relay, (0, LAT))
        many(spread, (2, LAT), (3, LAT), (0, VALUE))
        own_tok.wait()
        norm_block(z)
        many(relay, (0, QUERY), (0, KEY), (2, LAT))
        line_relay(tok_part, 0, 1)
        many(spread, (1, LAT), (0, OUT_RET), (0, OUT_ATT))
        many(relay, (3, LAT), (0, VALUE), (1, LAT))
        line_relay(tok_part, 0, 2)
        line_pair(tok_part, 0)
        many(relay, (0, OUT_RET), (0, OUT_ATT))
        norm_others()
        for k in range(n_sp):
            arrive(k, LAT)
        multiply(LAT)
        finish_lat()
        for i in range(LAT_PARTS):
            line_start(lat_part(i), i + 1)
        for i in range(LAT_PARTS):
            pair_own(lat_part(i), i + 1)
        for u in out_weights:
            send_middle(u)
            send_far_end(u)
        many(spread, (1, QUERY), (2, QUERY), (3, QUERY))
        many(spread, (1, KEY), (2, KEY))
        many(relay, (1, QUERY), (2, QUERY), (3, QUERY))
        many(spread, (3, KEY), (1, VALUE), (2, VALUE))
        many(relay, (1, KEY), (2, KEY))
        many(spread, (3, VALUE))
        line_relay(lat_part(0), 1, 1)
        many(relay, (3, KEY))
        project(QUERY)
        many(relay, (1, VALUE), (2, VALUE))
        many(spread, (1, OUT_RET))
        line_relay(lat_part(1), 2, 1)
        many(relay, (3, VALUE))
        project(KEY)
        many(spread, (1, OUT_ATT))

    project(VALUE)
    for d in others:
        shift_copy(d).wait_recv()
    own_shift.wait()
    own_state.wait()
    own_kvup.wait()
    own_qup.wait()
    many(spread, (2, OUT_RET))
    for b in range(n_sp):
        with jax.named_scope(f"retention#b={b}"):
            retention(b)
    many(spread, (3, OUT_RET), (2, OUT_ATT))
    pl.when(~is_end)(lambda: many(relay, (1, OUT_RET)))
    many(relay, (2, OUT_RET))
    many(spread, (3, OUT_ATT))
    pl.when(~is_end)(lambda: many(relay, (1, OUT_ATT)))

    blocks = n_sp // LAT_PARTS
    for i in range(LAT_PARTS):
        line_pair(lat_part(i), i + 1)
        if i == 0:
            many(relay, (3, OUT_RET))
        else:
            many(relay, (2, OUT_ATT), (3, OUT_ATT))
        pair_arrive(lat_part(i), i + 1, True)
        for b in range(i * blocks, (i + 1) * blocks):
            with jax.named_scope(f"expand#b={b}"):
                expand(b)
        for b in range(i * blocks, (i + 1) * blocks):
            with jax.named_scope(f"attend#b={b}"):
                attend(b)
    for u in out_weights:
        for k in range(n_sp):
            arrive(k, u)
    order = (3 - 3 * upper, 2 - upper, z + 1 - 2 * (z % 2), z)
    for step, b in enumerate(order):
        with jax.named_scope(f"out#b={step}"):
            project_out(b)
        if step:
            send_rows(order[step - 1])
    send_rows(order[-1])
    total = own_sum[z]
    for k in others:
        with jax.named_scope(f"rows#k={k}"):
            row_copy(0, origin_of(k)).wait_recv()
        total = total + row_in[origin_of(k)].astype(f32)
    out_ref[...] = total.astype(bf16)

    for u in range(UNITS):
        for k in range(n_sp):

            def drain(k=k, u=u):
                x_copy(k, u).wait_send()
                y_copy(k, u).wait_send()
                f_copy(k, u).wait_send()

            when(has(u, z), drain)
            if k and u != LAT:
                z_copy(origin_of(k), u).wait_send()
    for place in lat_sources:
        pl.when(z != place)(
            lambda place=place: z_copy(place, LAT, lat_sources[place]).wait_send()
        )
    for d in others:
        shift_copy(d).wait_send()
    line_drain(tok_part, 0, False)
    for i in range(LAT_PARTS):
        line_drain(lat_part(i), i + 1, True)
    for b in range(n_sp):
        out_copy(b).wait_send()
        pl.when(z != b)(lambda b=b: row_copy(b, z).wait_send())


def heads_plan(
    tokens,
    norm_gain,
    w_ret_query,
    w_ret_key,
    w_ret_value,
    w_q_down,
    w_kv_down,
    w_rope_key,
    w_q_up,
    w_kv_up,
    q_lat_gain,
    kv_lat_gain,
    att_norm_gain,
    ret_norm_gain,
    w_ret_out,
    w_att_out,
    head_rate,
    decay_shift,
    start_state,
):
    n_sp = lax.axis_size("sp")
    rows, width = tokens.shape[1:]
    length = n_sp * rows
    q_wide, kv_wide = w_q_down.shape[1], w_kv_down.shape[1]
    w_rows = w_q_down.shape[0]
    att_heads = w_q_up.shape[1] // (NOPE_DIM + ROPE_DIM) // n_sp

    ret_cos, ret_sin = wave_tables(length, RET_DIM)
    rope_cos, rope_sin = wave_tables(length, ROPE_DIM)
    pair_cos = np.concatenate([rope_cos] * 4, axis=1)
    pair_sin = np.concatenate([-rope_sin, rope_sin] * 2, axis=1)
    dma = pltpu.SemaphoreType.DMA
    vmem = pltpu.VMEM
    f32, bf16 = jnp.float32, jnp.bfloat16
    half = rows // 2
    out_wide = 4 * n_sp * w_rows
    any_spec = pl.BlockSpec(memory_space=pl.ANY)
    vmem_spec = pl.BlockSpec(memory_space=pltpu.VMEM)
    mixed = pl.pallas_call(
        functools.partial(layer_kernel, n_sp, q_wide, kv_wide),
        out_shape=jax.ShapeDtypeStruct((half, out_wide), bf16),
        in_specs=[any_spec] * 8 + [vmem_spec, any_spec] + [vmem_spec] * 10 + [any_spec] * 3,
        out_specs=vmem_spec,
        scratch_shapes=[
            vmem((n_sp, rows, width), bf16),
            vmem((n_sp * 4 * w_rows, (UNITS - 1) * WIDE), bf16),
            vmem((n_sp * 4 * w_rows, q_wide), bf16),
            vmem((w_rows, q_wide), bf16),
            vmem((n_sp,) + decay_shift.shape[1:], f32),
            vmem((length, width), bf16),
            vmem((length, WIDE), f32),
            vmem((length, q_wide), f32),
            vmem((length, WIDE), bf16),
            vmem((length, WIDE), bf16),
            vmem((length, WIDE), bf16),
            vmem((2, 2, length, q_wide), bf16),
            vmem((RET_DIM, RET_DIM), f32),
            vmem((length, att_heads * NOPE_DIM), bf16),
            vmem((length, att_heads * ROPE_DIM), bf16),
            vmem((length, att_heads * (NOPE_DIM + VAL_DIM)), bf16),
            vmem((length, 2 * ROPE_DIM), bf16),
            vmem((w_kv_up.shape[0], att_heads * (NOPE_DIM + VAL_DIM)), bf16),
            vmem((w_q_up.shape[0], att_heads * (NOPE_DIM + ROPE_DIM)), bf16),
            vmem((length, WIDE + att_heads * VAL_DIM), bf16),
            vmem((n_sp, half, out_wide), f32),
            vmem((n_sp, half, out_wide), bf16),
            vmem((n_sp, half, out_wide), bf16),
            vmem((n_sp, half, out_wide), bf16),
            vmem((n_sp, half, out_wide), bf16),
            dma((12,)),
            *[dma((n_sp, UNITS))] * 8,
            *[dma((3, n_sp))] * 2,
            *[dma((LAT_PARTS + 1, n_sp))] * 5,
        ],
        compiler_params=pltpu.CompilerParams(
            collective_id=0, has_side_effects=True, vmem_limit_bytes=62 * 1024 * 1024
        ),
    )(
        tokens[0],
        w_q_down,
        w_kv_down,
        w_ret_query,
        w_ret_key,
        w_ret_value,
        w_ret_out,
        w_att_out,
        w_rope_key,
        decay_shift[0],
        head_rate[None],
        norm_gain[None],
        q_lat_gain[None],
        kv_lat_gain[None],
        att_norm_gain.reshape(n_sp, 1, -1),
        ret_norm_gain.reshape(n_sp, 1, -1),
        ret_cos,
        ret_sin,
        pair_cos,
        pair_sin,
        w_q_up,
        w_kv_up,
        start_state[0],
    )
    return mixed[None]


def solution(mesh):
    placed = (
        P("fs", "sp", None),
        P(),
        P(("sp", "fs"), "tp"),
        P(("sp", "fs"), "tp"),
        P(("sp", "fs"), "tp"),
        P(("sp", "fs"), "tp"),
        P(("sp", "fs"), "tp"),
        P(("sp", "fs"), None),
        P(None, "tp"),
        P(None, "tp"),
        P(),
        P(),
        P("tp"),
        P("tp"),
        P(("sp", "fs"), "tp"),
        P(("sp", "fs"), "tp"),
        P("tp"),
        P("fs", "tp", "sp"),
        P("fs", "tp", None, None),
    )

    def pick(*args):
        if heads_fit(
            mesh, args[16].shape[0], args[0].shape[0], args[5].shape[1], args[6].shape[1], args[8].shape[1]
        ):
            return heads_plan(*args)
        return rows_plan(*args)

    return jax.shard_map(
        pick,
        mesh=mesh,
        in_specs=placed,
        out_specs=P("fs", ("sp", "tp"), None),
        check_vma=False,
    )
```

```python
import functools

import numpy as np

import jax
import jax.numpy as jnp
from jax import lax
from jax.experimental import pallas as pl
from jax.experimental.pallas import tpu as pltpu
from jax.sharding import PartitionSpec as P

RET_DIM = 256
NOPE_DIM = 128
ROPE_DIM = 64
VAL_DIM = 128
KV_LAT = 512


EPSILON = 1e-06
THETA_BASE = 10000.0
TOP_PRECISION = lax.Precision.HIGHEST


def prefix(x, axis, combine, identity):
    peers, position = (lax.axis_size(axis), lax.axis_index(axis))
    everything = jax.tree.map(
        lambda part, kind: lax.all_gather(part.astype(kind), axis), x, (jnp.bfloat16, jnp.bfloat16)
    )
    start = jax.tree.map(
        lambda part, zero: jnp.broadcast_to(jnp.asarray(zero, part.dtype), part.shape), x, identity
    )

    def lap(k, before):
        reached = k < position
        new = combine(
            before, jax.tree.map(lambda part, own: part[k].astype(own.dtype), everything, x)
        )
        return jax.tree.map(lambda a, b: jnp.where(reached, a, b), new, before)

    return lax.fori_loop(0, peers, lap, start)


def angle_tables(positions, rot_width):
    half_width = rot_width // 2
    inverse = THETA_BASE ** (-jnp.arange(half_width, dtype=jnp.float32) * 2.0 / rot_width)
    angles = positions.astype(jnp.float32)[:, None] * inverse[None, :]
    return (jnp.cos(angles), jnp.sin(angles))


def rotate(values, cosine, sine):
    half_width = values.shape[-1] // 2
    front_half = values[..., :half_width]
    back_half = values[..., half_width:]
    return jnp.concatenate(
        [front_half * cosine - back_half * sine, back_half * cosine + front_half * sine], axis=-1
    )


def rms_scale(values, gain_vector):
    return (
        values
        * lax.rsqrt(jnp.mean(values * values, axis=-1, keepdims=True) + EPSILON)
        * gain_vector
    )


def chain_states(earlier, later):
    early_log, early_state = earlier
    late_log, late_state = later
    return (early_log + late_log, jnp.exp(late_log)[:, None, None] * early_state + late_state)


def rows_plan(
    tokens,
    norm_gain,
    w_ret_query,
    w_ret_key,
    w_ret_value,
    w_q_down,
    w_kv_down,
    w_rope_key,
    w_q_up,
    w_kv_up,
    q_lat_gain,
    kv_lat_gain,
    att_norm_gain,
    ret_norm_gain,
    w_ret_out,
    w_att_out,
    head_rate,
    decay_shift,
    start_state,
):
    tok_rows = tokens.shape[1]
    ret_local = head_rate.shape[0]
    att_local = w_q_up.shape[1] // (NOPE_DIM + ROPE_DIM)
    row_offset = lax.axis_index("sp") * tok_rows
    positions = row_offset + jnp.arange(tok_rows, dtype=jnp.int32)
    (
        full_query,
        full_key,
        full_value,
        full_q_down,
        full_kv_down,
        full_rope,
        full_ret_out,
        full_att_out,
    ) = (
        lax.all_gather(w_ret_query, ("sp", "fs"), axis=0, tiled=True),
        lax.all_gather(w_ret_key, ("sp", "fs"), axis=0, tiled=True),
        lax.all_gather(w_ret_value, ("sp", "fs"), axis=0, tiled=True),
        lax.all_gather(w_q_down, ("sp", "fs"), axis=0, tiled=True),
        lax.all_gather(w_kv_down, ("sp", "fs"), axis=0, tiled=True),
        lax.all_gather(w_rope_key, ("sp", "fs"), axis=0, tiled=True),
        lax.all_gather(w_ret_out, ("sp", "fs"), axis=0, tiled=True),
        lax.all_gather(w_att_out, ("sp", "fs"), axis=0, tiled=True),
    )
    source = tokens[0].astype(jnp.float32)
    normed = rms_scale(source, norm_gain).astype(jnp.bfloat16)
    ret_cos, ret_sin = angle_tables(positions, RET_DIM)
    rope_cos, rope_sin = angle_tables(positions, ROPE_DIM)

    def project(weight):
        return jnp.dot(normed, weight, preferred_element_type=jnp.float32)

    part_q = project(full_q_down).astype(jnp.bfloat16)
    part_kv = project(full_kv_down).astype(jnp.bfloat16)
    lat_q_raw, lat_kv_raw = (
        lax.all_gather(part_q, "tp", axis=1, tiled=True),
        lax.all_gather(part_kv, "tp", axis=1, tiled=True),
    )
    retention_query = rotate(
        project(full_query).reshape(tok_rows, ret_local, RET_DIM),
        ret_cos[:, None],
        ret_sin[:, None],
    ).astype(jnp.bfloat16)
    retention_key = (
        rotate(
            project(full_key).reshape(tok_rows, ret_local, RET_DIM),
            ret_cos[:, None],
            ret_sin[:, None],
        )
        * RET_DIM ** (-0.5)
    ).astype(jnp.bfloat16)
    retention_value = project(full_value).reshape(tok_rows, ret_local, RET_DIM).astype(jnp.bfloat16)
    rope_key = rotate(project(full_rope), rope_cos, rope_sin).astype(jnp.bfloat16)
    log_rates = head_rate[:, None] + decay_shift[0]
    cumul = jnp.cumsum(log_rates, axis=1)
    offsets = jnp.arange(tok_rows, dtype=jnp.int32)
    lower_mask = offsets[None, :] <= offsets[:, None]
    decay_matrix = jnp.exp(
        jnp.where(lower_mask[None], cumul[:, :, None] - cumul[:, None, :], -jnp.inf)
    )
    block_score_grid = (
        jnp.einsum(
            "zgq,ugq->gzu", retention_query, retention_key, preferred_element_type=jnp.float32
        )
        * decay_matrix
    ).astype(jnp.bfloat16)
    inside_block_output = jnp.einsum(
        "vzs,svp->zvp", block_score_grid, retention_value, preferred_element_type=jnp.float32
    )
    block_output_sum = cumul[:, -1]
    weighted_values = (
        retention_key.astype(jnp.float32) * jnp.exp(block_output_sum[:, None] - cumul).T[:, :, None]
    )
    contribution = jnp.einsum(
        "uzj,uzv->zjv",
        weighted_values,
        retention_value.astype(jnp.float32),
        precision=TOP_PRECISION,
    )
    identity = (jnp.zeros_like(block_output_sum), jnp.zeros_like(contribution))
    before_log, before_state = prefix(
        (block_output_sum, contribution), "sp", chain_states, identity
    )
    q_latent = rms_scale(lat_q_raw.astype(jnp.float32), q_lat_gain).astype(jnp.bfloat16)
    kv_latent = rms_scale(lat_kv_raw.astype(jnp.float32), kv_lat_gain).astype(jnp.bfloat16)
    query_full = jnp.dot(q_latent, w_q_up, preferred_element_type=jnp.float32).reshape(
        tok_rows, att_local, NOPE_DIM + ROPE_DIM
    )
    query_nope = query_full[..., :NOPE_DIM].astype(jnp.bfloat16)
    query_rope = rotate(query_full[..., NOPE_DIM:], rope_cos[:, None], rope_sin[:, None]).astype(
        jnp.bfloat16
    )
    att_scale = (NOPE_DIM + ROPE_DIM) ** (-0.5)

    def attend(carry, key_nope, key_values, key_rope, start):
        running_max, running_sum, running_acc = carry
        key_count = key_rope.shape[0]
        score_matrix = (
            jnp.einsum("qhd,khd->hqk", query_nope, key_nope, preferred_element_type=jnp.float32)
            + jnp.einsum("qhd,kd->hqk", query_rope, key_rope, preferred_element_type=jnp.float32)
        ) * att_scale
        key_positions = start + jnp.arange(key_count, dtype=jnp.int32)
        allowed = key_positions[None, :] <= positions[:, None]
        masked = jnp.where(allowed[None], score_matrix, -jnp.inf)
        new_max = jnp.maximum(running_max, jnp.max(masked, axis=-1))
        safe_max = jnp.where(jnp.isfinite(new_max), new_max, 0.0)
        weights = jnp.exp(masked - safe_max[..., None])
        rescale = jnp.exp(running_max - safe_max)
        new_sum = running_sum * rescale + jnp.sum(weights, axis=-1)
        new_acc = running_acc * rescale[..., None] + jnp.einsum(
            "hqk,khd->hqd",
            weights.astype(jnp.bfloat16),
            key_values,
            preferred_element_type=jnp.float32,
        )
        return (new_max, new_sum, new_acc)

    def expand_attend(carry_in, lat_piece, rope_piece, start):
        wide = (
            jnp.dot(lat_piece, w_kv_up, preferred_element_type=jnp.float32)
            .astype(jnp.bfloat16)
            .reshape(rope_piece.shape[0], att_local, NOPE_DIM + VAL_DIM)
        )
        return attend(carry_in, wide[..., :NOPE_DIM], wide[..., NOPE_DIM:], rope_piece, start)

    empty = (
        jnp.full((att_local, tok_rows), -jnp.inf, jnp.float32),
        jnp.zeros((att_local, tok_rows), jnp.float32),
        jnp.zeros((att_local, tok_rows, VAL_DIM), jnp.float32),
    )
    groups = lax.axis_size("tp")
    kv_part = KV_LAT // groups
    rope_part = ROPE_DIM // groups
    my_group = lax.axis_index("tp")
    joined = jnp.concatenate(
        [
            lax.dynamic_slice_in_dim(kv_latent, my_group * kv_part, kv_part, 1),
            lax.dynamic_slice_in_dim(rope_key, my_group * rope_part, rope_part, 1),
        ],
        axis=1,
    )
    all_rows = lax.all_gather(joined, "sp", axis=0, tiled=True)
    complete = lax.all_gather(all_rows, "tp", axis=1, tiled=True)
    total_rows = complete.shape[0]
    grouped = complete.reshape(total_rows, groups, kv_part + rope_part)
    lat_all = grouped[:, :, :kv_part].reshape(total_rows, KV_LAT)
    rope_all = grouped[:, :, kv_part:].reshape(total_rows, ROPE_DIM)

    def visit(block_index, carry_in):
        start = block_index * tok_rows
        lat_piece = lax.dynamic_slice_in_dim(lat_all, start, tok_rows, 0)
        rope_piece = lax.dynamic_slice_in_dim(rope_all, start, tok_rows, 0)
        return expand_attend(carry_in, lat_piece, rope_piece, start)

    final = lax.fori_loop(0, lax.axis_index("sp") + 1, visit, empty)
    att_raw = jnp.transpose(final[2] / final[1][..., None], (1, 0, 2))
    att_out = (
        rms_scale(att_raw, att_norm_gain.reshape(att_local, VAL_DIM))
        .astype(jnp.bfloat16)
        .reshape(tok_rows, att_local * VAL_DIM)
    )
    entering = jnp.exp(before_log)[:, None, None] * start_state[0] + before_state
    carried_term = (
        jnp.einsum(
            "nhd,hde->nhe", retention_query.astype(jnp.float32), entering, precision=TOP_PRECISION
        )
        * jnp.exp(cumul).T[:, :, None]
    )
    ret_raw = inside_block_output + carried_term
    row_mean = jnp.mean(ret_raw, axis=-1, keepdims=True)
    centered = ret_raw - row_mean
    row_var = jnp.mean(centered * centered, axis=-1, keepdims=True)
    ret_out = (
        (centered * lax.rsqrt(row_var + EPSILON) * ret_norm_gain.reshape(ret_local, RET_DIM))
        .astype(jnp.bfloat16)
        .reshape(tok_rows, ret_local * RET_DIM)
    )
    contract = (((1,), (1,)), ((), ()))
    mixed = lax.psum_scatter(
        (
            lax.dot_general(ret_out, full_ret_out, contract, preferred_element_type=jnp.float32)
            + lax.dot_general(att_out, full_att_out, contract, preferred_element_type=jnp.float32)
        ).astype(jnp.bfloat16),
        "tp",
        scatter_dimension=0,
        tiled=True,
    )
    return mixed[None]


MESH = pl.DeviceIdType.MESH
WIDE = RET_DIM
CONTRACT = (((1,), (1,)), ((), ()))
UNITS = 6
LAT, QUERY, KEY, VALUE, OUT_RET, OUT_ATT = range(UNITS)
LAT_PARTS = 2
OUT_PARTS = 2
LEAD = 5


def heads_fit(mesh, ret_local, sequences, q_wide, kv_wide, up_wide):
    sizes = mesh.shape
    return (
        sizes["sp"] == 4
        and sizes["fs"] == 4
        and sizes["tp"] == 2
        and ret_local == sizes["sp"]
        and sequences == 1
        and up_wide == 2 * (NOPE_DIM + ROPE_DIM) * ret_local
        and q_wide % 128 == 0
        and kv_wide % 128 == 0
        and q_wide == kv_wide + 2 * ROPE_DIM
    )


def wave_tables(length, wide):
    half_wide = wide // 2
    powers = np.arange(half_wide, dtype=np.float32) * np.float32(2.0 / wide)
    inverse = np.power(np.float32(THETA_BASE), -powers).astype(np.float32)
    angles = np.arange(length, dtype=np.float32)[:, None] * inverse[None, :]
    return np.cos(angles), np.sin(angles)


def three_parts(x):
    high = x.astype(jnp.bfloat16)
    rest = x - high.astype(jnp.float32)
    middle = rest.astype(jnp.bfloat16)
    low = (rest - middle.astype(jnp.float32)).astype(jnp.bfloat16)
    return high, middle, low


def layer_kernel(
    n_sp,
    q_wide,
    kv_wide,
    tok_ref,
    wqd_ref,
    wkvd_ref,
    wq_ref,
    wk_ref,
    wv_ref,
    wr_ref,
    wa_ref,
    rope_hbm,
    shift_ref,
    rate_hbm,
    gain_hbm,
    qgain_hbm,
    kvgain_hbm,
    again_hbm,
    rgain_hbm,
    rcos_hbm,
    rsin_hbm,
    pcos_hbm,
    psin_hbm,
    qup_ref,
    kvup_ref,
    start_ref,
    out_ref,
    tok_all,
    w_all,
    w_lat,
    kv_src,
    rope_vmem,
    rate_ref,
    gain_ref,
    qgain_ref,
    kvgain_ref,
    again_ref,
    rgain_ref,
    rcos_ref,
    rsin_ref,
    pcos_ref,
    psin_ref,
    shift_all,
    normed,
    acc_ret,
    acc_lat,
    ret_q,
    ret_k,
    ret_v,
    lat_all,
    state,
    qn,
    qr,
    expanded,
    rope_key,
    kvup,
    qup,
    merged,
    own_sum,
    pair_out,
    pair_in,
    row_out,
    row_in,
    far_in,
    local_sem,
    z_send,
    z_recv,
    x_send,
    x_recv,
    y_send,
    y_recv,
    f_send,
    f_recv,
    m_send,
    m_recv,
    small_sem,
    o_send,
    o_recv,
    r_send,
    r_recv,
    far_recv,
    l_send,
    l_recv,
    l_relay,
    p_send,
    p_recv,
):
    z, f, t = lax.axis_index("sp"), lax.axis_index("fs"), lax.axis_index("tp")
    xn = f + 1 - 2 * (f % 2)
    yn = (f + 2) % 4
    other = 1 - t
    fs = 4
    rows = tok_ref.shape[0]
    length = n_sp * rows
    half = rows // 2
    weights = (None, wq_ref, wk_ref, wv_ref, wr_ref, wa_ref)
    f32, bf16 = jnp.float32, jnp.bfloat16
    q_place, kv_place = n_sp // 2 - 1, n_sp // 2
    others = range(1, n_sp)

    def remote(src, dst, send, recv, **where):
        return pltpu.make_async_remote_copy(
            src_ref=src,
            dst_ref=dst,
            send_sem=send,
            recv_sem=recv,
            device_id={"sp": z, "fs": f, "tp": t, **where},
            device_id_type=MESH,
        )

    barrier = pltpu.get_barrier_semaphore()
    peers = [{"sp": (z + d) % n_sp, "fs": f, "tp": t} for d in others]
    peers += [{"sp": z, "fs": xn, "tp": t}, {"sp": z, "fs": yn, "tp": t}]
    peers += [{"sp": z, "fs": f, "tp": other}]
    for peer in peers:
        pl.semaphore_signal(barrier, inc=1, device_id=peer, device_id_type=MESH)
    with jax.named_scope("barrier"):
        pl.semaphore_wait(barrier, len(peers))

    def at(i, size=rows):
        if isinstance(i, int):
            return slice(i * size, (i + 1) * size)
        return pl.ds(pl.multiple_of(i * size, size), size)

    upper = z // (n_sp // 2)
    is_end = (z == 0) | (z == n_sp - 1)

    def origin_of(k):
        depth_in = z + upper * (n_sp - 1 - 2 * z)
        found = (depth_in * 0, 1 + depth_in, 2 - 2 * depth_in, depth_in * 0 + 3)[k]
        return z if k == 0 else found + upper * (n_sp - 1 - 2 * found)


    def piece(u, dest):
        return weights[u].at[:, at(dest, WIDE)]

    def part(owner_z, owner_f, u):
        where = at(owner_z * fs + owner_f)
        if u == LAT:
            return w_lat.at[where]
        return w_all.at[where, (u - 1) * WIDE : u * WIDE]

    def has(u, place):
        return (place == q_place) | (place == kv_place) if u == LAT else True

    def when(condition, action):
        if condition is True:
            action()
        else:
            pl.when(condition)(action)

    lat_sources = {q_place: wqd_ref, kv_place: kv_src}

    def z_copy(to, u, src=None):
        return remote(
            piece(u, to) if src is None else src,
            part(z, f, u),
            z_send.at[to, u],
            z_recv.at[z, u],
            sp=to,
        )

    def z_arrival(k, u):
        ref = part(origin_of(k), f, u)
        return remote(ref, ref, z_send.at[z, u], z_recv.at[origin_of(k), u], tp=other)

    def x_copy(k, u):
        ref = part(origin_of(k), f, u)
        return remote(ref, ref, x_send.at[k, u], x_recv.at[k, u], fs=xn)

    def y_copy(k, u):
        ref = part(origin_of(k), f, u)
        return remote(ref, ref, y_send.at[k, u], y_recv.at[k, u], fs=yn)

    def f_copy(k, u):
        source, to = (xn, yn) if (k + u) % 2 == 0 else (yn, xn)
        ref = part(origin_of(k), source, u)
        return remote(ref, ref, f_send.at[k, u], f_recv.at[k, u], fs=to)

    def own_copy(u):
        return pltpu.make_async_copy(piece(u, z), part(z, f, u), local_sem.at[u])

    def own_lat_copy(place):
        return pltpu.make_async_copy(lat_sources[place], part(z, f, LAT), local_sem.at[LAT])

    def send(u):
        for k in others:
            z_copy(origin_of(k), u).start()

    def send_lat(place):
        pl.when(z != place)(lambda: z_copy(place, LAT, lat_sources[place]).start())

    def spread(d, u):
        def action():
            with jax.named_scope(f"spread#d={d}#u={u}"):
                if d:
                    z_arrival(d, u).wait_recv()
                elif u == LAT:
                    own_lat_copy(q_place).wait()
                else:
                    own_copy(u).wait()
            x_copy(d, u).start()
            y_copy(d, u).start()

        when(has(u, z), action)

    def relay(d, u):
        def action():
            with jax.named_scope(f"relay#d={d}#u={u}"):
                (x_copy if (d + u) % 2 == 0 else y_copy)(d, u).wait_recv()
            f_copy(d, u).start()

        when(has(u, z), action)

    def arrive(d, u):
        def action():
            with jax.named_scope(f"arrive#d={d}#u={u}"):
                (y_copy if (d + u) % 2 == 0 else x_copy)(d, u).wait_recv()
                f_copy(d, u).wait_recv()

        when(has(u, z), action)


    mine = pl.ds(pl.multiple_of(t * half, half), half)

    def tok_part(origin):
        return tok_all.at[origin, mine]

    lat_rows = length // LAT_PARTS

    def lat_part(i):
        return lambda origin: lat_all.at[t, origin - q_place, pl.ds(i * lat_rows, lat_rows)]

    def sends(row, origin):
        return True if row == 0 else has(LAT, origin)

    def both(condition, more):
        return condition if more is True else condition & more

    def steps(row):
        return range(1, n_sp - 1 if row == 0 else 2)

    def line_copy(where, row, dest, src=None):
        return remote(
            where(z) if src is None else src,
            where(z),
            l_send.at[row, dest],
            l_recv.at[row, z],
            sp=dest,
        )

    def relay_copy(where, row, origin, dest):
        ref = where(origin)
        return remote(ref, ref, l_relay.at[row, origin], l_recv.at[row, origin], sp=dest)

    def pair_copy(where, row, origin):
        ref = where(origin)
        return remote(ref, ref, p_send.at[row, origin], p_recv.at[row, origin], tp=other)

    def direct(dest):
        near = (z - dest == 1) | (dest - z == 1)
        return near if dest in (0, n_sp - 1) else z != dest

    def line_start(where, row, src=None, distances=others):
        for distance in distances:
            for dest in range(n_sp):
                condition = direct(dest) & ((z - dest == distance) | (dest - z == distance))
                pl.when(both(condition, sends(row, z)))(
                    lambda dest=dest: line_copy(where, row, dest, src).start()
                )

    ends = ((1, 0), (n_sp - 2, n_sp - 1))

    def line_relay(where, row, distance):
        for middle, dest in ends:
            origin = middle + (middle - dest) * distance

            @pl.when(both(z == middle, sends(row, origin)))
            def _(origin=origin, dest=dest):
                with jax.named_scope(f"line#r={row}#k={distance}"):
                    relay_copy(where, row, origin, dest).wait_recv()
                relay_copy(where, row, origin, dest).start()

    def was_relayed(origin):
        return z == (n_sp - 2 if origin < n_sp // 2 else 1)

    def line_pair(where, row):
        for distance in others:
            for origin in range(n_sp):
                here = (z - origin == distance) | (origin - z == distance)

                @pl.when(both(here, sends(row, origin)))
                def _(origin=origin):
                    with jax.named_scope(f"pass#r={row}#k={distance}"):
                        pl.when(~was_relayed(origin))(
                            lambda: relay_copy(where, row, origin, 0).wait_recv()
                        )
                    pair_copy(where, row, origin).start()

    def pair_own(where, row):
        for origin in range(n_sp):
            pl.when(both(origin == z, sends(row, origin)))(
                lambda origin=origin: pair_copy(where, row, origin).start()
            )

    def pair_arrive(where, row, own):
        with jax.named_scope(f"pair#r={row}"):
            for origin in range(n_sp):
                condition = sends(row, origin) if own else both(origin != z, sends(row, origin))
                when(condition, lambda origin=origin: pair_copy(where, row, origin).wait_recv())

    def line_drain(where, row, own):
        for dest in range(n_sp):
            pl.when(both(direct(dest), sends(row, z)))(
                lambda dest=dest: line_copy(where, row, dest).wait_send()
            )
        for middle, dest in ends:
            for distance in steps(row):
                origin = middle + (middle - dest) * distance
                pl.when(both(z == middle, sends(row, origin)))(
                    lambda origin=origin, dest=dest: relay_copy(
                        where, row, origin, dest
                    ).wait_send()
                )
        for origin in range(n_sp):
            condition = sends(row, origin) if own else both(origin != z, sends(row, origin))
            when(condition, lambda origin=origin: pair_copy(where, row, origin).wait_send())

    def shift_copy(d):
        to = (z + d) % n_sp
        return remote(shift_ref, shift_all.at[z], m_send.at[0, d], m_recv.at[0, d], sp=to)


    staged = (
        (rope_hbm, rope_vmem),
        (rate_hbm, rate_ref),
        (gain_hbm, gain_ref),
        (qgain_hbm, qgain_ref),
        (kvgain_hbm, kvgain_ref),
        (again_hbm, again_ref),
        (rgain_hbm, rgain_ref),
        (rcos_hbm, rcos_ref),
        (rsin_hbm, rsin_ref),
        (pcos_hbm, pcos_ref),
        (psin_hbm, psin_ref),
    )
    staged_copies = [
        pltpu.make_async_copy(src, dst, small_sem.at[i]) for i, (src, dst) in enumerate(staged)
    ]
    small_copies, table_copies = staged_copies[:7], staged_copies[7:]

    def wait_tables():
        for copy in table_copies:
            copy.wait()

    def start_inputs():
        for copy in table_copies:
            copy.start()
        own_tok.start()
        own_shift.start()
        own_kvup.start()
        own_qup.start()
        own_state.start()
        for d in others:
            shift_copy(d).start()

    own_tok = pltpu.make_async_copy(tok_ref, tok_all.at[z], local_sem.at[6])
    own_shift = pltpu.make_async_copy(shift_ref, shift_all.at[z], local_sem.at[7])
    att_wide = kvup.shape[1]
    own_kvup = pltpu.make_async_copy(kvup_ref.at[:, at(z, att_wide)], kvup, local_sem.at[8])
    own_state = pltpu.make_async_copy(start_ref.at[z], state, local_sem.at[9])
    up_wide = qup.shape[1]
    own_qup = pltpu.make_async_copy(qup_ref.at[:, at(z, up_wide)], qup, local_sem.at[10])
    own_kvd = pltpu.make_async_copy(wkvd_ref, kv_src.at[:, :kv_wide], local_sem.at[11])

    def norm_block(i):
        x = tok_all[i].astype(f32)
        scaled = x * lax.rsqrt(jnp.mean(x * x, axis=-1, keepdims=True) + EPSILON)
        normed[at(i), :] = (scaled * gain_ref[...]).astype(bf16)

    depth = fs * rows

    def multiply(u):
        weight, columns = (
            (w_lat, slice(None)) if u == LAT else (w_all, slice((u - 1) * WIDE, u * WIDE))
        )
        acc = acc_lat if u == LAT else acc_ret
        with jax.named_scope(f"multiply#u={u}"):
            acc[...] = jnp.dot(
                normed[:, :depth],
                weight[:depth, columns],
                preferred_element_type=f32,
            )

            def chunk(i, carry):
                begin = at(i, depth)
                acc[...] += jnp.dot(
                    normed[:, begin],
                    weight[begin, columns],
                    preferred_element_type=f32,
                )
                return carry

            lax.fori_loop(1, n_sp, chunk, 0)

    rd = RET_DIM // 2

    def finish_lat():
        def block(i, carry):
            lat_all[t, z - q_place, at(i), :kv_wide] = acc_lat[at(i), :kv_wide].astype(bf16)
            pair = acc_lat[at(i), kv_wide:]
            turned = pair * pcos_ref[at(i), :] + pltpu.roll(pair, ROPE_DIM, 1) * psin_ref[at(i), :]
            lane = lax.broadcasted_iota(jnp.int32, turned.shape, 1)
            turned = jnp.where(lane < ROPE_DIM, turned, pltpu.roll(turned, ROPE_DIM, 1))
            lat_all[t, z - q_place, at(i), kv_wide:] = jnp.where(
                z == kv_place, turned, pair
            ).astype(bf16)
            return carry

        lax.fori_loop(0, n_sp, block, 0)

    def finish_turned(dst, factor):
        def block(i, carry):
            cosine, sine = rcos_ref[at(i), :], rsin_ref[at(i), :]
            a, b = acc_ret[at(i), :rd], acc_ret[at(i), rd:]
            dst[at(i), :rd] = ((a * cosine - b * sine) * factor).astype(bf16)
            dst[at(i), rd:] = ((b * cosine + a * sine) * factor).astype(bf16)
            return carry

        lax.fori_loop(0, n_sp, block, 0)

    def project(u):
        for d in range(n_sp):
            arrive(d, u)
        multiply(u)
        if u == QUERY:
            finish_turned(ret_q, 1.0)
        elif u == KEY:
            finish_turned(ret_k, RET_DIM ** (-0.5))
        else:
            ret_v[...] = acc_ret[...].astype(bf16)

    r_iota = lax.broadcasted_iota(jnp.int32, (rows, rows), 0)
    c_iota = lax.broadcasted_iota(jnp.int32, (rows, rows), 1)

    def retention(b):
        rates = shift_all[b]
        pick = lax.broadcasted_iota(jnp.int32, rates.shape, 0) == z
        chosen = lax.broadcasted_iota(jnp.int32, rate_ref.shape, 1) == z
        rate = jnp.sum(jnp.where(chosen, rate_ref[...], 0.0), axis=1, keepdims=True)
        row = jnp.sum(jnp.where(pick, rates, 0.0), axis=0, keepdims=True) + rate
        column = jnp.sum(jnp.where(r_iota == c_iota, row, 0.0), axis=1, keepdims=True)
        c_col = jnp.sum(jnp.where(c_iota <= r_iota, row, 0.0), axis=1, keepdims=True)
        c_row = jnp.sum(jnp.where(r_iota <= c_iota, column, 0.0), axis=0, keepdims=True)
        last = jnp.sum(row, axis=1, keepdims=True)
        decay = jnp.exp(jnp.where(c_iota <= r_iota, c_col - c_row, -jnp.inf))
        block = slice(b * rows, (b + 1) * rows)
        q, k, v = ret_q[block, :], ret_k[block, :], ret_v[block, :]
        scores = lax.dot_general(q, k, CONTRACT, preferred_element_type=f32) * decay
        raw = jnp.dot(scores.astype(bf16), v, preferred_element_type=f32)
        carried = sum(
            jnp.dot(q, s, preferred_element_type=f32) for s in three_parts(state[...])
        )
        raw = raw + carried * jnp.exp(c_col)
        if b < n_sp - 1:
            weighted = k.astype(f32) * jnp.exp(last - c_col)
            added = sum(
                lax.dot_general(w, v, (((0,), (0,)), ((), ())), preferred_element_type=f32)
                for w in three_parts(weighted)
            )
            state[...] = jnp.exp(last) * state[...] + added
        centered = raw - jnp.mean(raw, axis=-1, keepdims=True)
        variance = jnp.mean(centered * centered, axis=-1, keepdims=True)
        merged[block, :WIDE] = (centered * lax.rsqrt(variance + EPSILON) * rgain_ref[z]).astype(
            bf16
        )

    att_heads = att_wide // (NOPE_DIM + VAL_DIM)

    def expand(i):
        def latent(slot, wide, gain):
            x = jnp.concatenate(
                [lat_all[core, slot, at(i), :wide] for core in range(2)], axis=1
            ).astype(f32)
            scaled = x * lax.rsqrt(jnp.mean(x * x, axis=-1, keepdims=True) + EPSILON)
            return (scaled * gain[...].reshape(1, wide * 2)).astype(bf16)

        query = jnp.dot(latent(0, q_wide, qgain_ref), qup[...], preferred_element_type=f32)
        first, middle, end = query[:, :128], query[:, 128:256], query[:, 256:]
        lane = lax.broadcasted_iota(jnp.int32, first.shape, 1)
        second = jnp.where(
            lane < ROPE_DIM, pltpu.roll(middle, ROPE_DIM, 1), pltpu.roll(end, ROPE_DIM, 1)
        )
        pair = jnp.where(lane < ROPE_DIM, middle, end)
        quarter = ROPE_DIM // 2
        swapped = jnp.where(
            lane % ROPE_DIM < quarter,
            pltpu.roll(pair, 2 * ROPE_DIM - quarter, 1),
            pltpu.roll(pair, quarter, 1),
        )
        qn[at(i), :NOPE_DIM] = first.astype(bf16)
        qn[at(i), NOPE_DIM:] = second.astype(bf16)
        qr[at(i), :] = (pair * pcos_ref[at(i), :] + swapped * psin_ref[at(i), :]).astype(bf16)
        expanded[at(i), :] = jnp.dot(
            latent(1, kv_wide, kvgain_ref), kvup[...], preferred_element_type=f32
        ).astype(bf16)
        rope_key[at(i), :] = lat_all[0, 1, at(i), kv_wide:]

    scale = (NOPE_DIM + ROPE_DIM) ** (-0.5)

    def attend(b):
        seen = (b + 1) * rows
        block = slice(b * rows, seen)
        q_at = lax.broadcasted_iota(jnp.int32, (rows, seen), 0) + b * rows
        k_at = lax.broadcasted_iota(jnp.int32, (rows, seen), 1)
        for h in range(att_heads):
            base = h * (NOPE_DIM + VAL_DIM)
            turned = qr[block, :]
            lane = lax.broadcasted_iota(jnp.int32, turned.shape, 1)
            turned = jnp.where(lane // ROPE_DIM == h, turned, jnp.zeros_like(turned))
            s = lax.dot_general(
                qn[block, h * NOPE_DIM : (h + 1) * NOPE_DIM],
                expanded[:seen, base : base + NOPE_DIM],
                CONTRACT,
                preferred_element_type=f32,
            ) + lax.dot_general(
                turned, rope_key[:seen, :], CONTRACT, preferred_element_type=f32
            )
            s = jnp.where(k_at <= q_at, s * scale, -jnp.inf)
            p = jnp.exp(s - jnp.max(s, axis=-1, keepdims=True))
            raw = jnp.dot(
                p.astype(bf16),
                expanded[:seen, base + NOPE_DIM : base + NOPE_DIM + VAL_DIM],
                preferred_element_type=f32,
            ) / jnp.sum(p, axis=-1, keepdims=True)
            scaled = raw * lax.rsqrt(jnp.mean(raw * raw, axis=-1, keepdims=True) + EPSILON)
            gain = again_ref[z][:, h * VAL_DIM : (h + 1) * VAL_DIM]
            merged[block, WIDE + h * VAL_DIM : WIDE + (h + 1) * VAL_DIM] = (
                scaled * gain
            ).astype(bf16)


    part_wide = out_ref.shape[1] // OUT_PARTS

    def out_place(j):
        depth_in = z + upper * (n_sp - 1 - 2 * z)
        found = (depth_in * 0 + 3, depth_in * 0 + 2, 1 - depth_in, depth_in)[j]
        return found + upper * (n_sp - 1 - 2 * found)

    def out_columns(c):
        return slice(c * part_wide, (c + 1) * part_wide)

    def pair_sum(j, c):
        return remote(
            pair_out.at[j, c], pair_in.at[j, c], o_send.at[j, c], o_recv.at[j, c], tp=other
        )

    def near_rows(j, c):
        return remote(
            row_out.at[j, c], row_in.at[0, c], r_send.at[j, c], r_recv.at[0, c], sp=out_place(j)
        )

    def far_rows(j, c):
        return remote(
            row_out.at[j, c],
            far_in.at[j, c],
            r_send.at[j, c],
            far_recv.at[j, c],
            sp=z + 1 - 2 * upper,
        )

    def sum_rows(j, c):
        return remote(
            row_out.at[j, c], row_in.at[1, c], r_send.at[j, c], r_recv.at[1, c], sp=out_place(j)
        )

    def rows_arrival(k, c):
        return remote(row_in.at[k, c], row_in.at[k, c], r_send.at[0, c], r_recv.at[k, c], tp=other)

    def project_out(j, c):
        first = slice(c * part_wide, (c + 1) * part_wide)
        got = lax.dot_general(
            merged[at(out_place(j)), :],
            w_all[first, (OUT_RET - 1) * WIDE :],
            CONTRACT,
            preferred_element_type=f32,
        )
        front, back = got[:half, :], got[half:, :]
        pair_out[j, c] = jnp.where(t == 0, back, front).astype(bf16)
        pair_sum(j, c).start()
        own_sum[j, :, out_columns(c)] = jnp.where(t == 0, front, back)

    def finish_out(j, c):
        with jax.named_scope("rows_pair"):
            pair_sum(j, c).wait_recv()
        total = own_sum[j, :, out_columns(c)] + pair_in[j, c].astype(f32)
        own_sum[j, :, out_columns(c)] = total
        if j == n_sp - 1:
            return

        def ship(copy):
            row_out[j, c] = total.astype(bf16)
            copy.start()

        if j == n_sp - 2:
            ship(near_rows(j, c))
        else:
            pl.when(is_end)(lambda: ship(far_rows(j, c)))

    def combine(j, c):
        with jax.named_scope("combine"):
            far_rows(j, c).wait_recv()
        total = own_sum[j, :, out_columns(c)] + far_in[j, c].astype(f32)
        row_out[j, c] = total.astype(bf16)
        sum_rows(j, c).start()


    def many(action, *pairs):
        for k, u in pairs:
            action(k, u)

    def norm_others():
        pair_arrive(tok_part, 0, False)
        for k in others:
            norm_block(origin_of(k))

    def send_near_end(u):
        for dest in (0, n_sp - 1):
            pl.when(direct(dest))(lambda dest=dest: z_copy(dest, u).start())

    def send_far_end(u):
        for dest in (0, n_sp - 1):
            pl.when((z - dest == 2) | (dest - z == 2))(lambda dest=dest: z_copy(dest, u).start())

    def send_middle(u):
        for dest in lat_sources:
            pl.when(z != dest)(lambda dest=dest: z_copy(dest, u).start())

    ret_weights = (QUERY, KEY, VALUE)
    out_weights = (OUT_RET, OUT_ATT)

    own_kvd.start()
    for copy in small_copies:
        copy.start()
    pl.when(~is_end)(lambda: line_start(tok_part, 0, tok_ref.at[mine]))

    @pl.when(z == q_place)
    def _():
        own_lat_copy(q_place).start()

    for u in ret_weights + out_weights:
        own_copy(u).start()
    send_lat(q_place)
    for u in ret_weights + out_weights:
        send_near_end(u)
    with jax.named_scope("kvsrc"):
        own_kvd.wait()
        for copy in small_copies:
            copy.wait()
    rope = rope_vmem[...].astype(f32).T.astype(bf16)
    kv_src[:, kv_wide:] = jnp.concatenate(
        [rope, rope[:, ROPE_DIM // 2 :], rope[:, : ROPE_DIM // 2]], axis=1
    )

    @pl.when(z == kv_place)
    def _():
        own_lat_copy(kv_place).start()

    send_lat(kv_place)

    @pl.when(is_end)
    def _():
        line_start(tok_part, 0, tok_ref.at[mine], (2, 1))
        for u in ret_weights:
            send(u)
        for u in out_weights:
            z_copy(origin_of(1), u).start()
        start_inputs()
        many(spread, (0, QUERY), (0, KEY), (0, VALUE), (0, OUT_RET), (0, OUT_ATT))
        own_tok.wait()
        norm_block(z)
        many(spread, (1, QUERY), (1, KEY))
        many(relay, (0, QUERY), (0, KEY))
        many(spread, (1, VALUE))
        many(relay, (0, VALUE))
        many(spread, (1, OUT_RET), (1, OUT_ATT))
        many(relay, (0, OUT_RET), (0, OUT_ATT))
        many(relay, (1, QUERY), (1, KEY))
        many(spread, (2, QUERY))
        many(relay, (1, VALUE))
        many(spread, (2, KEY))
        many(relay, (1, OUT_RET), (1, OUT_ATT))
        many(spread, (2, VALUE))
        many(relay, (2, QUERY), (2, KEY))
        many(spread, (3, QUERY))
        many(relay, (2, VALUE))
        many(spread, (3, KEY))
        many(relay, (3, QUERY))
        many(spread, (3, VALUE))
        many(relay, (3, KEY))
        line_pair(tok_part, 0)
        for u in out_weights:
            z_copy(origin_of(2), u).start()
            z_copy(origin_of(3), u).start()
        norm_others()
        wait_tables()
        project(QUERY)
        many(relay, (3, VALUE))
        project(KEY)

    @pl.when(~is_end)
    def _():
        for u in ret_weights:
            send_far_end(u)
        for u in ret_weights:
            send_middle(u)
        start_inputs()
        many(spread, (0, LAT), (0, QUERY), (0, KEY))
        many(relay, (0, LAT))
        many(spread, (2, LAT), (3, LAT), (0, VALUE))
        own_tok.wait()
        norm_block(z)
        many(relay, (0, QUERY), (0, KEY), (2, LAT))
        line_relay(tok_part, 0, 1)
        many(spread, (1, LAT), (0, OUT_RET), (0, OUT_ATT))
        many(relay, (3, LAT), (0, VALUE), (1, LAT))
        many(spread, (2, QUERY))
        line_relay(tok_part, 0, 2)
        line_pair(tok_part, 0)
        many(relay, (0, OUT_RET), (0, OUT_ATT))
        many(spread, (3, QUERY), (2, KEY))
        norm_others()
        many(relay, (2, QUERY))
        for k in range(n_sp):
            arrive(k, LAT)
        wait_tables()
        multiply(LAT)
        finish_lat()
        for i in range(LAT_PARTS):
            line_start(lat_part(i), i + 1)
        for i in range(LAT_PARTS):
            pair_own(lat_part(i), i + 1)
        for u in out_weights:
            send_middle(u)
            send_far_end(u)
        many(spread, (3, KEY), (2, VALUE), (1, QUERY))
        many(relay, (3, QUERY), (2, KEY))
        many(spread, (2, OUT_RET))
        many(relay, (3, KEY), (2, VALUE))
        many(spread, (1, KEY), (2, OUT_ATT))
        many(relay, (1, QUERY))
        many(spread, (3, VALUE))
        many(relay, (2, OUT_RET), (1, KEY))
        many(spread, (1, VALUE))
        line_relay(lat_part(0), 1, 1)
        line_pair(lat_part(0), 1)
        project(QUERY)
        many(relay, (2, OUT_ATT), (3, VALUE), (1, VALUE))
        line_relay(lat_part(1), 2, 1)
        line_pair(lat_part(1), 2)
        many(spread, (1, OUT_RET))
        project(KEY)
        many(spread, (3, OUT_RET), (1, OUT_ATT))

    project(VALUE)
    for d in others:
        shift_copy(d).wait_recv()
    own_shift.wait()
    own_state.wait()
    own_kvup.wait()
    own_qup.wait()
    pl.when(is_end)(lambda: many(spread, (2, OUT_RET)))
    pl.when(~is_end)(lambda: many(relay, (1, OUT_RET)))
    for b in range(n_sp):
        with jax.named_scope(f"retention#b={b}"):
            retention(b)

    @pl.when(is_end)
    def _():
        many(spread, (3, OUT_RET), (2, OUT_ATT))
        many(relay, (2, OUT_RET))
        many(spread, (3, OUT_ATT))

    @pl.when(~is_end)
    def _():
        many(spread, (3, OUT_ATT))
        many(relay, (3, OUT_RET), (1, OUT_ATT))

    blocks = n_sp // LAT_PARTS
    for i in range(LAT_PARTS):
        pl.when(is_end)(lambda i=i: line_pair(lat_part(i), i + 1))
        if i == 0:
            pl.when(is_end)(lambda: many(relay, (3, OUT_RET)))
        else:
            pl.when(is_end)(lambda: many(relay, (2, OUT_ATT)))
            many(relay, (3, OUT_ATT))
        pair_arrive(lat_part(i), i + 1, True)
        for b in range(i * blocks, (i + 1) * blocks):
            with jax.named_scope(f"expand#b={b}"):
                expand(b)
        for b in range(i * blocks, (i + 1) * blocks):
            with jax.named_scope(f"attend#b={b}"):
                attend(b)
    for u in out_weights:
        for k in range(n_sp):
            arrive(k, u)
    turns = [(j, c) for j in range(n_sp) for c in range(OUT_PARTS)]
    shared = [(j, c) for j in range(2) for c in range(OUT_PARTS)]
    for step, turn in enumerate(turns):
        with jax.named_scope(f"out#b={step}"):
            project_out(*turn)
        if step:
            finish_out(*turns[step - 1])
        if step >= LEAD and step - LEAD < len(shared):
            pl.when(~is_end)(lambda step=step: combine(*shared[step - LEAD]))
    finish_out(*turns[-1])

    @pl.when(~is_end)
    def _():
        for turn in shared[len(turns) - LEAD :]:
            combine(*turn)

    for c in range(OUT_PARTS):
        total = own_sum[n_sp - 1, :, out_columns(c)]
        for k in range(2):
            with jax.named_scope(f"rows#k={k}"):
                rows_arrival(k, c).wait_recv()
            total = total + row_in[k, c].astype(f32)
        out_ref[:, out_columns(c)] = total.astype(bf16)

    for u in range(UNITS):
        for k in range(n_sp):

            def drain(k=k, u=u):
                x_copy(k, u).wait_send()
                y_copy(k, u).wait_send()
                f_copy(k, u).wait_send()

            when(has(u, z), drain)
            if k and u != LAT:
                z_copy(origin_of(k), u).wait_send()
    for place in lat_sources:
        pl.when(z != place)(
            lambda place=place: z_copy(place, LAT, lat_sources[place]).wait_send()
        )
    for d in others:
        shift_copy(d).wait_send()
    line_drain(tok_part, 0, False)
    for i in range(LAT_PARTS):
        line_drain(lat_part(i), i + 1, True)
    for j in range(n_sp):
        for c in range(OUT_PARTS):
            pair_sum(j, c).wait_send()
            if j < n_sp - 1:
                near_rows(j, c).wait_send()


def heads_plan(
    tokens,
    norm_gain,
    w_ret_query,
    w_ret_key,
    w_ret_value,
    w_q_down,
    w_kv_down,
    w_rope_key,
    w_q_up,
    w_kv_up,
    q_lat_gain,
    kv_lat_gain,
    att_norm_gain,
    ret_norm_gain,
    w_ret_out,
    w_att_out,
    head_rate,
    decay_shift,
    start_state,
):
    n_sp = lax.axis_size("sp")
    rows, width = tokens.shape[1:]
    length = n_sp * rows
    q_wide, kv_wide = w_q_down.shape[1], w_kv_down.shape[1]
    w_rows = w_q_down.shape[0]
    att_heads = w_q_up.shape[1] // (NOPE_DIM + ROPE_DIM) // n_sp

    ret_cos, ret_sin = wave_tables(length, RET_DIM)
    rope_cos, rope_sin = wave_tables(length, ROPE_DIM)
    pair_cos = np.concatenate([rope_cos] * 4, axis=1)
    pair_sin = np.concatenate([-rope_sin, rope_sin] * 2, axis=1)
    small = (
        w_rope_key.T,
        head_rate[None],
        norm_gain[None],
        q_lat_gain,
        kv_lat_gain[None],
        att_norm_gain.reshape(n_sp, 1, -1),
        ret_norm_gain.reshape(n_sp, 1, -1),
        ret_cos,
        ret_sin,
        pair_cos,
        pair_sin,
    )
    dma = pltpu.SemaphoreType.DMA
    vmem = pltpu.VMEM
    f32, bf16 = jnp.float32, jnp.bfloat16
    half = rows // 2
    out_wide = 4 * n_sp * w_rows
    any_spec = pl.BlockSpec(memory_space=pl.ANY)
    vmem_spec = pl.BlockSpec(memory_space=pltpu.VMEM)
    mixed = pl.pallas_call(
        functools.partial(layer_kernel, n_sp, q_wide, kv_wide),
        out_shape=jax.ShapeDtypeStruct((half, out_wide), bf16),
        in_specs=[any_spec] * 23,
        out_specs=vmem_spec,
        scratch_shapes=[
            vmem((n_sp, rows, width), bf16),
            vmem((n_sp * 4 * w_rows, (UNITS - 1) * WIDE), bf16),
            vmem((n_sp * 4 * w_rows, q_wide), bf16),
            vmem((w_rows, q_wide), bf16),
            *[vmem(x.shape, x.dtype) for x in small],
            vmem((n_sp,) + decay_shift.shape[1:], f32),
            vmem((length, width), bf16),
            vmem((length, WIDE), f32),
            vmem((length, q_wide), f32),
            vmem((length, WIDE), bf16),
            vmem((length, WIDE), bf16),
            vmem((length, WIDE), bf16),
            vmem((2, 2, length, q_wide), bf16),
            vmem((RET_DIM, RET_DIM), f32),
            vmem((length, att_heads * NOPE_DIM), bf16),
            vmem((length, att_heads * ROPE_DIM), bf16),
            vmem((length, att_heads * (NOPE_DIM + VAL_DIM)), bf16),
            vmem((length, 2 * ROPE_DIM), bf16),
            vmem((w_kv_up.shape[0], att_heads * (NOPE_DIM + VAL_DIM)), bf16),
            vmem((w_q_up.shape[0], att_heads * (NOPE_DIM + ROPE_DIM)), bf16),
            vmem((length, WIDE + att_heads * VAL_DIM), bf16),
            vmem((n_sp, half, out_wide), f32),
            *[vmem((n_sp, OUT_PARTS, half, out_wide // OUT_PARTS), bf16)] * 2,
            vmem((n_sp - 1, OUT_PARTS, half, out_wide // OUT_PARTS), bf16),
            *[vmem((2, OUT_PARTS, half, out_wide // OUT_PARTS), bf16)] * 2,
            dma((12,)),
            *[dma((n_sp, UNITS))] * 8,
            *[dma((1, n_sp))] * 2,
            dma((len(small),)),
            *[dma((n_sp, OUT_PARTS))] * 5,
            *[dma((LAT_PARTS + 1, n_sp))] * 5,
        ],
        compiler_params=pltpu.CompilerParams(
            collective_id=0, has_side_effects=True, vmem_limit_bytes=62 * 1024 * 1024
        ),
    )(
        tokens[0],
        w_q_down,
        w_kv_down,
        w_ret_query,
        w_ret_key,
        w_ret_value,
        w_ret_out,
        w_att_out,
        small[0],
        decay_shift[0],
        *small[1:],
        w_q_up,
        w_kv_up,
        start_state[0],
    )
    return mixed[None]


def solution(mesh):
    placed = (
        P("fs", "sp", None),
        P(),
        P(("sp", "fs"), "tp"),
        P(("sp", "fs"), "tp"),
        P(("sp", "fs"), "tp"),
        P(("sp", "fs"), "tp"),
        P(("sp", "fs"), "tp"),
        P(("sp", "fs"), None),
        P(None, "tp"),
        P(None, "tp"),
        P(),
        P(),
        P("tp"),
        P("tp"),
        P(("sp", "fs"), "tp"),
        P(("sp", "fs"), "tp"),
        P("tp"),
        P("fs", "tp", "sp"),
        P("fs", "tp", None, None),
    )

    def pick(*args):
        if heads_fit(
            mesh, args[16].shape[0], args[0].shape[0], args[5].shape[1], args[6].shape[1], args[8].shape[1]
        ):
            return heads_plan(*args)
        return rows_plan(*args)

    return jax.shard_map(
        pick,
        mesh=mesh,
        in_specs=placed,
        out_specs=P("fs", ("sp", "tp"), None),
        check_vma=False,
    )
```

```python
import functools

import numpy as np

import jax
import jax.numpy as jnp
from jax import lax
from jax.experimental import pallas as pl
from jax.experimental.pallas import tpu as pltpu
from jax.sharding import PartitionSpec as P

RET_DIM = 256
NOPE_DIM = 128
ROPE_DIM = 64
VAL_DIM = 128
KV_LAT = 512


EPSILON = 1e-06
THETA_BASE = 10000.0
TOP_PRECISION = lax.Precision.HIGHEST


def prefix(x, axis, combine, identity):
    peers, position = (lax.axis_size(axis), lax.axis_index(axis))
    everything = jax.tree.map(
        lambda part, kind: lax.all_gather(part.astype(kind), axis), x, (jnp.bfloat16, jnp.bfloat16)
    )
    start = jax.tree.map(
        lambda part, zero: jnp.broadcast_to(jnp.asarray(zero, part.dtype), part.shape), x, identity
    )

    def lap(k, before):
        reached = k < position
        new = combine(
            before, jax.tree.map(lambda part, own: part[k].astype(own.dtype), everything, x)
        )
        return jax.tree.map(lambda a, b: jnp.where(reached, a, b), new, before)

    return lax.fori_loop(0, peers, lap, start)


def angle_tables(positions, rot_width):
    half_width = rot_width // 2
    inverse = THETA_BASE ** (-jnp.arange(half_width, dtype=jnp.float32) * 2.0 / rot_width)
    angles = positions.astype(jnp.float32)[:, None] * inverse[None, :]
    return (jnp.cos(angles), jnp.sin(angles))


def rotate(values, cosine, sine):
    half_width = values.shape[-1] // 2
    front_half = values[..., :half_width]
    back_half = values[..., half_width:]
    return jnp.concatenate(
        [front_half * cosine - back_half * sine, back_half * cosine + front_half * sine], axis=-1
    )


def rms_scale(values, gain_vector):
    return (
        values
        * lax.rsqrt(jnp.mean(values * values, axis=-1, keepdims=True) + EPSILON)
        * gain_vector
    )


def chain_states(earlier, later):
    early_log, early_state = earlier
    late_log, late_state = later
    return (early_log + late_log, jnp.exp(late_log)[:, None, None] * early_state + late_state)


def rows_plan(
    tokens,
    norm_gain,
    w_ret_query,
    w_ret_key,
    w_ret_value,
    w_q_down,
    w_kv_down,
    w_rope_key,
    w_q_up,
    w_kv_up,
    q_lat_gain,
    kv_lat_gain,
    att_norm_gain,
    ret_norm_gain,
    w_ret_out,
    w_att_out,
    head_rate,
    decay_shift,
    start_state,
):
    tok_rows = tokens.shape[1]
    ret_local = head_rate.shape[0]
    att_local = w_q_up.shape[1] // (NOPE_DIM + ROPE_DIM)
    row_offset = lax.axis_index("sp") * tok_rows
    positions = row_offset + jnp.arange(tok_rows, dtype=jnp.int32)
    (
        full_query,
        full_key,
        full_value,
        full_q_down,
        full_kv_down,
        full_rope,
        full_ret_out,
        full_att_out,
    ) = (
        lax.all_gather(w_ret_query, ("sp", "fs"), axis=0, tiled=True),
        lax.all_gather(w_ret_key, ("sp", "fs"), axis=0, tiled=True),
        lax.all_gather(w_ret_value, ("sp", "fs"), axis=0, tiled=True),
        lax.all_gather(w_q_down, ("sp", "fs"), axis=0, tiled=True),
        lax.all_gather(w_kv_down, ("sp", "fs"), axis=0, tiled=True),
        lax.all_gather(w_rope_key, ("sp", "fs"), axis=0, tiled=True),
        lax.all_gather(w_ret_out, ("sp", "fs"), axis=0, tiled=True),
        lax.all_gather(w_att_out, ("sp", "fs"), axis=0, tiled=True),
    )
    source = tokens[0].astype(jnp.float32)
    normed = rms_scale(source, norm_gain).astype(jnp.bfloat16)
    ret_cos, ret_sin = angle_tables(positions, RET_DIM)
    rope_cos, rope_sin = angle_tables(positions, ROPE_DIM)

    def project(weight):
        return jnp.dot(normed, weight, preferred_element_type=jnp.float32)

    part_q = project(full_q_down).astype(jnp.bfloat16)
    part_kv = project(full_kv_down).astype(jnp.bfloat16)
    lat_q_raw, lat_kv_raw = (
        lax.all_gather(part_q, "tp", axis=1, tiled=True),
        lax.all_gather(part_kv, "tp", axis=1, tiled=True),
    )
    retention_query = rotate(
        project(full_query).reshape(tok_rows, ret_local, RET_DIM),
        ret_cos[:, None],
        ret_sin[:, None],
    ).astype(jnp.bfloat16)
    retention_key = (
        rotate(
            project(full_key).reshape(tok_rows, ret_local, RET_DIM),
            ret_cos[:, None],
            ret_sin[:, None],
        )
        * RET_DIM ** (-0.5)
    ).astype(jnp.bfloat16)
    retention_value = project(full_value).reshape(tok_rows, ret_local, RET_DIM).astype(jnp.bfloat16)
    rope_key = rotate(project(full_rope), rope_cos, rope_sin).astype(jnp.bfloat16)
    log_rates = head_rate[:, None] + decay_shift[0]
    cumul = jnp.cumsum(log_rates, axis=1)
    offsets = jnp.arange(tok_rows, dtype=jnp.int32)
    lower_mask = offsets[None, :] <= offsets[:, None]
    decay_matrix = jnp.exp(
        jnp.where(lower_mask[None], cumul[:, :, None] - cumul[:, None, :], -jnp.inf)
    )
    block_score_grid = (
        jnp.einsum(
            "zgq,ugq->gzu", retention_query, retention_key, preferred_element_type=jnp.float32
        )
        * decay_matrix
    ).astype(jnp.bfloat16)
    inside_block_output = jnp.einsum(
        "vzs,svp->zvp", block_score_grid, retention_value, preferred_element_type=jnp.float32
    )
    block_output_sum = cumul[:, -1]
    weighted_values = (
        retention_key.astype(jnp.float32) * jnp.exp(block_output_sum[:, None] - cumul).T[:, :, None]
    )
    contribution = jnp.einsum(
        "uzj,uzv->zjv",
        weighted_values,
        retention_value.astype(jnp.float32),
        precision=TOP_PRECISION,
    )
    identity = (jnp.zeros_like(block_output_sum), jnp.zeros_like(contribution))
    before_log, before_state = prefix(
        (block_output_sum, contribution), "sp", chain_states, identity
    )
    q_latent = rms_scale(lat_q_raw.astype(jnp.float32), q_lat_gain).astype(jnp.bfloat16)
    kv_latent = rms_scale(lat_kv_raw.astype(jnp.float32), kv_lat_gain).astype(jnp.bfloat16)
    query_full = jnp.dot(q_latent, w_q_up, preferred_element_type=jnp.float32).reshape(
        tok_rows, att_local, NOPE_DIM + ROPE_DIM
    )
    query_nope = query_full[..., :NOPE_DIM].astype(jnp.bfloat16)
    query_rope = rotate(query_full[..., NOPE_DIM:], rope_cos[:, None], rope_sin[:, None]).astype(
        jnp.bfloat16
    )
    att_scale = (NOPE_DIM + ROPE_DIM) ** (-0.5)

    def attend(carry, key_nope, key_values, key_rope, start):
        running_max, running_sum, running_acc = carry
        key_count = key_rope.shape[0]
        score_matrix = (
            jnp.einsum("qhd,khd->hqk", query_nope, key_nope, preferred_element_type=jnp.float32)
            + jnp.einsum("qhd,kd->hqk", query_rope, key_rope, preferred_element_type=jnp.float32)
        ) * att_scale
        key_positions = start + jnp.arange(key_count, dtype=jnp.int32)
        allowed = key_positions[None, :] <= positions[:, None]
        masked = jnp.where(allowed[None], score_matrix, -jnp.inf)
        new_max = jnp.maximum(running_max, jnp.max(masked, axis=-1))
        safe_max = jnp.where(jnp.isfinite(new_max), new_max, 0.0)
        weights = jnp.exp(masked - safe_max[..., None])
        rescale = jnp.exp(running_max - safe_max)
        new_sum = running_sum * rescale + jnp.sum(weights, axis=-1)
        new_acc = running_acc * rescale[..., None] + jnp.einsum(
            "hqk,khd->hqd",
            weights.astype(jnp.bfloat16),
            key_values,
            preferred_element_type=jnp.float32,
        )
        return (new_max, new_sum, new_acc)

    def expand_attend(carry_in, lat_piece, rope_piece, start):
        wide = (
            jnp.dot(lat_piece, w_kv_up, preferred_element_type=jnp.float32)
            .astype(jnp.bfloat16)
            .reshape(rope_piece.shape[0], att_local, NOPE_DIM + VAL_DIM)
        )
        return attend(carry_in, wide[..., :NOPE_DIM], wide[..., NOPE_DIM:], rope_piece, start)

    empty = (
        jnp.full((att_local, tok_rows), -jnp.inf, jnp.float32),
        jnp.zeros((att_local, tok_rows), jnp.float32),
        jnp.zeros((att_local, tok_rows, VAL_DIM), jnp.float32),
    )
    groups = lax.axis_size("tp")
    kv_part = KV_LAT // groups
    rope_part = ROPE_DIM // groups
    my_group = lax.axis_index("tp")
    joined = jnp.concatenate(
        [
            lax.dynamic_slice_in_dim(kv_latent, my_group * kv_part, kv_part, 1),
            lax.dynamic_slice_in_dim(rope_key, my_group * rope_part, rope_part, 1),
        ],
        axis=1,
    )
    all_rows = lax.all_gather(joined, "sp", axis=0, tiled=True)
    complete = lax.all_gather(all_rows, "tp", axis=1, tiled=True)
    total_rows = complete.shape[0]
    grouped = complete.reshape(total_rows, groups, kv_part + rope_part)
    lat_all = grouped[:, :, :kv_part].reshape(total_rows, KV_LAT)
    rope_all = grouped[:, :, kv_part:].reshape(total_rows, ROPE_DIM)

    def visit(block_index, carry_in):
        start = block_index * tok_rows
        lat_piece = lax.dynamic_slice_in_dim(lat_all, start, tok_rows, 0)
        rope_piece = lax.dynamic_slice_in_dim(rope_all, start, tok_rows, 0)
        return expand_attend(carry_in, lat_piece, rope_piece, start)

    final = lax.fori_loop(0, lax.axis_index("sp") + 1, visit, empty)
    att_raw = jnp.transpose(final[2] / final[1][..., None], (1, 0, 2))
    att_out = (
        rms_scale(att_raw, att_norm_gain.reshape(att_local, VAL_DIM))
        .astype(jnp.bfloat16)
        .reshape(tok_rows, att_local * VAL_DIM)
    )
    entering = jnp.exp(before_log)[:, None, None] * start_state[0] + before_state
    carried_term = (
        jnp.einsum(
            "nhd,hde->nhe", retention_query.astype(jnp.float32), entering, precision=TOP_PRECISION
        )
        * jnp.exp(cumul).T[:, :, None]
    )
    ret_raw = inside_block_output + carried_term
    row_mean = jnp.mean(ret_raw, axis=-1, keepdims=True)
    centered = ret_raw - row_mean
    row_var = jnp.mean(centered * centered, axis=-1, keepdims=True)
    ret_out = (
        (centered * lax.rsqrt(row_var + EPSILON) * ret_norm_gain.reshape(ret_local, RET_DIM))
        .astype(jnp.bfloat16)
        .reshape(tok_rows, ret_local * RET_DIM)
    )
    contract = (((1,), (1,)), ((), ()))
    mixed = lax.psum_scatter(
        (
            lax.dot_general(ret_out, full_ret_out, contract, preferred_element_type=jnp.float32)
            + lax.dot_general(att_out, full_att_out, contract, preferred_element_type=jnp.float32)
        ).astype(jnp.bfloat16),
        "tp",
        scatter_dimension=0,
        tiled=True,
    )
    return mixed[None]


MESH = pl.DeviceIdType.MESH
WIDE = RET_DIM
CONTRACT = (((1,), (1,)), ((), ()))
UNITS = 7
LAT, QUERY, KEY, VALUE, OUT_RET, OUT_ATT, OUT_ATT2 = range(UNITS)
LAT_PARTS = 2
OUT_PARTS = 2


def heads_fit(mesh, ret_local, sequences, q_wide, kv_wide, up_wide):
    sizes = mesh.shape
    return (
        sizes["sp"] == 4
        and sizes["fs"] == 4
        and sizes["tp"] == 2
        and ret_local == sizes["sp"]
        and sequences == 1
        and up_wide == 2 * (NOPE_DIM + ROPE_DIM) * ret_local
        and q_wide % 128 == 0
        and kv_wide % 128 == 0
        and q_wide == kv_wide + 2 * ROPE_DIM
    )


def wave_tables(length, wide):
    half_wide = wide // 2
    powers = np.arange(half_wide, dtype=np.float32) * np.float32(2.0 / wide)
    inverse = np.power(np.float32(THETA_BASE), -powers).astype(np.float32)
    angles = np.arange(length, dtype=np.float32)[:, None] * inverse[None, :]
    return np.cos(angles), np.sin(angles)


def three_parts(x):
    high = x.astype(jnp.bfloat16)
    rest = x - high.astype(jnp.float32)
    middle = rest.astype(jnp.bfloat16)
    low = (rest - middle.astype(jnp.float32)).astype(jnp.bfloat16)
    return high, middle, low


def layer_kernel(
    n_sp,
    q_wide,
    kv_wide,
    tok_ref,
    wqd_ref,
    wkvd_ref,
    wq_ref,
    wk_ref,
    wv_ref,
    wr_ref,
    wa_ref,
    rope_hbm,
    shift_ref,
    rate_hbm,
    gain_hbm,
    qgain_hbm,
    kvgain_hbm,
    again_hbm,
    rgain_hbm,
    rcos_hbm,
    rsin_hbm,
    pcos_hbm,
    psin_hbm,
    qup_ref,
    kvup_ref,
    start_ref,
    out_ref,
    tok_all,
    w_all,
    w_lat,
    kv_src,
    rope_vmem,
    rate_ref,
    gain_ref,
    qgain_ref,
    kvgain_ref,
    again_ref,
    rgain_ref,
    rcos_ref,
    rsin_ref,
    pcos_ref,
    psin_ref,
    shift_all,
    normed,
    acc_ret,
    acc_lat,
    ret_q,
    ret_k,
    ret_v,
    lat_all,
    state,
    qn,
    qr,
    expanded,
    rope_key,
    kvup,
    qup,
    merged,
    own_sum,
    pair_out,
    pair_in,
    row_out,
    row_in,
    far_in,
    local_sem,
    z_send,
    z_recv,
    x_send,
    x_recv,
    y_send,
    y_recv,
    f_send,
    f_recv,
    m_send,
    m_recv,
    small_sem,
    o_send,
    o_recv,
    r_send,
    r_recv,
    far_recv,
    l_send,
    l_recv,
    l_relay,
    p_send,
    p_recv,
):
    z, f, t = lax.axis_index("sp"), lax.axis_index("fs"), lax.axis_index("tp")
    xn = f + 1 - 2 * (f % 2)
    yn = (f + 2) % 4
    other = 1 - t
    fs = 4
    rows = tok_ref.shape[0]
    length = n_sp * rows
    half = rows // 2
    weights = (None, wq_ref, wk_ref, wv_ref, wr_ref, wa_ref, wa_ref)
    f32, bf16 = jnp.float32, jnp.bfloat16
    q_place, kv_place = 0, n_sp - 1
    att_first = n_sp // 2 - 1
    middles = (att_first, att_first + 1)
    others = range(1, n_sp)

    def remote(src, dst, send, recv, **where):
        return pltpu.make_async_remote_copy(
            src_ref=src,
            dst_ref=dst,
            send_sem=send,
            recv_sem=recv,
            device_id={"sp": z, "fs": f, "tp": t, **where},
            device_id_type=MESH,
        )

    barrier = pltpu.get_barrier_semaphore()
    peers = [{"sp": (z + d) % n_sp, "fs": f, "tp": t} for d in others]
    peers += [{"sp": z, "fs": xn, "tp": t}, {"sp": z, "fs": yn, "tp": t}]
    peers += [{"sp": z, "fs": f, "tp": other}]
    for peer in peers:
        pl.semaphore_signal(barrier, inc=1, device_id=peer, device_id_type=MESH)
    with jax.named_scope("barrier"):
        pl.semaphore_wait(barrier, len(peers))

    def at(i, size=rows):
        if isinstance(i, int):
            return slice(i * size, (i + 1) * size)
        return pl.ds(pl.multiple_of(i * size, size), size)

    upper = z // (n_sp // 2)
    is_end = (z == 0) | (z == n_sp - 1)

    def origin_of(k):
        depth_in = z + upper * (n_sp - 1 - 2 * z)
        found = (depth_in * 0, 1 + depth_in, 2 - 2 * depth_in, depth_in * 0 + 3)[k]
        return z if k == 0 else found + upper * (n_sp - 1 - 2 * found)


    def piece(u, dest):
        column = dest if u < OUT_ATT else 2 * (dest - att_first) + u - OUT_ATT
        return weights[u].at[:, at(column, WIDE)]

    def part(owner_z, owner_f, u):
        where = at(owner_z * fs + owner_f)
        if u == LAT:
            return w_lat.at[where]
        return w_all.at[where, (u - 1) * WIDE : u * WIDE]

    def has(u, place):
        edge = (place == q_place) | (place == kv_place)
        return edge if u == LAT else ~edge if u >= OUT_ATT else True

    def when(condition, action):
        if condition is True:
            action()
        else:
            pl.when(condition)(action)

    lat_sources = {q_place: wqd_ref, kv_place: kv_src}

    def z_copy(to, u, src=None):
        return remote(
            piece(u, to) if src is None else src,
            part(z, f, u),
            z_send.at[to, u],
            z_recv.at[z, u],
            sp=to,
        )

    def z_arrival(k, u):
        ref = part(origin_of(k), f, u)
        return remote(ref, ref, z_send.at[z, u], z_recv.at[origin_of(k), u], tp=other)

    def x_copy(k, u):
        ref = part(origin_of(k), f, u)
        return remote(ref, ref, x_send.at[k, u], x_recv.at[k, u], fs=xn)

    def y_copy(k, u):
        ref = part(origin_of(k), f, u)
        return remote(ref, ref, y_send.at[k, u], y_recv.at[k, u], fs=yn)

    def f_copy(k, u):
        source, to = (xn, yn) if (k + u) % 2 == 0 else (yn, xn)
        ref = part(origin_of(k), source, u)
        return remote(ref, ref, f_send.at[k, u], f_recv.at[k, u], fs=to)

    def own_copy(u):
        return pltpu.make_async_copy(piece(u, z), part(z, f, u), local_sem.at[u])

    def own_lat_copy(place):
        return pltpu.make_async_copy(lat_sources[place], part(z, f, LAT), local_sem.at[LAT])

    def send(u, *to):
        for k in to or others:
            when(has(u, origin_of(k)), lambda k=k: z_copy(origin_of(k), u).start())

    def send_lat(place):
        pl.when(z != place)(lambda: z_copy(place, LAT, lat_sources[place]).start())

    def spread(d, u):
        def action():
            with jax.named_scope(f"spread#d={d}#u={u}"):
                if d:
                    z_arrival(d, u).wait_recv()
                elif u == LAT:
                    own_lat_copy(q_place).wait()
                else:
                    own_copy(u).wait()
            x_copy(d, u).start()
            y_copy(d, u).start()

        when(has(u, z), action)

    def relay(d, u):
        def action():
            with jax.named_scope(f"relay#d={d}#u={u}"):
                (x_copy if (d + u) % 2 == 0 else y_copy)(d, u).wait_recv()
            f_copy(d, u).start()

        when(has(u, z), action)

    def arrive(d, u):
        def action():
            with jax.named_scope(f"arrive#d={d}#u={u}"):
                (y_copy if (d + u) % 2 == 0 else x_copy)(d, u).wait_recv()
                f_copy(d, u).wait_recv()

        when(has(u, z), action)


    mine = pl.ds(pl.multiple_of(t * half, half), half)

    def tok_part(origin):
        return tok_all.at[origin, mine]

    lat_rows = length // LAT_PARTS

    def lat_part(i):
        return lambda origin: lat_all.at[t, origin // (n_sp - 1), pl.ds(i * lat_rows, lat_rows)]

    def line_copy(where, row, dest, src=None):
        return remote(
            where(z) if src is None else src,
            where(z),
            l_send.at[row, dest],
            l_recv.at[row, z],
            sp=dest,
        )

    def relay_copy(where, row, origin, dest):
        ref = where(origin)
        return remote(ref, ref, l_relay.at[row, origin], l_recv.at[row, origin], sp=dest)

    def pair_copy(where, row, origin):
        ref = where(origin)
        return remote(ref, ref, p_send.at[row, origin], p_recv.at[row, origin], tp=other)

    def direct(dest):
        near = (z - dest == 1) | (dest - z == 1)
        return near if dest in (0, n_sp - 1) else z != dest

    def line_start(where, row, src=None, distances=others):
        for distance in distances:
            for dest in range(n_sp):
                condition = direct(dest) & ((z - dest == distance) | (dest - z == distance))
                pl.when(condition)(
                    lambda dest=dest: line_copy(where, row, dest, src).start()
                )

    ends = ((1, 0), (n_sp - 2, n_sp - 1))

    def line_relay(where, row, distance):
        for middle, dest in ends:
            origin = middle + (middle - dest) * distance

            @pl.when(z == middle)
            def _(origin=origin, dest=dest):
                with jax.named_scope(f"line#r={row}#k={distance}"):
                    relay_copy(where, row, origin, dest).wait_recv()
                relay_copy(where, row, origin, dest).start()

    def was_relayed(origin):
        return z == (n_sp - 2 if origin < n_sp // 2 else 1)

    def line_pair(where, row):
        for distance in others:
            for origin in range(n_sp):
                here = (z - origin == distance) | (origin - z == distance)

                @pl.when(here)
                def _(origin=origin):
                    with jax.named_scope(f"pass#r={row}#k={distance}"):
                        pl.when(~was_relayed(origin))(
                            lambda: relay_copy(where, row, origin, 0).wait_recv()
                        )
                    pair_copy(where, row, origin).start()

    def pair_arrive(where, row):
        with jax.named_scope(f"pair#r={row}"):
            for origin in range(n_sp):
                pl.when(origin != z)(
                    lambda origin=origin: pair_copy(where, row, origin).wait_recv()
                )

    def line_drain(where, row):
        for dest in range(n_sp):
            pl.when(direct(dest))(lambda dest=dest: line_copy(where, row, dest).wait_send())
        for middle, dest in ends:
            for distance in range(1, n_sp - 1):
                origin = middle + (middle - dest) * distance
                pl.when(z == middle)(
                    lambda origin=origin, dest=dest: relay_copy(
                        where, row, origin, dest
                    ).wait_send()
                )
        for origin in range(n_sp):
            pl.when(origin != z)(
                lambda origin=origin: pair_copy(where, row, origin).wait_send()
            )


    near_end, far_end = upper * (n_sp - 1), (1 - upper) * (n_sp - 1)

    def lat_copy(i, origin, to):
        ref = lat_part(i)(origin)
        return remote(ref, ref, l_send.at[i + 1, 0], l_recv.at[i + 1, origin], sp=to)

    def lat_send(i):
        return lat_copy(i, z, z + 1 - 2 * upper)

    def lat_forward(i):
        with jax.named_scope(f"latnear#i={i}"):
            lat_copy(i, near_end, z).wait_recv()
        lat_copy(i, near_end, n_sp - 1 - z).start()
        pair_copy(lat_part(i), i + 1, near_end).start()

    def lat_far(i):
        with jax.named_scope(f"latfar#i={i}"):
            lat_copy(i, far_end, z).wait_recv()
        pair_copy(lat_part(i), i + 1, far_end).start()

    def lat_arrive(i):
        with jax.named_scope(f"latpair#i={i}"):
            for origin in (q_place, kv_place):
                pair_copy(lat_part(i), i + 1, origin).wait_recv()

    def shift_copy(d):
        to = (z + d) % n_sp
        return remote(shift_ref, shift_all.at[z], m_send.at[0, d], m_recv.at[0, d], sp=to)


    staged = (
        (rope_hbm, rope_vmem),
        (rate_hbm, rate_ref),
        (gain_hbm, gain_ref),
        (qgain_hbm, qgain_ref),
        (kvgain_hbm, kvgain_ref),
        (again_hbm, again_ref),
        (rgain_hbm, rgain_ref),
        (rcos_hbm, rcos_ref),
        (rsin_hbm, rsin_ref),
        (pcos_hbm, pcos_ref),
        (psin_hbm, psin_ref),
    )
    staged_copies = [
        pltpu.make_async_copy(src, dst, small_sem.at[i]) for i, (src, dst) in enumerate(staged)
    ]
    small_copies, table_copies = staged_copies[:7], staged_copies[7:]

    def wait_tables():
        for copy in table_copies:
            copy.wait()

    def start_inputs():
        for copy in table_copies:
            copy.start()
        own_tok.start()
        own_shift.start()

        @pl.when(~is_end)
        def _():
            own_kvup.start()
            own_qup.start()

        own_state.start()
        for d in others:
            shift_copy(d).start()

    own_tok = pltpu.make_async_copy(tok_ref, tok_all.at[z], local_sem.at[12])
    own_shift = pltpu.make_async_copy(shift_ref, shift_all.at[z], local_sem.at[13])
    att_wide = kvup.shape[1]
    own_kvup = pltpu.make_async_copy(kvup_ref.at[:, at(z - att_first, att_wide)], kvup, local_sem.at[8])
    own_state = pltpu.make_async_copy(start_ref.at[z], state, local_sem.at[9])
    up_wide = qup.shape[1]
    own_qup = pltpu.make_async_copy(qup_ref.at[:, at(z - att_first, up_wide)], qup, local_sem.at[10])
    own_kvd = pltpu.make_async_copy(wkvd_ref, kv_src.at[:, :kv_wide], local_sem.at[11])

    def norm_block(i):
        x = tok_all[i].astype(f32)
        scaled = x * lax.rsqrt(jnp.mean(x * x, axis=-1, keepdims=True) + EPSILON)
        normed[at(i), :] = (scaled * gain_ref[...]).astype(bf16)

    depth = fs * rows

    def multiply(u):
        weight, columns = (
            (w_lat, slice(None)) if u == LAT else (w_all, slice((u - 1) * WIDE, u * WIDE))
        )
        acc = acc_lat if u == LAT else acc_ret
        with jax.named_scope(f"multiply#u={u}"):
            acc[...] = jnp.dot(
                normed[:, :depth],
                weight[:depth, columns],
                preferred_element_type=f32,
            )

            def chunk(i, carry):
                begin = at(i, depth)
                acc[...] += jnp.dot(
                    normed[:, begin],
                    weight[begin, columns],
                    preferred_element_type=f32,
                )
                return carry

            lax.fori_loop(1, n_sp, chunk, 0)

    rd = RET_DIM // 2

    def finish_lat():
        def block(i, carry):
            lat_all[t, upper, at(i), :kv_wide] = acc_lat[at(i), :kv_wide].astype(bf16)
            pair = acc_lat[at(i), kv_wide:]
            turned = pair * pcos_ref[at(i), :] + pltpu.roll(pair, ROPE_DIM, 1) * psin_ref[at(i), :]
            lane = lax.broadcasted_iota(jnp.int32, turned.shape, 1)
            turned = jnp.where(lane < ROPE_DIM, turned, pltpu.roll(turned, ROPE_DIM, 1))
            lat_all[t, upper, at(i), kv_wide:] = jnp.where(
                z == kv_place, turned, pair
            ).astype(bf16)
            return carry

        lax.fori_loop(0, n_sp, block, 0)

    def finish_turned(dst, factor):
        def block(i, carry):
            cosine, sine = rcos_ref[at(i), :], rsin_ref[at(i), :]
            a, b = acc_ret[at(i), :rd], acc_ret[at(i), rd:]
            dst[at(i), :rd] = ((a * cosine - b * sine) * factor).astype(bf16)
            dst[at(i), rd:] = ((b * cosine + a * sine) * factor).astype(bf16)
            return carry

        lax.fori_loop(0, n_sp, block, 0)

    def project(u):
        for d in range(n_sp):
            arrive(d, u)
        multiply(u)
        if u == QUERY:
            finish_turned(ret_q, 1.0)
        elif u == KEY:
            finish_turned(ret_k, RET_DIM ** (-0.5))
        else:
            ret_v[...] = acc_ret[...].astype(bf16)

    r_iota = lax.broadcasted_iota(jnp.int32, (rows, rows), 0)
    c_iota = lax.broadcasted_iota(jnp.int32, (rows, rows), 1)

    def retention(b):
        rates = shift_all[b]
        pick = lax.broadcasted_iota(jnp.int32, rates.shape, 0) == z
        chosen = lax.broadcasted_iota(jnp.int32, rate_ref.shape, 1) == z
        rate = jnp.sum(jnp.where(chosen, rate_ref[...], 0.0), axis=1, keepdims=True)
        row = jnp.sum(jnp.where(pick, rates, 0.0), axis=0, keepdims=True) + rate
        column = jnp.sum(jnp.where(r_iota == c_iota, row, 0.0), axis=1, keepdims=True)
        c_col = jnp.sum(jnp.where(c_iota <= r_iota, row, 0.0), axis=1, keepdims=True)
        c_row = jnp.sum(jnp.where(r_iota <= c_iota, column, 0.0), axis=0, keepdims=True)
        last = jnp.sum(row, axis=1, keepdims=True)
        decay = jnp.exp(jnp.where(c_iota <= r_iota, c_col - c_row, -jnp.inf))
        block = slice(b * rows, (b + 1) * rows)
        q, k, v = ret_q[block, :], ret_k[block, :], ret_v[block, :]
        scores = lax.dot_general(q, k, CONTRACT, preferred_element_type=f32) * decay
        raw = jnp.dot(scores.astype(bf16), v, preferred_element_type=f32)
        carried = sum(
            jnp.dot(q, s, preferred_element_type=f32) for s in three_parts(state[...])
        )
        raw = raw + carried * jnp.exp(c_col)
        if b < n_sp - 1:
            weighted = k.astype(f32) * jnp.exp(last - c_col)
            added = sum(
                lax.dot_general(w, v, (((0,), (0,)), ((), ())), preferred_element_type=f32)
                for w in three_parts(weighted)
            )
            state[...] = jnp.exp(last) * state[...] + added
        centered = raw - jnp.mean(raw, axis=-1, keepdims=True)
        variance = jnp.mean(centered * centered, axis=-1, keepdims=True)
        merged[block, :WIDE] = (centered * lax.rsqrt(variance + EPSILON) * rgain_ref[z]).astype(
            bf16
        )

    att_heads = att_wide // (NOPE_DIM + VAL_DIM)

    def expand(i):
        def latent(slot, wide, gain):
            x = jnp.concatenate(
                [lat_all[core, slot, at(i), :wide] for core in range(2)], axis=1
            ).astype(f32)
            scaled = x * lax.rsqrt(jnp.mean(x * x, axis=-1, keepdims=True) + EPSILON)
            return (scaled * gain[...].reshape(1, wide * 2)).astype(bf16)

        query = jnp.dot(latent(0, q_wide, qgain_ref), qup[...], preferred_element_type=f32)
        for pair_at in range(att_heads // 2):
            lanes = query[:, pair_at * 384 : (pair_at + 1) * 384]
            first, middle, end = lanes[:, :128], lanes[:, 128:256], lanes[:, 256:]
            lane = lax.broadcasted_iota(jnp.int32, first.shape, 1)
            second = jnp.where(
                lane < ROPE_DIM, pltpu.roll(middle, ROPE_DIM, 1), pltpu.roll(end, ROPE_DIM, 1)
            )
            pair = jnp.where(lane < ROPE_DIM, middle, end)
            quarter = ROPE_DIM // 2
            swapped = jnp.where(
                lane % ROPE_DIM < quarter,
                pltpu.roll(pair, 2 * ROPE_DIM - quarter, 1),
                pltpu.roll(pair, quarter, 1),
            )
            base = 2 * pair_at * NOPE_DIM
            qn[at(i), base : base + NOPE_DIM] = first.astype(bf16)
            qn[at(i), base + NOPE_DIM : base + 2 * NOPE_DIM] = second.astype(bf16)
            qr[at(i), pair_at * 128 : (pair_at + 1) * 128] = (
                pair * pcos_ref[at(i), :] + swapped * psin_ref[at(i), :]
            ).astype(bf16)
        expanded[at(i), :] = jnp.dot(
            latent(1, kv_wide, kvgain_ref), kvup[...], preferred_element_type=f32
        ).astype(bf16)
        rope_key[at(i), :] = lat_all[0, 1, at(i), kv_wide:]

    scale = (NOPE_DIM + ROPE_DIM) ** (-0.5)

    def attend(b):
        seen = (b + 1) * rows
        block = slice(b * rows, seen)
        q_at = lax.broadcasted_iota(jnp.int32, (rows, seen), 0) + b * rows
        k_at = lax.broadcasted_iota(jnp.int32, (rows, seen), 1)
        for h in range(att_heads):
            base = h * (NOPE_DIM + VAL_DIM)
            turned = qr[block, h // 2 * 128 : (h // 2 + 1) * 128]
            lane = lax.broadcasted_iota(jnp.int32, turned.shape, 1)
            turned = jnp.where(lane // ROPE_DIM == h % 2, turned, jnp.zeros_like(turned))
            s = lax.dot_general(
                qn[block, h * NOPE_DIM : (h + 1) * NOPE_DIM],
                expanded[:seen, base : base + NOPE_DIM],
                CONTRACT,
                preferred_element_type=f32,
            ) + lax.dot_general(
                turned, rope_key[:seen, :], CONTRACT, preferred_element_type=f32
            )
            s = jnp.where(k_at <= q_at, s * scale, -jnp.inf)
            p = jnp.exp(s - jnp.max(s, axis=-1, keepdims=True))
            raw = jnp.dot(
                p.astype(bf16),
                expanded[:seen, base + NOPE_DIM : base + NOPE_DIM + VAL_DIM],
                preferred_element_type=f32,
            ) / jnp.sum(p, axis=-1, keepdims=True)
            scaled = raw * lax.rsqrt(jnp.mean(raw * raw, axis=-1, keepdims=True) + EPSILON)
            gain = again_ref[z - att_first][:, h * VAL_DIM : (h + 1) * VAL_DIM]
            merged[block, WIDE + h * VAL_DIM : WIDE + (h + 1) * VAL_DIM] = (
                scaled * gain
            ).astype(bf16)


    part_wide = out_ref.shape[1] // OUT_PARTS

    def out_place(j):
        depth_in = z + upper * (n_sp - 1 - 2 * z)
        found = (3 - 3 * depth_in, 2 + depth_in, 1 + depth_in, depth_in)[j]
        return found + upper * (n_sp - 1 - 2 * found)

    def out_columns(c):
        return slice(c * part_wide, (c + 1) * part_wide)

    def pair_sum(j, c):
        return remote(
            pair_out.at[j, c], pair_in.at[j, c], o_send.at[j, c], o_recv.at[j, c], tp=other
        )

    def near_rows(j, c):
        return remote(
            row_out.at[j, c], row_in.at[0, c], r_send.at[j, c], r_recv.at[0, c], sp=out_place(j)
        )

    def far_rows(j, c):
        return remote(
            row_out.at[j, c],
            far_in.at[j % 2, c],
            r_send.at[j, c],
            far_recv.at[j % 2, c],
            sp=z + 1 - 2 * upper,
        )

    def sum_rows(j, c):
        return remote(
            row_out.at[j, c], row_in.at[1, c], r_send.at[j, c], r_recv.at[1, c], sp=out_place(j)
        )

    def rows_arrival(k, c):
        return remote(row_in.at[k, c], row_in.at[k, c], r_send.at[0, c], r_recv.at[k, c], tp=other)

    def project_out(j, c):
        def action(wide):
            start = (OUT_RET - 1) * WIDE
            got = lax.dot_general(
                merged[at(out_place(j)), :wide],
                w_all[out_columns(c), start : start + wide],
                CONTRACT,
                preferred_element_type=f32,
            )
            front, back = got[:half, :], got[half:, :]
            pair_out[j, c] = jnp.where(t == 0, back, front).astype(bf16)
            pair_sum(j, c).start()
            own_sum[j, :, out_columns(c)] = jnp.where(t == 0, front, back)

        pl.when(is_end)(lambda: action(WIDE))
        pl.when(~is_end)(lambda: action(merged.shape[1]))

    def finish_out(j, c):
        with jax.named_scope("rows_pair"):
            pair_sum(j, c).wait_recv()
        total = own_sum[j, :, out_columns(c)] + pair_in[j, c].astype(f32)
        if j == n_sp - 1:
            own_sum[j, :, out_columns(c)] = total
            return

        def ship(copy):
            row_out[j, c] = total.astype(bf16)
            copy.start()

        def combine():
            with jax.named_scope("combine"):
                far_rows(j - 1, c).wait_recv()
            row_out[j, c] = (total + far_in[j - 1, c].astype(f32)).astype(bf16)
            sum_rows(j, c).start()

        pl.when(is_end)(lambda: ship((near_rows if j == n_sp - 2 else far_rows)(j, c)))
        pl.when(~is_end)(lambda: ship(near_rows(j, c)) if j == 0 else combine())


    def many(action, *pairs):
        for k, u in pairs:
            action(k, u)

    def norm_others():
        pair_arrive(tok_part, 0)
        for k in others:
            norm_block(origin_of(k))

    def retain():
        for d in others:
            shift_copy(d).wait_recv()
        own_shift.wait()
        own_state.wait()
        for b in range(n_sp):
            with jax.named_scope(f"retention#b={b}"):
                retention(b)

    def output():
        turns = [(j, c) for j in range(n_sp) for c in range(OUT_PARTS)]
        for step, turn in enumerate(turns):
            with jax.named_scope(f"out#b={step}"):
                project_out(*turn)
            if step:
                finish_out(*turns[step - 1])
        finish_out(*turns[-1])

    ret_weights = (QUERY, KEY, VALUE)
    out_weights = (OUT_RET, OUT_ATT, OUT_ATT2)

    own_kvd.start()
    for copy in small_copies:
        copy.start()
    pl.when(z == q_place)(lambda: own_lat_copy(q_place).start())
    send_lat(q_place)
    for u in range(QUERY, UNITS):
        when(has(u, z), lambda u=u: own_copy(u).start())
    with jax.named_scope("kvsrc"):
        own_kvd.wait()
        for copy in small_copies:
            copy.wait()
    rope = rope_vmem[...].astype(f32).T.astype(bf16)
    kv_src[:, kv_wide:] = jnp.concatenate(
        [rope, rope[:, ROPE_DIM // 2 :], rope[:, : ROPE_DIM // 2]], axis=1
    )
    pl.when(z == kv_place)(lambda: own_lat_copy(kv_place).start())
    send_lat(kv_place)

    @pl.when(is_end)
    def _():
        line_start(tok_part, 0, tok_ref.at[mine], (2, 1))
        for k in (1, 2):
            for u in (*ret_weights, *out_weights):
                send(u, k)
        for u in ret_weights:
            send(u, 3)
        start_inputs()
        many(spread, (0, LAT), (0, QUERY), (0, KEY), (1, LAT), (0, VALUE))
        many(relay, (0, LAT))
        many(spread, (2, LAT), (3, LAT))
        own_tok.wait()
        norm_block(z)
        many(relay, (0, QUERY), (1, LAT), (0, KEY))
        many(spread, (0, OUT_RET))
        many(relay, (2, LAT), (3, LAT))
        many(spread, (1, QUERY), (1, KEY), (1, VALUE))
        many(relay, (0, VALUE), (0, OUT_RET))
        many(spread, (1, OUT_RET))
        many(relay, (1, QUERY), (1, KEY), (1, VALUE), (1, OUT_RET))
        line_pair(tok_part, 0)
        norm_others()
        for k in range(n_sp):
            arrive(k, LAT)
        wait_tables()
        multiply(LAT)
        finish_lat()
        for i in range(LAT_PARTS):
            lat_send(i).start()
        send(OUT_RET, 3)
        many(spread, (2, QUERY), (2, KEY), (2, VALUE), (3, QUERY))
        many(relay, (2, QUERY), (2, KEY))
        many(spread, (3, KEY))
        many(relay, (2, VALUE))
        many(spread, (3, VALUE), (2, OUT_RET))
        many(relay, (3, QUERY), (3, KEY))
        many(spread, (3, OUT_RET))
        many(relay, (3, VALUE), (2, OUT_RET))
        project(QUERY)
        project(KEY)
        many(relay, (3, OUT_RET))
        project(VALUE)
        with jax.named_scope("retain"):
            retain()
        for k in range(n_sp):
            arrive(k, OUT_RET)
        output()

    @pl.when(~is_end)
    def _():
        line_start(tok_part, 0, tok_ref.at[mine])
        for u in (*ret_weights, OUT_RET):
            send(u, 2)
        for u in ret_weights:
            send(u, 1)
        start_inputs()
        many(spread, *[(0, u) for u in range(QUERY, UNITS)])
        own_tok.wait()
        norm_block(z)
        many(relay, *[(0, u) for u in range(QUERY, UNITS)])
        line_relay(tok_part, 0, 1)
        line_relay(tok_part, 0, 2)
        line_pair(tok_part, 0)
        many(spread, (2, QUERY), (2, KEY), (1, QUERY))
        norm_others()
        wait_tables()
        for u in (*ret_weights, OUT_RET):
            send(u, 3)
        for u in out_weights:
            send(u, 1)
        many(relay, (2, QUERY))
        many(spread, (2, VALUE), (3, QUERY))
        many(relay, (2, KEY), (1, QUERY))
        many(spread, (1, KEY), (3, KEY))
        many(relay, (3, QUERY), (2, VALUE))
        many(spread, (1, VALUE), (3, VALUE))
        many(relay, (1, KEY), (3, KEY))
        many(spread, (2, OUT_RET), (2, OUT_ATT), (2, OUT_ATT2))
        many(relay, (1, VALUE), (3, VALUE))
        lat_forward(0)
        many(spread, (1, OUT_RET))
        project(QUERY)
        many(relay, (2, OUT_RET), (2, OUT_ATT))
        many(spread, (1, OUT_ATT), (1, OUT_ATT2))
        lat_forward(1)
        many(relay, (2, OUT_ATT2))
        project(KEY)
        many(spread, (3, OUT_RET), (3, OUT_ATT), (3, OUT_ATT2))
        project(VALUE)
        retain()
        own_kvup.wait()
        own_qup.wait()
        many(relay, (1, OUT_RET))
        lat_far(0)
        many(relay, (1, OUT_ATT), (1, OUT_ATT2))
        blocks = n_sp // LAT_PARTS
        for i in range(LAT_PARTS):
            lat_arrive(i)
            for b in range(i * blocks, (i + 1) * blocks):
                with jax.named_scope(f"expand#b={b}"):
                    expand(b)
            if i == 0:
                lat_far(1)
            for b in range(i * blocks, (i + 1) * blocks):
                if i == 0:
                    many(relay, (3, OUT_RET + b))
                with jax.named_scope(f"attend#b={b}"):
                    attend(b)
            if i == 0:
                many(relay, (3, OUT_ATT2))
        for u in out_weights:
            for k in range(n_sp):
                arrive(k, u)
        output()

    for c in range(OUT_PARTS):
        total = own_sum[n_sp - 1, :, out_columns(c)]
        for k in range(2):
            with jax.named_scope(f"rows#k={k}"):
                rows_arrival(k, c).wait_recv()
            total = total + row_in[k, c].astype(f32)
        out_ref[:, out_columns(c)] = total.astype(bf16)

    for u in range(UNITS):
        for k in range(n_sp):

            def drain(k=k, u=u):
                x_copy(k, u).wait_send()
                y_copy(k, u).wait_send()
                f_copy(k, u).wait_send()

            when(has(u, z), drain)
            if k and u != LAT:
                when(
                    has(u, origin_of(k)),
                    lambda k=k, u=u: z_copy(origin_of(k), u).wait_send(),
                )
    for place in lat_sources:
        pl.when(z != place)(
            lambda place=place: z_copy(place, LAT, lat_sources[place]).wait_send()
        )
    for d in others:
        shift_copy(d).wait_send()
    line_drain(tok_part, 0)
    for i in range(LAT_PARTS):
        pl.when(is_end)(lambda i=i: lat_send(i).wait_send())

        @pl.when(~is_end)
        def _(i=i):
            lat_copy(i, near_end, n_sp - 1 - z).wait_send()
            for origin in (q_place, kv_place):
                pair_copy(lat_part(i), i + 1, origin).wait_send()

    for j in range(n_sp):
        for c in range(OUT_PARTS):
            pair_sum(j, c).wait_send()
            if j < n_sp - 1:
                near_rows(j, c).wait_send()


def heads_plan(
    tokens,
    norm_gain,
    w_ret_query,
    w_ret_key,
    w_ret_value,
    w_q_down,
    w_kv_down,
    w_rope_key,
    w_q_up,
    w_kv_up,
    q_lat_gain,
    kv_lat_gain,
    att_norm_gain,
    ret_norm_gain,
    w_ret_out,
    w_att_out,
    head_rate,
    decay_shift,
    start_state,
):
    n_sp = lax.axis_size("sp")
    rows, width = tokens.shape[1:]
    length = n_sp * rows
    q_wide, kv_wide = w_q_down.shape[1], w_kv_down.shape[1]
    w_rows = w_q_down.shape[0]
    att_heads = w_q_up.shape[1] // (NOPE_DIM + ROPE_DIM) // 2

    ret_cos, ret_sin = wave_tables(length, RET_DIM)
    rope_cos, rope_sin = wave_tables(length, ROPE_DIM)
    pair_cos = np.concatenate([rope_cos] * 4, axis=1)
    pair_sin = np.concatenate([-rope_sin, rope_sin] * 2, axis=1)
    small = (
        w_rope_key.T,
        head_rate[None],
        norm_gain[None],
        q_lat_gain,
        kv_lat_gain[None],
        att_norm_gain.reshape(2, 1, -1),
        ret_norm_gain.reshape(n_sp, 1, -1),
        ret_cos,
        ret_sin,
        pair_cos,
        pair_sin,
    )
    dma = pltpu.SemaphoreType.DMA
    vmem = pltpu.VMEM
    f32, bf16 = jnp.float32, jnp.bfloat16
    half = rows // 2
    out_wide = 4 * n_sp * w_rows
    any_spec = pl.BlockSpec(memory_space=pl.ANY)
    vmem_spec = pl.BlockSpec(memory_space=pltpu.VMEM)
    mixed = pl.pallas_call(
        functools.partial(layer_kernel, n_sp, q_wide, kv_wide),
        out_shape=jax.ShapeDtypeStruct((half, out_wide), bf16),
        in_specs=[any_spec] * 23,
        out_specs=vmem_spec,
        scratch_shapes=[
            vmem((n_sp, rows, width), bf16),
            vmem((n_sp * 4 * w_rows, (UNITS - 1) * WIDE), bf16),
            vmem((n_sp * 4 * w_rows, q_wide), bf16),
            vmem((w_rows, q_wide), bf16),
            *[vmem(x.shape, x.dtype) for x in small],
            vmem((n_sp,) + decay_shift.shape[1:], f32),
            vmem((length, width), bf16),
            vmem((length, WIDE), f32),
            vmem((length, q_wide), f32),
            vmem((length, WIDE), bf16),
            vmem((length, WIDE), bf16),
            vmem((length, WIDE), bf16),
            vmem((2, 2, length, q_wide), bf16),
            vmem((RET_DIM, RET_DIM), f32),
            vmem((length, att_heads * NOPE_DIM), bf16),
            vmem((length, att_heads * ROPE_DIM), bf16),
            vmem((length, att_heads * (NOPE_DIM + VAL_DIM)), bf16),
            vmem((length, 2 * ROPE_DIM), bf16),
            vmem((w_kv_up.shape[0], att_heads * (NOPE_DIM + VAL_DIM)), bf16),
            vmem((w_q_up.shape[0], att_heads * (NOPE_DIM + ROPE_DIM)), bf16),
            vmem((length, WIDE + att_heads * VAL_DIM), bf16),
            vmem((n_sp, half, out_wide), f32),
            *[vmem((n_sp, OUT_PARTS, half, out_wide // OUT_PARTS), bf16)] * 2,
            vmem((n_sp - 1, OUT_PARTS, half, out_wide // OUT_PARTS), bf16),
            *[vmem((2, OUT_PARTS, half, out_wide // OUT_PARTS), bf16)] * 2,
            dma((14,)),
            *[dma((n_sp, UNITS))] * 8,
            *[dma((1, n_sp))] * 2,
            dma((len(small),)),
            *[dma((n_sp, OUT_PARTS))] * 5,
            *[dma((LAT_PARTS + 1, n_sp))] * 5,
        ],
        compiler_params=pltpu.CompilerParams(
            collective_id=0, has_side_effects=True, vmem_limit_bytes=62 * 1024 * 1024
        ),
    )(
        tokens[0],
        w_q_down,
        w_kv_down,
        w_ret_query,
        w_ret_key,
        w_ret_value,
        w_ret_out,
        w_att_out,
        small[0],
        decay_shift[0],
        *small[1:],
        w_q_up,
        w_kv_up,
        start_state[0],
    )
    return mixed[None]


def solution(mesh):
    placed = (
        P("fs", "sp", None),
        P(),
        P(("sp", "fs"), "tp"),
        P(("sp", "fs"), "tp"),
        P(("sp", "fs"), "tp"),
        P(("sp", "fs"), "tp"),
        P(("sp", "fs"), "tp"),
        P(("sp", "fs"), None),
        P(None, "tp"),
        P(None, "tp"),
        P(),
        P(),
        P("tp"),
        P("tp"),
        P(("sp", "fs"), "tp"),
        P(("sp", "fs"), "tp"),
        P("tp"),
        P("fs", "tp", "sp"),
        P("fs", "tp", None, None),
    )

    def pick(*args):
        if heads_fit(
            mesh, args[16].shape[0], args[0].shape[0], args[5].shape[1], args[6].shape[1], args[8].shape[1]
        ):
            return heads_plan(*args)
        return rows_plan(*args)

    return jax.shard_map(
        pick,
        mesh=mesh,
        in_specs=placed,
        out_specs=P("fs", ("sp", "tp"), None),
        check_vma=False,
    )
```

```python
import functools

import numpy as np

import jax
import jax.numpy as jnp
from jax import lax
from jax.experimental import pallas as pl
from jax.experimental.pallas import tpu as pltpu
from jax.sharding import PartitionSpec as P

RET_DIM = 256
NOPE_DIM = 128
ROPE_DIM = 64
VAL_DIM = 128
KV_LAT = 512


EPSILON = 1e-06
THETA_BASE = 10000.0
TOP_PRECISION = lax.Precision.HIGHEST


def prefix(x, axis, combine, identity):
    peers, position = (lax.axis_size(axis), lax.axis_index(axis))
    everything = jax.tree.map(
        lambda part, kind: lax.all_gather(part.astype(kind), axis), x, (jnp.bfloat16, jnp.bfloat16)
    )
    start = jax.tree.map(
        lambda part, zero: jnp.broadcast_to(jnp.asarray(zero, part.dtype), part.shape), x, identity
    )

    def lap(k, before):
        reached = k < position
        new = combine(
            before, jax.tree.map(lambda part, own: part[k].astype(own.dtype), everything, x)
        )
        return jax.tree.map(lambda a, b: jnp.where(reached, a, b), new, before)

    return lax.fori_loop(0, peers, lap, start)


def angle_tables(positions, rot_width):
    half_width = rot_width // 2
    inverse = THETA_BASE ** (-jnp.arange(half_width, dtype=jnp.float32) * 2.0 / rot_width)
    angles = positions.astype(jnp.float32)[:, None] * inverse[None, :]
    return (jnp.cos(angles), jnp.sin(angles))


def rotate(values, cosine, sine):
    half_width = values.shape[-1] // 2
    front_half = values[..., :half_width]
    back_half = values[..., half_width:]
    return jnp.concatenate(
        [front_half * cosine - back_half * sine, back_half * cosine + front_half * sine], axis=-1
    )


def rms_scale(values, gain_vector):
    return (
        values
        * lax.rsqrt(jnp.mean(values * values, axis=-1, keepdims=True) + EPSILON)
        * gain_vector
    )


def chain_states(earlier, later):
    early_log, early_state = earlier
    late_log, late_state = later
    return (early_log + late_log, jnp.exp(late_log)[:, None, None] * early_state + late_state)


def rows_plan(
    tokens,
    norm_gain,
    w_ret_query,
    w_ret_key,
    w_ret_value,
    w_q_down,
    w_kv_down,
    w_rope_key,
    w_q_up,
    w_kv_up,
    q_lat_gain,
    kv_lat_gain,
    att_norm_gain,
    ret_norm_gain,
    w_ret_out,
    w_att_out,
    head_rate,
    decay_shift,
    start_state,
):
    tok_rows = tokens.shape[1]
    ret_local = head_rate.shape[0]
    att_local = w_q_up.shape[1] // (NOPE_DIM + ROPE_DIM)
    row_offset = lax.axis_index("sp") * tok_rows
    positions = row_offset + jnp.arange(tok_rows, dtype=jnp.int32)
    (
        full_query,
        full_key,
        full_value,
        full_q_down,
        full_kv_down,
        full_rope,
        full_ret_out,
        full_att_out,
    ) = (
        lax.all_gather(w_ret_query, ("sp", "fs"), axis=0, tiled=True),
        lax.all_gather(w_ret_key, ("sp", "fs"), axis=0, tiled=True),
        lax.all_gather(w_ret_value, ("sp", "fs"), axis=0, tiled=True),
        lax.all_gather(w_q_down, ("sp", "fs"), axis=0, tiled=True),
        lax.all_gather(w_kv_down, ("sp", "fs"), axis=0, tiled=True),
        lax.all_gather(w_rope_key, ("sp", "fs"), axis=0, tiled=True),
        lax.all_gather(w_ret_out, ("sp", "fs"), axis=0, tiled=True),
        lax.all_gather(w_att_out, ("sp", "fs"), axis=0, tiled=True),
    )
    source = tokens[0].astype(jnp.float32)
    normed = rms_scale(source, norm_gain).astype(jnp.bfloat16)
    ret_cos, ret_sin = angle_tables(positions, RET_DIM)
    rope_cos, rope_sin = angle_tables(positions, ROPE_DIM)

    def project(weight):
        return jnp.dot(normed, weight, preferred_element_type=jnp.float32)

    part_q = project(full_q_down).astype(jnp.bfloat16)
    part_kv = project(full_kv_down).astype(jnp.bfloat16)
    lat_q_raw, lat_kv_raw = (
        lax.all_gather(part_q, "tp", axis=1, tiled=True),
        lax.all_gather(part_kv, "tp", axis=1, tiled=True),
    )
    retention_query = rotate(
        project(full_query).reshape(tok_rows, ret_local, RET_DIM),
        ret_cos[:, None],
        ret_sin[:, None],
    ).astype(jnp.bfloat16)
    retention_key = (
        rotate(
            project(full_key).reshape(tok_rows, ret_local, RET_DIM),
            ret_cos[:, None],
            ret_sin[:, None],
        )
        * RET_DIM ** (-0.5)
    ).astype(jnp.bfloat16)
    retention_value = project(full_value).reshape(tok_rows, ret_local, RET_DIM).astype(jnp.bfloat16)
    rope_key = rotate(project(full_rope), rope_cos, rope_sin).astype(jnp.bfloat16)
    log_rates = head_rate[:, None] + decay_shift[0]
    cumul = jnp.cumsum(log_rates, axis=1)
    offsets = jnp.arange(tok_rows, dtype=jnp.int32)
    lower_mask = offsets[None, :] <= offsets[:, None]
    decay_matrix = jnp.exp(
        jnp.where(lower_mask[None], cumul[:, :, None] - cumul[:, None, :], -jnp.inf)
    )
    block_score_grid = (
        jnp.einsum(
            "zgq,ugq->gzu", retention_query, retention_key, preferred_element_type=jnp.float32
        )
        * decay_matrix
    ).astype(jnp.bfloat16)
    inside_block_output = jnp.einsum(
        "vzs,svp->zvp", block_score_grid, retention_value, preferred_element_type=jnp.float32
    )
    block_output_sum = cumul[:, -1]
    weighted_values = (
        retention_key.astype(jnp.float32) * jnp.exp(block_output_sum[:, None] - cumul).T[:, :, None]
    )
    contribution = jnp.einsum(
        "uzj,uzv->zjv",
        weighted_values,
        retention_value.astype(jnp.float32),
        precision=TOP_PRECISION,
    )
    identity = (jnp.zeros_like(block_output_sum), jnp.zeros_like(contribution))
    before_log, before_state = prefix(
        (block_output_sum, contribution), "sp", chain_states, identity
    )
    q_latent = rms_scale(lat_q_raw.astype(jnp.float32), q_lat_gain).astype(jnp.bfloat16)
    kv_latent = rms_scale(lat_kv_raw.astype(jnp.float32), kv_lat_gain).astype(jnp.bfloat16)
    query_full = jnp.dot(q_latent, w_q_up, preferred_element_type=jnp.float32).reshape(
        tok_rows, att_local, NOPE_DIM + ROPE_DIM
    )
    query_nope = query_full[..., :NOPE_DIM].astype(jnp.bfloat16)
    query_rope = rotate(query_full[..., NOPE_DIM:], rope_cos[:, None], rope_sin[:, None]).astype(
        jnp.bfloat16
    )
    att_scale = (NOPE_DIM + ROPE_DIM) ** (-0.5)

    def attend(carry, key_nope, key_values, key_rope, start):
        running_max, running_sum, running_acc = carry
        key_count = key_rope.shape[0]
        score_matrix = (
            jnp.einsum("qhd,khd->hqk", query_nope, key_nope, preferred_element_type=jnp.float32)
            + jnp.einsum("qhd,kd->hqk", query_rope, key_rope, preferred_element_type=jnp.float32)
        ) * att_scale
        key_positions = start + jnp.arange(key_count, dtype=jnp.int32)
        allowed = key_positions[None, :] <= positions[:, None]
        masked = jnp.where(allowed[None], score_matrix, -jnp.inf)
        new_max = jnp.maximum(running_max, jnp.max(masked, axis=-1))
        safe_max = jnp.where(jnp.isfinite(new_max), new_max, 0.0)
        weights = jnp.exp(masked - safe_max[..., None])
        rescale = jnp.exp(running_max - safe_max)
        new_sum = running_sum * rescale + jnp.sum(weights, axis=-1)
        new_acc = running_acc * rescale[..., None] + jnp.einsum(
            "hqk,khd->hqd",
            weights.astype(jnp.bfloat16),
            key_values,
            preferred_element_type=jnp.float32,
        )
        return (new_max, new_sum, new_acc)

    def expand_attend(carry_in, lat_piece, rope_piece, start):
        wide = (
            jnp.dot(lat_piece, w_kv_up, preferred_element_type=jnp.float32)
            .astype(jnp.bfloat16)
            .reshape(rope_piece.shape[0], att_local, NOPE_DIM + VAL_DIM)
        )
        return attend(carry_in, wide[..., :NOPE_DIM], wide[..., NOPE_DIM:], rope_piece, start)

    empty = (
        jnp.full((att_local, tok_rows), -jnp.inf, jnp.float32),
        jnp.zeros((att_local, tok_rows), jnp.float32),
        jnp.zeros((att_local, tok_rows, VAL_DIM), jnp.float32),
    )
    groups = lax.axis_size("tp")
    kv_part = KV_LAT // groups
    rope_part = ROPE_DIM // groups
    my_group = lax.axis_index("tp")
    joined = jnp.concatenate(
        [
            lax.dynamic_slice_in_dim(kv_latent, my_group * kv_part, kv_part, 1),
            lax.dynamic_slice_in_dim(rope_key, my_group * rope_part, rope_part, 1),
        ],
        axis=1,
    )
    all_rows = lax.all_gather(joined, "sp", axis=0, tiled=True)
    complete = lax.all_gather(all_rows, "tp", axis=1, tiled=True)
    total_rows = complete.shape[0]
    grouped = complete.reshape(total_rows, groups, kv_part + rope_part)
    lat_all = grouped[:, :, :kv_part].reshape(total_rows, KV_LAT)
    rope_all = grouped[:, :, kv_part:].reshape(total_rows, ROPE_DIM)

    def visit(block_index, carry_in):
        start = block_index * tok_rows
        lat_piece = lax.dynamic_slice_in_dim(lat_all, start, tok_rows, 0)
        rope_piece = lax.dynamic_slice_in_dim(rope_all, start, tok_rows, 0)
        return expand_attend(carry_in, lat_piece, rope_piece, start)

    final = lax.fori_loop(0, lax.axis_index("sp") + 1, visit, empty)
    att_raw = jnp.transpose(final[2] / final[1][..., None], (1, 0, 2))
    att_out = (
        rms_scale(att_raw, att_norm_gain.reshape(att_local, VAL_DIM))
        .astype(jnp.bfloat16)
        .reshape(tok_rows, att_local * VAL_DIM)
    )
    entering = jnp.exp(before_log)[:, None, None] * start_state[0] + before_state
    carried_term = (
        jnp.einsum(
            "nhd,hde->nhe", retention_query.astype(jnp.float32), entering, precision=TOP_PRECISION
        )
        * jnp.exp(cumul).T[:, :, None]
    )
    ret_raw = inside_block_output + carried_term
    row_mean = jnp.mean(ret_raw, axis=-1, keepdims=True)
    centered = ret_raw - row_mean
    row_var = jnp.mean(centered * centered, axis=-1, keepdims=True)
    ret_out = (
        (centered * lax.rsqrt(row_var + EPSILON) * ret_norm_gain.reshape(ret_local, RET_DIM))
        .astype(jnp.bfloat16)
        .reshape(tok_rows, ret_local * RET_DIM)
    )
    contract = (((1,), (1,)), ((), ()))
    mixed = lax.psum_scatter(
        (
            lax.dot_general(ret_out, full_ret_out, contract, preferred_element_type=jnp.float32)
            + lax.dot_general(att_out, full_att_out, contract, preferred_element_type=jnp.float32)
        ).astype(jnp.bfloat16),
        "tp",
        scatter_dimension=0,
        tiled=True,
    )
    return mixed[None]


MESH = pl.DeviceIdType.MESH
WIDE = RET_DIM
CONTRACT = (((1,), (1,)), ((), ()))
UNITS = 7
LAT, QUERY, KEY, VALUE, OUT_RET, OUT_ATT, OUT_ATT2 = range(UNITS)
LAT_PARTS = 2
OUT_PARTS = 2


def heads_fit(mesh, ret_local, sequences, q_wide, kv_wide, up_wide):
    sizes = mesh.shape
    return (
        sizes["sp"] == 4
        and sizes["fs"] == 4
        and sizes["tp"] == 2
        and ret_local == sizes["sp"]
        and sequences == 1
        and up_wide == 2 * (NOPE_DIM + ROPE_DIM) * ret_local
        and q_wide % 128 == 0
        and kv_wide % 128 == 0
        and q_wide == kv_wide + 2 * ROPE_DIM
    )


def wave_tables(length, wide):
    half_wide = wide // 2
    powers = np.arange(half_wide, dtype=np.float32) * np.float32(2.0 / wide)
    inverse = np.power(np.float32(THETA_BASE), -powers).astype(np.float32)
    angles = np.arange(length, dtype=np.float32)[:, None] * inverse[None, :]
    return np.cos(angles), np.sin(angles)


def three_parts(x):
    high = x.astype(jnp.bfloat16)
    rest = x - high.astype(jnp.float32)
    middle = rest.astype(jnp.bfloat16)
    low = (rest - middle.astype(jnp.float32)).astype(jnp.bfloat16)
    return high, middle, low


def layer_kernel(
    n_sp,
    q_wide,
    kv_wide,
    tok_ref,
    wqd_ref,
    wkvd_ref,
    wq_ref,
    wk_ref,
    wv_ref,
    wr_ref,
    wa_ref,
    rope_hbm,
    shift_ref,
    rate_hbm,
    gain_hbm,
    qgain_hbm,
    kvgain_hbm,
    again_hbm,
    rgain_hbm,
    rcos_hbm,
    rsin_hbm,
    pcos_hbm,
    psin_hbm,
    qup_ref,
    kvup_ref,
    start_ref,
    out_ref,
    tok_all,
    w_all,
    w_lat,
    kv_src,
    rope_vmem,
    rate_ref,
    gain_ref,
    qgain_ref,
    kvgain_ref,
    again_ref,
    rgain_ref,
    rcos_ref,
    rsin_ref,
    pcos_ref,
    psin_ref,
    shift_all,
    normed,
    acc_ret,
    acc_lat,
    ret_q,
    ret_k,
    ret_v,
    lat_all,
    state,
    qn,
    qr,
    expanded,
    rope_key,
    kvup,
    qup,
    merged,
    own_sum,
    pair_out,
    pair_in,
    row_out,
    row_in,
    far_in,
    out_vmem,
    local_sem,
    z_send,
    z_recv,
    x_send,
    x_recv,
    y_send,
    y_recv,
    f_send,
    f_recv,
    m_send,
    m_recv,
    small_sem,
    out_sem,
    o_send,
    o_recv,
    r_send,
    r_recv,
    far_recv,
    l_send,
    l_recv,
    l_relay,
    p_send,
    p_recv,
):
    z, f, t = lax.axis_index("sp"), lax.axis_index("fs"), lax.axis_index("tp")
    xn = f + 1 - 2 * (f % 2)
    yn = (f + 2) % 4
    other = 1 - t
    fs = 4
    rows = tok_ref.shape[0]
    length = n_sp * rows
    half = rows // 2
    weights = (None, wq_ref, wk_ref, wv_ref, wr_ref, wa_ref, wa_ref)
    f32, bf16 = jnp.float32, jnp.bfloat16
    q_place, kv_place = 0, n_sp - 1
    att_first = n_sp // 2 - 1
    middles = (att_first, att_first + 1)
    others = range(1, n_sp)

    def remote(src, dst, send, recv, **where):
        return pltpu.make_async_remote_copy(
            src_ref=src,
            dst_ref=dst,
            send_sem=send,
            recv_sem=recv,
            device_id={"sp": z, "fs": f, "tp": t, **where},
            device_id_type=MESH,
        )

    barrier = pltpu.get_barrier_semaphore()
    peers = [{"sp": (z + d) % n_sp, "fs": f, "tp": t} for d in others]
    peers += [{"sp": z, "fs": xn, "tp": t}, {"sp": z, "fs": yn, "tp": t}]
    peers += [{"sp": z, "fs": f, "tp": other}]
    for peer in peers:
        pl.semaphore_signal(barrier, inc=1, device_id=peer, device_id_type=MESH)
    with jax.named_scope("barrier"):
        pl.semaphore_wait(barrier, len(peers))

    def at(i, size=rows):
        if isinstance(i, int):
            return slice(i * size, (i + 1) * size)
        return pl.ds(pl.multiple_of(i * size, size), size)

    upper = z // (n_sp // 2)
    is_end = (z == 0) | (z == n_sp - 1)

    def origin_of(k):
        depth_in = z + upper * (n_sp - 1 - 2 * z)
        found = (depth_in * 0, 1 + depth_in, 2 - 2 * depth_in, depth_in * 0 + 3)[k]
        return z if k == 0 else found + upper * (n_sp - 1 - 2 * found)


    def piece(u, dest):
        column = dest if u < OUT_ATT else 2 * (dest - att_first) + u - OUT_ATT
        return weights[u].at[:, at(column, WIDE)]

    def part(owner_z, owner_f, u):
        where = at(owner_z * fs + owner_f)
        if u == LAT:
            return w_lat.at[where]
        return w_all.at[where, (u - 1) * WIDE : u * WIDE]

    def has(u, place):
        edge = (place == q_place) | (place == kv_place)
        return edge if u == LAT else ~edge if u >= OUT_ATT else True

    def when(condition, action):
        if condition is True:
            action()
        else:
            pl.when(condition)(action)

    lat_sources = {q_place: wqd_ref, kv_place: kv_src}

    def z_copy(to, u, src=None):
        return remote(
            piece(u, to) if src is None else src,
            part(z, f, u),
            z_send.at[to, u],
            z_recv.at[z, u],
            sp=to,
        )

    def z_arrival(k, u):
        ref = part(origin_of(k), f, u)
        return remote(ref, ref, z_send.at[z, u], z_recv.at[origin_of(k), u], tp=other)

    def x_copy(k, u):
        ref = part(origin_of(k), f, u)
        return remote(ref, ref, x_send.at[k, u], x_recv.at[k, u], fs=xn)

    def y_copy(k, u):
        ref = part(origin_of(k), f, u)
        return remote(ref, ref, y_send.at[k, u], y_recv.at[k, u], fs=yn)

    def f_copy(k, u):
        source, to = (xn, yn) if (k + u) % 2 == 0 else (yn, xn)
        ref = part(origin_of(k), source, u)
        return remote(ref, ref, f_send.at[k, u], f_recv.at[k, u], fs=to)

    def own_copy(u):
        return pltpu.make_async_copy(piece(u, z), part(z, f, u), local_sem.at[u])

    def own_lat_copy(place):
        return pltpu.make_async_copy(lat_sources[place], part(z, f, LAT), local_sem.at[LAT])

    def send(u, *to):
        for k in to or others:
            when(has(u, origin_of(k)), lambda k=k: z_copy(origin_of(k), u).start())

    def send_lat(place):
        pl.when(z != place)(lambda: z_copy(place, LAT, lat_sources[place]).start())

    def spread(d, u):
        def action():
            with jax.named_scope(f"spread#d={d}#u={u}"):
                if d:
                    z_arrival(d, u).wait_recv()
                elif u == LAT:
                    own_lat_copy(q_place).wait()
                else:
                    own_copy(u).wait()
            x_copy(d, u).start()
            y_copy(d, u).start()

        when(has(u, z), action)

    def relay(d, u):
        def action():
            with jax.named_scope(f"relay#d={d}#u={u}"):
                (x_copy if (d + u) % 2 == 0 else y_copy)(d, u).wait_recv()
            f_copy(d, u).start()

        when(has(u, z), action)

    def arrive(d, u):
        def action():
            with jax.named_scope(f"arrive#d={d}#u={u}"):
                (y_copy if (d + u) % 2 == 0 else x_copy)(d, u).wait_recv()
                f_copy(d, u).wait_recv()

        when(has(u, z), action)


    mine = pl.ds(pl.multiple_of(t * half, half), half)

    def tok_part(origin):
        return tok_all.at[origin, mine]

    lat_rows = length // LAT_PARTS

    def lat_part(i):
        return lambda origin: lat_all.at[t, origin // (n_sp - 1), pl.ds(i * lat_rows, lat_rows)]

    def line_copy(where, row, dest, src=None):
        return remote(
            where(z) if src is None else src,
            where(z),
            l_send.at[row, dest],
            l_recv.at[row, z],
            sp=dest,
        )

    def relay_copy(where, row, origin, dest):
        ref = where(origin)
        return remote(ref, ref, l_relay.at[row, origin], l_recv.at[row, origin], sp=dest)

    def pair_copy(where, row, origin):
        ref = where(origin)
        return remote(ref, ref, p_send.at[row, origin], p_recv.at[row, origin], tp=other)

    def direct(dest):
        near = (z - dest == 1) | (dest - z == 1)
        return near if dest in (0, n_sp - 1) else z != dest

    def line_start(where, row, src=None, distances=others):
        for distance in distances:
            for dest in range(n_sp):
                condition = direct(dest) & ((z - dest == distance) | (dest - z == distance))
                pl.when(condition)(
                    lambda dest=dest: line_copy(where, row, dest, src).start()
                )

    ends = ((1, 0), (n_sp - 2, n_sp - 1))

    def line_relay(where, row, distance):
        for middle, dest in ends:
            origin = middle + (middle - dest) * distance

            @pl.when(z == middle)
            def _(origin=origin, dest=dest):
                with jax.named_scope(f"line#r={row}#k={distance}"):
                    relay_copy(where, row, origin, dest).wait_recv()
                relay_copy(where, row, origin, dest).start()

    def was_relayed(origin):
        return z == (n_sp - 2 if origin < n_sp // 2 else 1)

    def line_pair(where, row):
        for distance in others:
            for origin in range(n_sp):
                here = (z - origin == distance) | (origin - z == distance)

                @pl.when(here)
                def _(origin=origin):
                    with jax.named_scope(f"pass#r={row}#k={distance}"):
                        pl.when(~was_relayed(origin))(
                            lambda: relay_copy(where, row, origin, 0).wait_recv()
                        )
                    pair_copy(where, row, origin).start()

    def pair_arrive(where, row):
        with jax.named_scope(f"pair#r={row}"):
            for origin in range(n_sp):
                pl.when(origin != z)(
                    lambda origin=origin: pair_copy(where, row, origin).wait_recv()
                )

    def line_drain(where, row):
        for dest in range(n_sp):
            pl.when(direct(dest))(lambda dest=dest: line_copy(where, row, dest).wait_send())
        for middle, dest in ends:
            for distance in range(1, n_sp - 1):
                origin = middle + (middle - dest) * distance
                pl.when(z == middle)(
                    lambda origin=origin, dest=dest: relay_copy(
                        where, row, origin, dest
                    ).wait_send()
                )
        for origin in range(n_sp):
            pl.when(origin != z)(
                lambda origin=origin: pair_copy(where, row, origin).wait_send()
            )


    near_end, far_end = upper * (n_sp - 1), (1 - upper) * (n_sp - 1)

    def lat_copy(i, origin, to):
        ref = lat_part(i)(origin)
        return remote(ref, ref, l_send.at[i + 1, 0], l_recv.at[i + 1, origin], sp=to)

    def lat_send(i):
        return lat_copy(i, z, z + 1 - 2 * upper)

    def lat_forward(i):
        with jax.named_scope(f"latnear#i={i}"):
            lat_copy(i, near_end, z).wait_recv()
        lat_copy(i, near_end, n_sp - 1 - z).start()
        pair_copy(lat_part(i), i + 1, near_end).start()

    def lat_far(i):
        with jax.named_scope(f"latfar#i={i}"):
            lat_copy(i, far_end, z).wait_recv()
        pair_copy(lat_part(i), i + 1, far_end).start()

    def lat_arrive(i):
        with jax.named_scope(f"latpair#i={i}"):
            for origin in (q_place, kv_place):
                pair_copy(lat_part(i), i + 1, origin).wait_recv()

    def shift_copy(d):
        to = (z + d) % n_sp
        return remote(shift_ref, shift_all.at[z], m_send.at[0, d], m_recv.at[0, d], sp=to)


    staged = (
        (rope_hbm, rope_vmem),
        (rate_hbm, rate_ref),
        (gain_hbm, gain_ref),
        (qgain_hbm, qgain_ref),
        (kvgain_hbm, kvgain_ref),
        (again_hbm, again_ref),
        (rgain_hbm, rgain_ref),
        (rcos_hbm, rcos_ref),
        (rsin_hbm, rsin_ref),
        (pcos_hbm, pcos_ref),
        (psin_hbm, psin_ref),
    )
    staged_copies = [
        pltpu.make_async_copy(src, dst, small_sem.at[i]) for i, (src, dst) in enumerate(staged)
    ]
    small_copies, table_copies = staged_copies[:7], staged_copies[7:]

    def wait_tables():
        for copy in table_copies:
            copy.wait()

    def start_inputs():
        for copy in table_copies:
            copy.start()
        own_tok.start()
        own_shift.start()

        @pl.when(~is_end)
        def _():
            own_kvup.start()
            own_qup.start()

        own_state.start()
        for d in others:
            shift_copy(d).start()

    own_tok = pltpu.make_async_copy(tok_ref, tok_all.at[z], local_sem.at[12])
    own_shift = pltpu.make_async_copy(shift_ref, shift_all.at[z], local_sem.at[13])
    att_wide = kvup.shape[1]
    own_kvup = pltpu.make_async_copy(kvup_ref.at[:, at(z - att_first, att_wide)], kvup, local_sem.at[8])
    own_state = pltpu.make_async_copy(start_ref.at[z], state, local_sem.at[9])
    up_wide = qup.shape[1]
    own_qup = pltpu.make_async_copy(qup_ref.at[:, at(z - att_first, up_wide)], qup, local_sem.at[10])
    own_kvd = pltpu.make_async_copy(wkvd_ref, kv_src.at[:, :kv_wide], local_sem.at[11])

    def norm_block(i):
        x = tok_all[i].astype(f32)
        scaled = x * lax.rsqrt(jnp.mean(x * x, axis=-1, keepdims=True) + EPSILON)
        normed[at(i), :] = (scaled * gain_ref[...]).astype(bf16)

    depth = fs * rows

    def multiply(u):
        weight, columns = (
            (w_lat, slice(None)) if u == LAT else (w_all, slice((u - 1) * WIDE, u * WIDE))
        )
        acc = acc_lat if u == LAT else acc_ret
        with jax.named_scope(f"multiply#u={u}"):
            acc[...] = jnp.dot(
                normed[:, :depth],
                weight[:depth, columns],
                preferred_element_type=f32,
            )

            def chunk(i, carry):
                begin = at(i, depth)
                acc[...] += jnp.dot(
                    normed[:, begin],
                    weight[begin, columns],
                    preferred_element_type=f32,
                )
                return carry

            lax.fori_loop(1, n_sp, chunk, 0)

    rd = RET_DIM // 2

    def finish_lat():
        def block(i, carry):
            lat_all[t, upper, at(i), :kv_wide] = acc_lat[at(i), :kv_wide].astype(bf16)
            pair = acc_lat[at(i), kv_wide:]
            turned = pair * pcos_ref[at(i), :] + pltpu.roll(pair, ROPE_DIM, 1) * psin_ref[at(i), :]
            lane = lax.broadcasted_iota(jnp.int32, turned.shape, 1)
            turned = jnp.where(lane < ROPE_DIM, turned, pltpu.roll(turned, ROPE_DIM, 1))
            lat_all[t, upper, at(i), kv_wide:] = jnp.where(
                z == kv_place, turned, pair
            ).astype(bf16)
            return carry

        lax.fori_loop(0, n_sp, block, 0)

    def finish_turned(dst, factor):
        def block(i, carry):
            cosine, sine = rcos_ref[at(i), :], rsin_ref[at(i), :]
            a, b = acc_ret[at(i), :rd], acc_ret[at(i), rd:]
            dst[at(i), :rd] = ((a * cosine - b * sine) * factor).astype(bf16)
            dst[at(i), rd:] = ((b * cosine + a * sine) * factor).astype(bf16)
            return carry

        lax.fori_loop(0, n_sp, block, 0)

    def project(u):
        for d in range(n_sp):
            arrive(d, u)
        multiply(u)
        if u == QUERY:
            finish_turned(ret_q, 1.0)
        elif u == KEY:
            finish_turned(ret_k, RET_DIM ** (-0.5))
        else:
            ret_v[...] = acc_ret[...].astype(bf16)

    r_iota = lax.broadcasted_iota(jnp.int32, (rows, rows), 0)
    c_iota = lax.broadcasted_iota(jnp.int32, (rows, rows), 1)

    def retention(b):
        rates = shift_all[b]
        pick = lax.broadcasted_iota(jnp.int32, rates.shape, 0) == z
        chosen = lax.broadcasted_iota(jnp.int32, rate_ref.shape, 1) == z
        rate = jnp.sum(jnp.where(chosen, rate_ref[...], 0.0), axis=1, keepdims=True)
        row = jnp.sum(jnp.where(pick, rates, 0.0), axis=0, keepdims=True) + rate
        column = jnp.sum(jnp.where(r_iota == c_iota, row, 0.0), axis=1, keepdims=True)
        c_col = jnp.sum(jnp.where(c_iota <= r_iota, row, 0.0), axis=1, keepdims=True)
        c_row = jnp.sum(jnp.where(r_iota <= c_iota, column, 0.0), axis=0, keepdims=True)
        last = jnp.sum(row, axis=1, keepdims=True)
        decay = jnp.exp(jnp.where(c_iota <= r_iota, c_col - c_row, -jnp.inf))
        block = slice(b * rows, (b + 1) * rows)
        q, k, v = ret_q[block, :], ret_k[block, :], ret_v[block, :]
        scores = lax.dot_general(q, k, CONTRACT, preferred_element_type=f32) * decay
        raw = jnp.dot(scores.astype(bf16), v, preferred_element_type=f32)
        carried = sum(
            jnp.dot(q, s, preferred_element_type=f32) for s in three_parts(state[...])
        )
        raw = raw + carried * jnp.exp(c_col)
        if b < n_sp - 1:
            weighted = k.astype(f32) * jnp.exp(last - c_col)
            added = sum(
                lax.dot_general(w, v, (((0,), (0,)), ((), ())), preferred_element_type=f32)
                for w in three_parts(weighted)
            )
            state[...] = jnp.exp(last) * state[...] + added
        centered = raw - jnp.mean(raw, axis=-1, keepdims=True)
        variance = jnp.mean(centered * centered, axis=-1, keepdims=True)
        merged[block, :WIDE] = (centered * lax.rsqrt(variance + EPSILON) * rgain_ref[z]).astype(
            bf16
        )

    att_heads = att_wide // (NOPE_DIM + VAL_DIM)

    def expand(i):
        def latent(slot, wide, gain):
            x = jnp.concatenate(
                [lat_all[core, slot, at(i), :wide] for core in range(2)], axis=1
            ).astype(f32)
            scaled = x * lax.rsqrt(jnp.mean(x * x, axis=-1, keepdims=True) + EPSILON)
            return (scaled * gain[...].reshape(1, wide * 2)).astype(bf16)

        query = jnp.dot(latent(0, q_wide, qgain_ref), qup[...], preferred_element_type=f32)
        for pair_at in range(att_heads // 2):
            lanes = query[:, pair_at * 384 : (pair_at + 1) * 384]
            first, middle, end = lanes[:, :128], lanes[:, 128:256], lanes[:, 256:]
            lane = lax.broadcasted_iota(jnp.int32, first.shape, 1)
            second = jnp.where(
                lane < ROPE_DIM, pltpu.roll(middle, ROPE_DIM, 1), pltpu.roll(end, ROPE_DIM, 1)
            )
            pair = jnp.where(lane < ROPE_DIM, middle, end)
            quarter = ROPE_DIM // 2
            swapped = jnp.where(
                lane % ROPE_DIM < quarter,
                pltpu.roll(pair, 2 * ROPE_DIM - quarter, 1),
                pltpu.roll(pair, quarter, 1),
            )
            base = 2 * pair_at * NOPE_DIM
            qn[at(i), base : base + NOPE_DIM] = first.astype(bf16)
            qn[at(i), base + NOPE_DIM : base + 2 * NOPE_DIM] = second.astype(bf16)
            qr[at(i), pair_at * 128 : (pair_at + 1) * 128] = (
                pair * pcos_ref[at(i), :] + swapped * psin_ref[at(i), :]
            ).astype(bf16)
        expanded[at(i), :] = jnp.dot(
            latent(1, kv_wide, kvgain_ref), kvup[...], preferred_element_type=f32
        ).astype(bf16)
        rope_key[at(i), :] = lat_all[0, 1, at(i), kv_wide:]

    scale = (NOPE_DIM + ROPE_DIM) ** (-0.5)

    def attend(b):
        seen = (b + 1) * rows
        block = slice(b * rows, seen)
        q_at = lax.broadcasted_iota(jnp.int32, (rows, seen), 0) + b * rows
        k_at = lax.broadcasted_iota(jnp.int32, (rows, seen), 1)
        for h in range(att_heads):
            base = h * (NOPE_DIM + VAL_DIM)
            turned = qr[block, h // 2 * 128 : (h // 2 + 1) * 128]
            lane = lax.broadcasted_iota(jnp.int32, turned.shape, 1)
            turned = jnp.where(lane // ROPE_DIM == h % 2, turned, jnp.zeros_like(turned))
            s = lax.dot_general(
                qn[block, h * NOPE_DIM : (h + 1) * NOPE_DIM],
                expanded[:seen, base : base + NOPE_DIM],
                CONTRACT,
                preferred_element_type=f32,
            ) + lax.dot_general(
                turned, rope_key[:seen, :], CONTRACT, preferred_element_type=f32
            )
            s = jnp.where(k_at <= q_at, s * scale, -jnp.inf)
            p = jnp.exp(s - jnp.max(s, axis=-1, keepdims=True))
            raw = jnp.dot(
                p.astype(bf16),
                expanded[:seen, base + NOPE_DIM : base + NOPE_DIM + VAL_DIM],
                preferred_element_type=f32,
            ) / jnp.sum(p, axis=-1, keepdims=True)
            scaled = raw * lax.rsqrt(jnp.mean(raw * raw, axis=-1, keepdims=True) + EPSILON)
            gain = again_ref[z - att_first][:, h * VAL_DIM : (h + 1) * VAL_DIM]
            merged[block, WIDE + h * VAL_DIM : WIDE + (h + 1) * VAL_DIM] = (
                scaled * gain
            ).astype(bf16)


    part_wide = out_ref.shape[1] // OUT_PARTS

    def out_place(j):
        depth_in = z + upper * (n_sp - 1 - 2 * z)
        found = (3 - 3 * depth_in, 2 + depth_in, 1 + depth_in, depth_in)[j]
        return found + upper * (n_sp - 1 - 2 * found)

    def out_columns(c):
        return slice(c * part_wide, (c + 1) * part_wide)

    def pair_sum(j, c):
        return remote(
            pair_out.at[j, c], pair_in.at[j, c], o_send.at[j, c], o_recv.at[j, c], tp=other
        )

    def near_rows(j, c):
        return remote(
            row_out.at[j, c], row_in.at[0, c], r_send.at[j, c], r_recv.at[0, c], sp=out_place(j)
        )

    def far_rows(j, c):
        return remote(
            row_out.at[j, c],
            far_in.at[j % 2, c],
            r_send.at[j, c],
            far_recv.at[j % 2, c],
            sp=z + 1 - 2 * upper,
        )

    def sum_rows(j, c):
        return remote(
            row_out.at[j, c], row_in.at[1, c], r_send.at[j, c], r_recv.at[1, c], sp=out_place(j)
        )

    def out_copy(c):
        return pltpu.make_async_copy(out_vmem.at[c], out_ref.at[:, out_columns(c)], out_sem.at[c])

    def rows_arrival(k, c):
        return remote(row_in.at[k, c], row_in.at[k, c], r_send.at[0, c], r_recv.at[k, c], tp=other)

    def project_out(j, c):
        def action(wide):
            start = (OUT_RET - 1) * WIDE
            got = lax.dot_general(
                merged[at(out_place(j)), :wide],
                w_all[out_columns(c), start : start + wide],
                CONTRACT,
                preferred_element_type=f32,
            )
            front, back = got[:half, :], got[half:, :]
            pair_out[j, c] = jnp.where(t == 0, back, front).astype(bf16)
            pair_sum(j, c).start()
            own_sum[j, :, out_columns(c)] = jnp.where(t == 0, front, back)

        pl.when(is_end)(lambda: action(WIDE))
        pl.when(~is_end)(lambda: action(merged.shape[1]))

    def finish_out(j, c):
        with jax.named_scope("rows_pair"):
            pair_sum(j, c).wait_recv()
        total = own_sum[j, :, out_columns(c)] + pair_in[j, c].astype(f32)
        if j == n_sp - 1:
            own_sum[j, :, out_columns(c)] = total
            return

        def ship(copy):
            row_out[j, c] = total.astype(bf16)
            copy.start()

        def combine():
            with jax.named_scope("combine"):
                far_rows(j - 1, c).wait_recv()
            row_out[j, c] = (total + far_in[j - 1, c].astype(f32)).astype(bf16)
            sum_rows(j, c).start()

        pl.when(is_end)(lambda: ship((near_rows if j == n_sp - 2 else far_rows)(j, c)))
        pl.when(~is_end)(lambda: ship(near_rows(j, c)) if j == 0 else combine())


    def many(action, *pairs):
        for k, u in pairs:
            action(k, u)

    def norm_others():
        pair_arrive(tok_part, 0)
        for k in others:
            norm_block(origin_of(k))

    def retain():
        for d in others:
            shift_copy(d).wait_recv()
        own_shift.wait()
        own_state.wait()
        for b in range(n_sp):
            with jax.named_scope(f"retention#b={b}"):
                retention(b)

    def output():
        turns = [(j, c) for j in range(n_sp) for c in range(OUT_PARTS)]
        for step, turn in enumerate(turns):
            with jax.named_scope(f"out#b={step}"):
                project_out(*turn)
            if step:
                finish_out(*turns[step - 1])
        finish_out(*turns[-1])

    ret_weights = (QUERY, KEY, VALUE)
    out_weights = (OUT_RET, OUT_ATT, OUT_ATT2)

    own_kvd.start()
    for copy in small_copies:
        copy.start()
    pl.when(z == q_place)(lambda: own_lat_copy(q_place).start())
    send_lat(q_place)
    for u in range(QUERY, UNITS):
        when(has(u, z), lambda u=u: own_copy(u).start())
    with jax.named_scope("kvsrc"):
        own_kvd.wait()
        for copy in small_copies:
            copy.wait()
    rope = rope_vmem[...].astype(f32).T.astype(bf16)
    kv_src[:, kv_wide:] = jnp.concatenate(
        [rope, rope[:, ROPE_DIM // 2 :], rope[:, : ROPE_DIM // 2]], axis=1
    )
    pl.when(z == kv_place)(lambda: own_lat_copy(kv_place).start())
    send_lat(kv_place)

    @pl.when(is_end)
    def _():
        line_start(tok_part, 0, tok_ref.at[mine], (2, 1))
        for k in (1, 2):
            for u in (*ret_weights, *out_weights):
                send(u, k)
        for u in ret_weights:
            send(u, 3)
        start_inputs()
        many(spread, (0, LAT), (0, QUERY), (0, KEY), (1, LAT), (0, VALUE))
        many(relay, (0, LAT))
        many(spread, (2, LAT), (3, LAT))
        own_tok.wait()
        norm_block(z)
        many(relay, (0, QUERY), (1, LAT), (0, KEY))
        many(spread, (0, OUT_RET))
        many(relay, (2, LAT), (3, LAT))
        many(spread, (1, QUERY), (1, KEY), (1, VALUE))
        many(relay, (0, VALUE), (0, OUT_RET))
        many(spread, (1, OUT_RET))
        many(relay, (1, QUERY), (1, KEY), (1, VALUE), (1, OUT_RET))
        line_pair(tok_part, 0)
        norm_others()
        for k in range(n_sp):
            arrive(k, LAT)
        wait_tables()
        multiply(LAT)
        finish_lat()
        for i in range(LAT_PARTS):
            lat_send(i).start()
        send(OUT_RET, 3)
        many(spread, (2, QUERY), (2, KEY), (2, VALUE), (3, QUERY))
        many(relay, (2, QUERY), (2, KEY))
        many(spread, (3, KEY))
        many(relay, (2, VALUE))
        many(spread, (3, VALUE), (2, OUT_RET))
        many(relay, (3, QUERY), (3, KEY))
        many(spread, (3, OUT_RET))
        many(relay, (3, VALUE), (2, OUT_RET))
        project(QUERY)
        project(KEY)
        many(relay, (3, OUT_RET))
        project(VALUE)
        with jax.named_scope("retain"):
            retain()
        for k in range(n_sp):
            arrive(k, OUT_RET)
        output()

    @pl.when(~is_end)
    def _():
        line_start(tok_part, 0, tok_ref.at[mine])
        for u in (*ret_weights, OUT_RET):
            send(u, 2)
        for u in ret_weights:
            send(u, 1)
        start_inputs()
        many(spread, *[(0, u) for u in range(QUERY, UNITS)])
        own_tok.wait()
        norm_block(z)
        many(relay, *[(0, u) for u in range(QUERY, UNITS)])
        line_relay(tok_part, 0, 1)
        line_relay(tok_part, 0, 2)
        line_pair(tok_part, 0)
        many(spread, (2, QUERY), (2, KEY), (1, QUERY))
        norm_others()
        wait_tables()
        for u in (*ret_weights, OUT_RET):
            send(u, 3)
        for u in out_weights:
            send(u, 1)
        many(relay, (2, QUERY))
        many(spread, (2, VALUE), (3, QUERY))
        many(relay, (2, KEY), (1, QUERY))
        many(spread, (1, KEY), (3, KEY))
        many(relay, (3, QUERY), (2, VALUE))
        many(spread, (1, VALUE), (3, VALUE))
        many(relay, (1, KEY), (3, KEY))
        many(spread, (2, OUT_RET), (2, OUT_ATT), (2, OUT_ATT2))
        many(relay, (1, VALUE), (3, VALUE))
        lat_forward(0)
        many(spread, (1, OUT_RET))
        project(QUERY)
        many(relay, (2, OUT_RET), (2, OUT_ATT))
        many(spread, (1, OUT_ATT), (1, OUT_ATT2))
        lat_forward(1)
        many(relay, (2, OUT_ATT2))
        project(KEY)
        many(spread, (3, OUT_RET), (3, OUT_ATT), (3, OUT_ATT2))
        lat_far(0)
        project(VALUE)
        retain()
        own_kvup.wait()
        own_qup.wait()
        many(relay, (1, OUT_RET), (1, OUT_ATT), (1, OUT_ATT2))
        blocks = n_sp // LAT_PARTS
        for i in range(LAT_PARTS):
            lat_arrive(i)
            for b in range(i * blocks, (i + 1) * blocks):
                with jax.named_scope(f"expand#b={b}"):
                    expand(b)
            if i == 0:
                lat_far(1)
            for b in range(i * blocks, (i + 1) * blocks):
                if i == 0:
                    many(relay, (3, OUT_RET + b))
                with jax.named_scope(f"attend#b={b}"):
                    attend(b)
            if i == 0:
                many(relay, (3, OUT_ATT2))
        for u in out_weights:
            for k in range(n_sp):
                arrive(k, u)
        output()

    for u in range(UNITS):
        for k in range(n_sp):

            def drain(k=k, u=u):
                x_copy(k, u).wait_send()
                y_copy(k, u).wait_send()
                f_copy(k, u).wait_send()

            when(has(u, z), drain)
            if k and u != LAT:
                when(
                    has(u, origin_of(k)),
                    lambda k=k, u=u: z_copy(origin_of(k), u).wait_send(),
                )
    for place in lat_sources:
        pl.when(z != place)(
            lambda place=place: z_copy(place, LAT, lat_sources[place]).wait_send()
        )
    for d in others:
        shift_copy(d).wait_send()
    line_drain(tok_part, 0)
    for i in range(LAT_PARTS):
        pl.when(is_end)(lambda i=i: lat_send(i).wait_send())

        @pl.when(~is_end)
        def _(i=i):
            lat_copy(i, near_end, n_sp - 1 - z).wait_send()
            for origin in (q_place, kv_place):
                pair_copy(lat_part(i), i + 1, origin).wait_send()

    for c in range(OUT_PARTS):
        total = own_sum[n_sp - 1, :, out_columns(c)]
        for k in range(2):
            with jax.named_scope(f"rows#k={k}"):
                rows_arrival(k, c).wait_recv()
            total = total + row_in[k, c].astype(f32)
        out_vmem[c] = total.astype(bf16)
        out_copy(c).start()
    for c in range(OUT_PARTS):
        out_copy(c).wait()

    for j in range(n_sp):
        for c in range(OUT_PARTS):
            pair_sum(j, c).wait_send()
            if j < n_sp - 1:
                near_rows(j, c).wait_send()


def heads_plan(
    tokens,
    norm_gain,
    w_ret_query,
    w_ret_key,
    w_ret_value,
    w_q_down,
    w_kv_down,
    w_rope_key,
    w_q_up,
    w_kv_up,
    q_lat_gain,
    kv_lat_gain,
    att_norm_gain,
    ret_norm_gain,
    w_ret_out,
    w_att_out,
    head_rate,
    decay_shift,
    start_state,
):
    n_sp = lax.axis_size("sp")
    rows, width = tokens.shape[1:]
    length = n_sp * rows
    q_wide, kv_wide = w_q_down.shape[1], w_kv_down.shape[1]
    w_rows = w_q_down.shape[0]
    att_heads = w_q_up.shape[1] // (NOPE_DIM + ROPE_DIM) // 2

    ret_cos, ret_sin = wave_tables(length, RET_DIM)
    rope_cos, rope_sin = wave_tables(length, ROPE_DIM)
    pair_cos = np.concatenate([rope_cos] * 4, axis=1)
    pair_sin = np.concatenate([-rope_sin, rope_sin] * 2, axis=1)
    small = (
        w_rope_key.T,
        head_rate[None],
        norm_gain[None],
        q_lat_gain,
        kv_lat_gain[None],
        att_norm_gain.reshape(2, 1, -1),
        ret_norm_gain.reshape(n_sp, 1, -1),
        ret_cos,
        ret_sin,
        pair_cos,
        pair_sin,
    )
    dma = pltpu.SemaphoreType.DMA
    vmem = pltpu.VMEM
    f32, bf16 = jnp.float32, jnp.bfloat16
    half = rows // 2
    out_wide = 4 * n_sp * w_rows
    any_spec = pl.BlockSpec(memory_space=pl.ANY)
    mixed = pl.pallas_call(
        functools.partial(layer_kernel, n_sp, q_wide, kv_wide),
        out_shape=jax.ShapeDtypeStruct((half, out_wide), bf16),
        in_specs=[any_spec] * 23,
        out_specs=any_spec,
        scratch_shapes=[
            vmem((n_sp, rows, width), bf16),
            vmem((n_sp * 4 * w_rows, (UNITS - 1) * WIDE), bf16),
            vmem((n_sp * 4 * w_rows, q_wide), bf16),
            vmem((w_rows, q_wide), bf16),
            *[vmem(x.shape, x.dtype) for x in small],
            vmem((n_sp,) + decay_shift.shape[1:], f32),
            vmem((length, width), bf16),
            vmem((length, WIDE), f32),
            vmem((length, q_wide), f32),
            vmem((length, WIDE), bf16),
            vmem((length, WIDE), bf16),
            vmem((length, WIDE), bf16),
            vmem((2, 2, length, q_wide), bf16),
            vmem((RET_DIM, RET_DIM), f32),
            vmem((length, att_heads * NOPE_DIM), bf16),
            vmem((length, att_heads * ROPE_DIM), bf16),
            vmem((length, att_heads * (NOPE_DIM + VAL_DIM)), bf16),
            vmem((length, 2 * ROPE_DIM), bf16),
            vmem((w_kv_up.shape[0], att_heads * (NOPE_DIM + VAL_DIM)), bf16),
            vmem((w_q_up.shape[0], att_heads * (NOPE_DIM + ROPE_DIM)), bf16),
            vmem((length, WIDE + att_heads * VAL_DIM), bf16),
            vmem((n_sp, half, out_wide), f32),
            *[vmem((n_sp, OUT_PARTS, half, out_wide // OUT_PARTS), bf16)] * 2,
            vmem((n_sp - 1, OUT_PARTS, half, out_wide // OUT_PARTS), bf16),
            *[vmem((2, OUT_PARTS, half, out_wide // OUT_PARTS), bf16)] * 2,
            vmem((OUT_PARTS, half, out_wide // OUT_PARTS), bf16),
            dma((14,)),
            *[dma((n_sp, UNITS))] * 8,
            *[dma((1, n_sp))] * 2,
            dma((len(small),)),
            dma((OUT_PARTS,)),
            *[dma((n_sp, OUT_PARTS))] * 5,
            *[dma((LAT_PARTS + 1, n_sp))] * 5,
        ],
        compiler_params=pltpu.CompilerParams(
            collective_id=0, has_side_effects=True, vmem_limit_bytes=62 * 1024 * 1024
        ),
    )(
        tokens[0],
        w_q_down,
        w_kv_down,
        w_ret_query,
        w_ret_key,
        w_ret_value,
        w_ret_out,
        w_att_out,
        small[0],
        decay_shift[0],
        *small[1:],
        w_q_up,
        w_kv_up,
        start_state[0],
    )
    return mixed[None]


def solution(mesh):
    placed = (
        P("fs", "sp", None),
        P(),
        P(("sp", "fs"), "tp"),
        P(("sp", "fs"), "tp"),
        P(("sp", "fs"), "tp"),
        P(("sp", "fs"), "tp"),
        P(("sp", "fs"), "tp"),
        P(("sp", "fs"), None),
        P(None, "tp"),
        P(None, "tp"),
        P(),
        P(),
        P("tp"),
        P("tp"),
        P(("sp", "fs"), "tp"),
        P(("sp", "fs"), "tp"),
        P("tp"),
        P("fs", "tp", "sp"),
        P("fs", "tp", None, None),
    )

    def pick(*args):
        if heads_fit(
            mesh, args[16].shape[0], args[0].shape[0], args[5].shape[1], args[6].shape[1], args[8].shape[1]
        ):
            return heads_plan(*args)
        return rows_plan(*args)

    return jax.shard_map(
        pick,
        mesh=mesh,
        in_specs=placed,
        out_specs=P("fs", ("sp", "tp"), None),
        check_vma=False,
    )
```
